32 devices in a mesh: rep: 2 (over x), fs: 4 (over z), tp: 4 (over y, core).
Axes of the slice: x: 2, y: 2, z: 4, core: 2. Of those that a mesh axis runs over, the one named last changes fastest.
Arguments:
- tokens: bfloat16 [4096, 2048], P(('rep', 'fs', 'tp')), may hold values from -6 to 6
- mixer_gain: float32 [2048], replicated, may hold values from 0.1 to 1.9
- direct_weight: float32 [2048, 1024], P('fs', 'tp'), may hold values from -0.125 to 0.125
- direct_scale: float32 [1024], P('tp'), may hold values from 0.5 to 2
- value_weight: float32 [2048, 1024], P('fs', 'tp'), may hold values from -0.125 to 0.125
- value_scale: float32 [1024], P('tp'), may hold values from 0.5 to 8, as said below
- value_gain: float32 [1024], P('tp'), may hold values from 0.1 to 1.9
- value_shift: float32 [1024], P('tp'), may hold values from -3 to 3
- spatial_weight: bfloat16 [16, 128, 128], P('tp'), may hold values from -0.25 to 0.25
- spatial_bias: float32 [16, 128], P('tp'), may hold values from 0.1 to 1.9
- merge_weight: float32 [1024, 2048], P('tp', 'fs'), may hold values from -0.1875 to 0.1875
- merge_scale: float32 [2048], P('fs'), may hold values from 0.5 to 2
- channel_gain: float32 [2048], replicated, may hold values from 0.1 to 1.9
- expand_weight: float32 [2048, 8192], P('fs', 'tp'), may hold values from -0.125 to 0.125
- expand_scale: float32 [8192], P('tp'), may hold values from 0.5 to 2
- reduce_weight: float32 [8192, 2048], P('tp', 'fs'), may hold values from -0.0625 to 0.0625
- reduce_scale: float32 [2048], P('fs'), may hold values from 0.5 to 2
Outputs:
- result: bfloat16 [4096, 2048], P(('rep', 'fs', 'tp'))
The draws below stay inside these ranges and needn't reach their ends.
Inputs may be any that keep to these rules, and one draw needn't show every extreme that they name: `value_scale`: positive column scales.
All inputs are finite; a program needn't handle non-finite values.
Results may differ from the reference program's by a relative error of at most 0.024.
Values may be sent and summed in bfloat16 or wider, within the bound.
A program may use at most 64 MiB of HBM per device.

```python
import math
import jax
import jax.numpy as jnp
from jax import lax

D = 2048
GROUPS = 16
GDIM = 64
AW = 1024
FF = 8192
BLOCK = 128
TOK_DEV = 128
TOKENS = 4096
N_TP = 4


def draw_value_scale(key, part):
    ramp = jnp.exp(jnp.log(4.0) * jnp.arange(AW, dtype=jnp.float32) / (AW - 1))
    factor = jnp.exp(jax.random.uniform(key, (AW,), jnp.float32, jnp.log(0.7), jnp.log(1.4)))
    return ramp * factor


def levels(stream_key, shape, shards, low, top_value):
    level = 1.0
    for axis_at, blocks in shards:
        draws = jax.random.uniform(jax.random.fold_in(jax.random.fold_in(stream_key, 6), axis_at), (blocks,), jnp.float32, low / len(shards), top_value / len(shards))
        level = level * jnp.repeat(jnp.exp(draws), shape[axis_at] // blocks).reshape((-1,) + (1,) * (len(shape) - 1 - axis_at))
    return level


def scatter_about(rng, extent, deviation, bound, shards=(), kind=jnp.bfloat16):
    result = jax.random.normal(rng, extent, jnp.float32) * deviation
    if len(shards) > 0:
        result = levels(rng, extent, shards, -0.22, 0.18) * result
    return jnp.clip(result, min=-bound, max=bound).astype(kind)


def setup_inputs(seed: int = 0) -> dict:
    seeds = jax.random.split(jax.random.key(seed), 18)
    tokens = scatter_about(seeds[0], (TOKENS, D), 1.0, 6.0, ((0, 32),))
    mixer_gain = jnp.clip(1.0 + 0.18 * jax.random.normal(seeds[1], (D,), jnp.float32), 0.1, 1.9)
    direct_weight = scatter_about(seeds[2], (D, AW), D ** -0.5, 0.125, ((0, 4), (1, 4)), jnp.float32)
    direct_scale = jnp.clip(jnp.exp(math.log(2.0) - 1.3862944 * jax.random.uniform(seeds[3], (AW,), jnp.float32) ** levels(seeds[3], (AW,), ((0, 4),), -0.2, 0.2)), 0.5, 2.0)
    value_weight = scatter_about(seeds[4], (D, AW), D ** -0.5, 0.125, ((0, 4), (1, 4)), jnp.float32)
    value_scale = draw_value_scale(jax.random.fold_in(seeds[17], 71), 0)
    value_gain = jnp.clip(1.0 + 0.18 * jax.random.normal(seeds[6], (AW,), jnp.float32), 0.1, 1.9)
    value_shift = scatter_about(seeds[7], (AW,), 0.5, 3.0, ((0, 4),), jnp.float32)
    spatial_weight = scatter_about(seeds[8], (GROUPS, BLOCK, BLOCK), (4 * BLOCK) ** -0.5, 0.25, ((0, 4),))
    spatial_bias = jnp.clip(1.0 + 0.18 * jax.random.normal(seeds[9], (GROUPS, BLOCK), jnp.float32), 0.1, 1.9)
    merge_weight = scatter_about(seeds[10], (AW, D), AW ** -0.5, 0.1875, ((0, 4), (1, 4)), jnp.float32)
    merge_scale = jnp.clip(jnp.exp(math.log(2.0) - 1.3862944 * jax.random.uniform(seeds[11], (D,), jnp.float32) ** levels(seeds[11], (D,), ((0, 4),), -0.2, 0.2)), 0.5, 2.0)
    channel_gain = jnp.clip(1.0 + 0.18 * jax.random.normal(seeds[12], (D,), jnp.float32), 0.1, 1.9)
    expand_weight = scatter_about(seeds[13], (D, FF), D ** -0.5, 0.125, ((0, 4), (1, 4)), jnp.float32)
    expand_scale = jnp.clip(jnp.exp(math.log(2.0) - 1.3862944 * jax.random.uniform(seeds[14], (FF,), jnp.float32) ** levels(seeds[14], (FF,), ((0, 4),), -0.2, 0.2)), 0.5, 2.0)
    reduce_weight = scatter_about(seeds[15], (FF, D), FF ** -0.5, 0.0625, ((0, 4), (1, 4)), jnp.float32)
    reduce_scale = jnp.clip(jnp.exp(math.log(2.0) - 1.3862944 * jax.random.uniform(seeds[16], (D,), jnp.float32) ** levels(seeds[16], (D,), ((0, 4),), -0.2, 0.2)), 0.5, 2.0)
    return {"tokens": tokens, "mixer_gain": mixer_gain, "direct_weight": direct_weight, "direct_scale": direct_scale, "value_weight": value_weight, "value_scale": value_scale, "value_gain": value_gain, "value_shift": value_shift, "spatial_weight": spatial_weight, "spatial_bias": spatial_bias, "merge_weight": merge_weight, "merge_scale": merge_scale, "channel_gain": channel_gain, "expand_weight": expand_weight, "expand_scale": expand_scale, "reduce_weight": reduce_weight, "reduce_scale": reduce_scale}


epsilon = 1e-06

def rms_rows(rows, gain):
    floats = rows.astype(jnp.float32)
    scaled = floats * lax.rsqrt(lax.optimization_barrier(jnp.mean(floats * floats, axis=-1, keepdims=True)) + epsilon)
    return (scaled * gain).astype(jnp.bfloat16)

def split_sum(left, right, scale, parts):
    rows = left.shape[0]
    inner = left.shape[1] // parts
    lhs = left.reshape(rows, parts, inner).astype(jnp.float32)
    rhs = right.astype(jnp.bfloat16).astype(jnp.float32).reshape(parts, inner, right.shape[1])
    terms = jnp.einsum('gtk,tkd->tgd', lhs, rhs) * scale
    terms = lax.optimization_barrier(terms.astype(jnp.bfloat16)).astype(jnp.float32)
    return lax.optimization_barrier(jnp.sum(terms, axis=0))

def reference(tokens, mixer_gain, direct_weight, direct_scale, value_weight, value_scale, value_gain, value_shift, spatial_weight, spatial_bias, merge_weight, merge_scale, channel_gain, expand_weight, expand_scale, reduce_weight, reduce_scale):
    seq_rows = TOK_DEV * N_TP

    def one_sequence(rows):
        normed = rms_rows(rows, mixer_gain)
        direct = jax.nn.gelu(jnp.dot(normed, direct_weight.astype(jnp.bfloat16), preferred_element_type=jnp.float32) * direct_scale)
        value = jax.nn.gelu(jnp.dot(normed, value_weight.astype(jnp.bfloat16), preferred_element_type=jnp.float32) * value_scale)
        total = lax.optimization_barrier(jnp.sum(value, axis=1, keepdims=True))
        squares = lax.optimization_barrier(jnp.sum(value * value, axis=1, keepdims=True))
        mean = total / AW
        var = squares / AW - mean * mean
        gated_value = ((value - mean) * lax.rsqrt(var + epsilon) * value_gain + value_shift).astype(jnp.bfloat16)
        blocks = gated_value.reshape(seq_rows // BLOCK, BLOCK, GROUPS, GDIM).astype(jnp.float32)
        mixed = jnp.einsum('gpq,nqgc->npgc', spatial_weight.astype(jnp.float32), blocks)
        mixed = mixed + jnp.transpose(spatial_bias)[None, :, :, None]
        gated = (direct * mixed.reshape(seq_rows, AW)).astype(jnp.bfloat16)
        mix = split_sum(gated, merge_weight, merge_scale, N_TP)
        middle = (rows.astype(jnp.float32) + mix).astype(jnp.bfloat16)
        normed_mid = rms_rows(middle, channel_gain)
        upper = jnp.dot(normed_mid, expand_weight.astype(jnp.bfloat16), preferred_element_type=jnp.float32) * expand_scale
        hidden = jnp.square(jax.nn.relu(upper)).astype(jnp.bfloat16)
        lower = split_sum(hidden, reduce_weight, reduce_scale, N_TP)
        return (middle.astype(jnp.float32) + lower).astype(jnp.bfloat16)
    grouped = tokens.reshape(-1, seq_rows, D)
    return lax.map(one_sequence, grouped).reshape(tokens.shape)
```

```python
import jax
import jax.numpy as jnp
from jax import lax
from jax.experimental import pallas as pl
from jax.experimental.pallas import tpu as pltpu
from jax.sharding import PartitionSpec as P

GDIM = 64
BLOCK = 128


epsilon = 1e-06


def rms_rows(rows, gain):
    floats = rows.astype(jnp.float32)
    scaled = floats * lax.rsqrt(jnp.mean(floats * floats, axis=-1, keepdims=True) + epsilon)
    return (scaled * gain).astype(jnp.bfloat16)


def body(
    tokens,
    mixer_gain,
    direct_weight,
    direct_scale,
    value_weight,
    value_scale,
    value_gain,
    value_shift,
    spatial_weight,
    spatial_bias,
    merge_weight,
    merge_scale,
    channel_gain,
    expand_weight,
    expand_scale,
    reduce_weight,
    reduce_scale,
):
    direct_half = direct_weight.astype(jnp.bfloat16)
    value_half = value_weight.astype(jnp.bfloat16)
    merge_half = merge_weight.astype(jnp.bfloat16)
    expand_half = expand_weight.astype(jnp.bfloat16)
    reduce_half = reduce_weight.astype(jnp.bfloat16)
    full_expand, full_reduce, reduce_full_scale = (
        lax.all_gather(expand_half, "fs", axis=0, tiled=True),
        lax.all_gather(reduce_half, "fs", axis=1, tiled=True),
        lax.all_gather(reduce_scale.astype(jnp.bfloat16), "fs", axis=0, tiled=True).astype(
            reduce_scale.dtype
        ),
    )
    normed = rms_rows(tokens, mixer_gain)
    whole = lax.all_gather(normed, "tp", axis=0, tiled=True)
    seq_rows = whole.shape[0]
    local_width = direct_weight.shape[1]
    direct_pre = jnp.dot(
        whole,
        lax.all_gather(direct_half, "fs", axis=0, tiled=True),
        preferred_element_type=jnp.float32,
    )
    value_pre = jnp.dot(
        whole,
        lax.all_gather(value_half, "fs", axis=0, tiled=True),
        preferred_element_type=jnp.float32,
    )
    full_merge, merge_full_scale = (
        lax.all_gather(merge_half, "fs", axis=1, tiled=True),
        lax.all_gather(merge_scale.astype(jnp.bfloat16), "fs", axis=0, tiled=True).astype(
            merge_scale.dtype
        ),
    )
    direct = jax.nn.gelu(direct_pre * direct_scale)
    value = jax.nn.gelu(value_pre * value_scale)
    total, squares = lax.psum((jnp.sum(value, axis=1), jnp.sum(value * value, axis=1)), "tp")
    branch_width = local_width * lax.axis_size("tp")
    mean = (total / branch_width)[:, None]
    var = (squares / branch_width)[:, None] - mean * mean
    gated_value = ((value - mean) * lax.rsqrt(var + epsilon) * value_gain + value_shift).astype(
        jnp.bfloat16
    )
    local_groups = spatial_weight.shape[0]
    blocks = gated_value.reshape(seq_rows // BLOCK, BLOCK, local_groups, GDIM)
    mixed = jnp.einsum("gpq,nqgc->npgc", spatial_weight, blocks, preferred_element_type=jnp.float32)
    mixed = mixed + jnp.transpose(spatial_bias)[None, :, :, None]
    gated = (direct * mixed.reshape(seq_rows, local_width)).astype(jnp.bfloat16)
    rows = gated
    mix = lax.psum_scatter(
        (jnp.dot(rows, full_merge, preferred_element_type=jnp.float32) * merge_full_scale).astype(
            jnp.bfloat16
        ),
        "tp",
        scatter_dimension=0,
        tiled=True,
    ).astype(jnp.float32)
    middle = (tokens.astype(jnp.float32) + mix).astype(jnp.bfloat16)
    normed_mid = rms_rows(middle, channel_gain)
    whole_mid = lax.all_gather(normed_mid, "tp", axis=0, tiled=True)
    upper = jnp.dot(whole_mid, full_expand, preferred_element_type=jnp.float32)
    hidden = jnp.square(jax.nn.relu(upper * expand_scale)).astype(jnp.bfloat16)
    rows = hidden
    lower = lax.psum_scatter(
        (jnp.dot(rows, full_reduce, preferred_element_type=jnp.float32) * reduce_full_scale).astype(
            jnp.bfloat16
        ),
        "tp",
        scatter_dimension=0,
        tiled=True,
    ).astype(jnp.float32)
    return (middle.astype(jnp.float32) + lower).astype(jnp.bfloat16)


MESH = pl.DeviceIdType.MESH


def fused_kernel(
    tok_ref, mgain_ref, dscale_ref, vscale_ref, vgain_ref, vshift_ref, sw_ref, sbias_ref,
    mscale_ref, cgain_ref, exscale_ref, rscale_ref,
    dw_ref, vw_ref, mw_ref, ew_ref, rw_ref,
    out_ref,
    dv_f32, mg_f32, ex_f32, rd_f32,
    dv_all, mg_all, ex_all, ex_out, rd_all, rd_out,
    xg, act, stat, gated, p1, r1, s1, x1, mid,
    nm, hid, p2, r2, f1, a1, f2, a2, f3, a3,
    load_sem, wsend, wrecv, xsend, xrecv, csend, crecv, gsend, grecv, tsend, trecv, msend, mrecv,
    nsend, nrecv, fsend, frecv,
):
    rows, width = tok_ref.shape
    piece, local = dw_ref.shape
    unit = hid.shape[2]
    half = rows // 2
    thin = piece // 2
    r = lax.axis_index("rep")
    f = lax.axis_index("fs")
    t = lax.axis_index("tp")
    y, c = t // 2, t % 2
    z = f % 2
    mate = f + 1 - 2 * z
    peers = (mate, (f + 2) % 4, (mate + 2) % 4)
    sib = {"tp": y * 2 + (1 - c)}
    ynb = {"tp": (1 - y) * 2 + c}
    xnb = {"rep": 1 - r}
    znb = {"fs": mate}

    barrier = pltpu.get_barrier_semaphore()
    for dev in (sib, ynb, xnb) + tuple({"fs": peer} for peer in peers):
        pl.semaphore_signal(barrier, inc=1, device_id=dev, device_id_type=MESH)

    def span(start, size):
        return pl.ds(pl.multiple_of(start, size), size)

    loads = [
        pltpu.make_async_copy(source, target, load_sem.at[i])
        for i, (source, target) in enumerate(
            (
                (dw_ref, dv_f32.at[0]),
                (vw_ref, dv_f32.at[1]),
                (mw_ref, mg_f32),
                (ew_ref.at[:, span((r * 2 + z) * unit, unit)], ex_f32.at[0]),
                (ew_ref.at[:, span((r * 2 + 1 - z) * unit, unit)], ex_f32.at[1]),
                (rw_ref.at[span((r * 2 + z) * unit, unit)], rd_f32.at[0]),
                (rw_ref.at[span((r * 2 + 1 - z) * unit, unit)], rd_f32.at[1]),
            )
        )
    ]
    for load in loads:
        load.start()

    def rcopy(src, dst, ssem, rsem, dev):
        return pltpu.make_async_remote_copy(
            src_ref=src, dst_ref=dst, send_sem=ssem, recv_sem=rsem,
            device_id=dev, device_id_type=MESH,
        )

    def item(i, slot, q):
        if i < 2:
            return dv_all.at[slot, span(q * 2 * rows + i * rows, rows)]
        return mg_all.at[slot, span(q * rows, rows)]

    def origin(way, d):
        return lax.rem(f + (4 - d if way == 0 else d), 4)

    def comes(way, d):
        return f >= d if way == 0 else f + d <= 3

    def goes(way):
        return f < 3 if way == 0 else f > 0

    def inward(way):
        return f < 2 if way == 0 else f >= 2

    def hop(i, way, d):
        ref = item(i, origin(way, d), r)
        to = lax.rem(f + (1 if way == 0 else 3), 4)
        return rcopy(ref, ref, wsend.at[i, way, d], wrecv.at[i, way, d], {"fs": to})

    def over(i, way, d):
        ref = item(i, origin(way, d), r)
        return rcopy(ref, ref, xsend.at[i, way, d - 1], xrecv.at[i, way, d - 1], xnb)

    def relay(i, d):
        for way in range(2):

            @pl.when(comes(way, d))
            def _(way=way):
                hop(i, way, d - 1).wait_recv()
                over(i, way, d).start()

            if d < 3:

                @pl.when(jnp.logical_and(comes(way, d), goes(way)))
                def _(way=way):
                    hop(i, way, d).start()

    def over_wait(i, d):
        for way in range(2):

            @pl.when(comes(way, d))
            def _(way=way):
                over(i, way, d).wait_recv()

    def ex_slot(slot):
        return ex_all.at[span(slot * piece, piece)]

    def chunk(i, j):
        if i == 0:
            src, dst = (ex_slot(f) if j == 1 else ex_out), ex_slot(f)
        else:
            src = rd_all.at[f, i - 1] if j == 1 else rd_out.at[i - 1]
            dst = rd_all.at[f, i - 1]
        return rcopy(src, dst, csend.at[i, j], crecv.at[i, j], {"fs": peers[j]})

    def norm(x, gain):
        return (
            x * lax.rsqrt(jnp.mean(x * x, axis=-1, keepdims=True) + epsilon) * gain
        ).astype(jnp.bfloat16)

    def block(n, size=1):
        return pl.ds(pl.multiple_of(n * rows, rows), size * rows)

    def columns(slot):
        return span(slot * piece, piece)

    for i in range(2):
        loads[i].wait()
        dv_all[f, :, i * local : (i + 1) * local] = dv_f32[i].astype(jnp.bfloat16)
    mine = xg.at[block(c * 2 + y)]
    mine[...] = norm(tok_ref[...].astype(jnp.float32), mgain_ref[...])
    far = xg.at[block(c * 2 + 1 - y)]
    gather = (
        rcopy(mine, mine, gsend.at[0], grecv.at[0], sib),
        rcopy(mine, mine, gsend.at[1], grecv.at[1], ynb),
        rcopy(far, far, gsend.at[2], grecv.at[2], sib),
    )
    pl.semaphore_wait(barrier, 6)
    for i in range(2):
        for way in range(2):

            @pl.when(goes(way))
            def _(i=i, way=way):
                hop(i, way, 0).start()

    gather[1].start()
    gather[0].start()
    loads[2].wait()
    mg_all[f] = (mg_f32[...] * mscale_ref[...]).astype(jnp.bfloat16)
    loads[3].wait()
    ex_all[columns(f)] = ex_f32[0].astype(jnp.bfloat16)
    loads[4].wait()
    ex_out[...] = ex_f32[1].astype(jnp.bfloat16)
    relay(0, 1)
    relay(1, 1)
    for way in range(2):

        @pl.when(inward(way))
        def _(way=way):
            hop(2, way, 0).start()

    relay(0, 2)
    relay(1, 2)
    for way in range(2):

        @pl.when(jnp.logical_and(jnp.logical_not(inward(way)), goes(way)))
        def _(way=way):
            hop(2, way, 0).start()

    gather[1].wait_recv()
    gather[2].start()
    relay(2, 1)
    chunk(0, 1).start()
    inner = jnp.logical_or(f == 1, f == 2)

    @pl.when(inner)
    def _():
        chunk(0, 2).start()

    loads[5].wait()
    rd_all[f, 0] = (rd_f32[0, :, :thin] * rscale_ref[:, :thin]).astype(jnp.bfloat16)
    rd_all[f, 1] = (rd_f32[0, :, thin:] * rscale_ref[:, thin:]).astype(jnp.bfloat16)
    loads[6].wait()
    rd_out[0] = (rd_f32[1, :, :thin] * rscale_ref[:, :thin]).astype(jnp.bfloat16)
    rd_out[1] = (rd_f32[1, :, thin:] * rscale_ref[:, thin:]).astype(jnp.bfloat16)

    def project(slot):
        return jnp.dot(xg[:, columns(slot)], dv_all[slot], preferred_element_type=jnp.float32)

    gather[0].wait_recv()
    gather[2].wait_recv()
    act[...] = project(f)
    relay(0, 3)
    relay(1, 3)
    relay(2, 2)

    def project_more(d):
        for i in range(2):
            over_wait(i, d)
        for way in range(2):

            @pl.when(comes(way, d))
            def _(way=way):
                act[...] += project(origin(way, d))

    project_more(1)
    project_more(2)
    project_more(3)
    relay(2, 3)
    dvscale = jnp.concatenate([dscale_ref[...], vscale_ref[...]], axis=1)
    act[...] = jax.nn.gelu(act[...] * dvscale)

    lane = lax.broadcasted_iota(jnp.int32, (rows, rows), 1)
    for n in range(4):
        value = act[n * rows : (n + 1) * rows, local:]
        total = jnp.sum(value, axis=1, keepdims=True)
        squares = jnp.sum(value * value, axis=1, keepdims=True)
        table = jnp.where(lane == 0, total, jnp.where(lane == 1, squares, 0.0))
        stat[t, n] = jnp.transpose(table)[:8]
    stats = [
        rcopy(stat.at[t], stat.at[t], tsend.at[0], trecv.at[0], sib),
        rcopy(stat.at[t], stat.at[t], tsend.at[1], trecv.at[1], ynb),
        rcopy(
            stat.at[(1 - y) * 2 + c], stat.at[(1 - y) * 2 + c], tsend.at[2], trecv.at[2], sib
        ),
    ]
    stats[1].start()
    stats[0].start()
    groups = sbias_ref.shape[0]
    down = lax.broadcasted_iota(jnp.int32, (rows, rows), 0)
    bias = jnp.zeros((rows, rows), jnp.float32)
    for n in range(groups):
        bias = jnp.where(down == n, sbias_ref[n : n + 1, :], bias)
    bias = jnp.transpose(bias)
    stats[1].wait_recv()
    stats[2].start()
    stats[0].wait_recv()
    stats[2].wait_recv()
    inverse = 1.0 / (local * 4)
    group_lane = lax.broadcasted_iota(jnp.int32, (rows, 128), 1) // GDIM
    for n in range(4):
        here = slice(n * rows, (n + 1) * rows)
        summed = stat[0, n] + stat[1, n] + stat[2, n] + stat[3, n]
        table = jnp.transpose(jnp.concatenate([summed] * (rows // 8), axis=0))
        mean = table[:, 0:1] * inverse
        var = table[:, 1:2] * inverse - mean * mean
        gv = (
            (act[here, local:] - mean) * lax.rsqrt(var + epsilon) * vgain_ref[...]
            + vshift_ref[...]
        ).astype(jnp.bfloat16)
        per = 128 // GDIM
        for j in range(local // 128):
            at = slice(j * 128, (j + 1) * 128)
            mixed = jnp.dot(sw_ref[j * per], gv[:, at], preferred_element_type=jnp.float32)
            mixed = mixed + bias[:, j * per : j * per + 1]
            for k in range(1, per):
                n_group = j * per + k
                other = jnp.dot(sw_ref[n_group], gv[:, at], preferred_element_type=jnp.float32)
                other = other + bias[:, n_group : n_group + 1]
                mixed = jnp.where(group_lane == k, other, mixed)
            gated[here, at] = (act[here, at] * mixed).astype(jnp.bfloat16)

    base = f - z
    order = (base, base + 1, 2 - base, 3 - base)

    def merge_pair(k):
        return rcopy(
            p1.at[k, block((1 - c) * 2, 2)], r1.at[k], msend.at[k, 0], mrecv.at[k, 0], sib
        )

    def merge_far(k):
        return rcopy(s1.at[k], x1.at[k], msend.at[k, 1], mrecv.at[k, 1], ynb)

    def merge_send(k):
        merge_pair(k).wait_recv()
        s1[k] = (
            p1[k, block(c * 2 + 1 - y)].astype(jnp.float32)
            + r1[k, block(1 - y)].astype(jnp.float32)
        ).astype(jnp.bfloat16)
        merge_far(k).start()

    for k, slot in enumerate(order):
        if k == 0:
            for d in range(1, 4):
                over_wait(2, d)
        p1[k] = jnp.dot(gated[...], mg_all[slot], preferred_element_type=jnp.float32).astype(
            jnp.bfloat16
        )
        merge_pair(k).start()
        if k > 0:
            merge_send(k - 1)
    merge_send(3)
    for k, slot in enumerate(order):
        merge_far(k).wait_recv()
        mid[:, columns(slot)] = (
            tok_ref[:, columns(slot)].astype(jnp.float32)
            + p1[k, block(c * 2 + y)].astype(jnp.float32)
            + r1[k, block(y)].astype(jnp.float32)
            + x1[k].astype(jnp.float32)
        ).astype(jnp.bfloat16)

    def group(zz, rr, yy):
        return zz * 4 + rr * 2 + yy

    def place(zz, rr, yy):
        return nm.at[group(zz, rr, yy), c]

    mine = place(z, r, y)
    mine[...] = norm(mid[...].astype(jnp.float32), cgain_ref[...])
    over_fs = rcopy(mine, mine, nsend.at[20], nrecv.at[20], znb)

    def spreading(b, zz):
        here, from_x = place(zz, r, y), place(zz, 1 - r, y)
        from_y, from_xy = place(zz, r, 1 - y), place(zz, 1 - r, 1 - y)

        def low(ref):
            return ref.at[pl.ds(0, half)]

        def high(ref):
            return ref.at[pl.ds(half, half)]

        routes = (
            (low(here), xnb), (high(here), xnb), (high(here), ynb), (low(here), ynb), (here, sib),
            (low(from_x), ynb), (high(from_y), xnb),
            (from_x, sib), (from_y, sib), (from_xy, sib),
        )
        return tuple(
            rcopy(ref, ref, nsend.at[10 * b + k], nrecv.at[10 * b + k], dev)
            for k, (ref, dev) in enumerate(routes)
        )

    near, away = spreading(0, z), spreading(1, 1 - z)

    def first(spread):
        for k in (0, 2, 1, 3, 4):
            spread[k].start()

    def second(spread):
        spread[0].wait_recv()
        spread[5].start()
        spread[2].wait_recv()
        spread[6].start()

    def third(spread):
        spread[1].wait_recv()
        spread[7].start()
        spread[3].wait_recv()
        spread[8].start()

    def fourth(spread):
        spread[5].wait_recv()
        spread[6].wait_recv()
        spread[9].start()

    def gathered(spread):
        for k in (4, 7, 8, 9):
            spread[k].wait_recv()

    over_fs.start()
    first(near)

    @pl.when(jnp.logical_not(inner))
    def _():
        chunk(0, 2).start()

    chunk(0, 0).start()
    for i in range(1, 3):
        chunk(i, 0).start()
    for i in range(1, 3):
        for j in range(1, 3):
            chunk(i, j).start()
    second(near)
    third(near)
    over_fs.wait_recv()
    first(away)
    fourth(near)
    second(away)
    third(away)

    tall = 2 * rows
    exscale = exscale_ref[:, span((r * 2 + z) * unit, unit)]

    def expand(zz):
        def step(i, _):
            g = zz * 4 + i
            upper = jnp.dot(
                nm[g].reshape(tall, width), ex_all[...], preferred_element_type=jnp.float32
            ) * exscale
            hid[g] = jnp.square(jax.nn.relu(upper)).astype(jnp.bfloat16)

        lax.fori_loop(0, 4, step, None)

    steps = ((0, 0), (1, 0), (0, 1), (1, 1), (2, 0), (3, 0), (2, 1), (3, 1))
    near_half, far_half = 0, 1
    units = tuple((k, h) for h in range(2) for k in range(4)) + tuple(
        (k + p, h) for k in (4, 6) for h in range(2) for p in range(2)
    )

    def plane(h):
        return z if h == near_half else 1 - z

    def arrived(side, j):
        rcopy(
            rd_out.at[side], rd_all.at[f, side], csend.at[1 + side, j], crecv.at[1 + side, j], znb
        ).wait_recv()

    def reduce(u):
        k, h = units[u]
        from_slot, side = steps[k]
        slot = order[from_slot]
        if h == near_half:
            if from_slot == 0:
                arrived(side, 0)
            elif from_slot > 1:
                arrived(side, 1 + (from_slot + z) % 2)
        zz = plane(h)

        def step(i, _):
            g = zz * 4 + i * 2
            p2[k, pl.ds(g, 2)] = (
                jnp.dot(
                    hid[pl.ds(g, 2)].reshape(2 * tall, unit), rd_all[slot, side],
                    preferred_element_type=jnp.float32,
                )
                .astype(jnp.bfloat16)
                .reshape(2, 2, rows, thin)
            )

        lax.fori_loop(0, 2, step, None)
        pair(u).start()

    def pair(u):
        k, h = units[u]
        at = pl.ds(plane(h) * 4, 4)
        return rcopy(p2.at[k, at, 1 - c], r2.at[k, at], fsend.at[0, u], frecv.at[0, u], sib)

    def summed_pair(k, g):
        return p2[k, g, c].astype(jnp.float32) + r2[k, g].astype(jnp.float32)

    def hop_one(u):
        return rcopy(
            f1.at[u], a1.at[u], fsend.at[1, u], frecv.at[1, u], (ynb, xnb)[units[u][0] % 2]
        )

    def hop_two(u):
        return rcopy(
            f2.at[u], a2.at[u], fsend.at[2, u], frecv.at[2, u], (xnb, ynb)[units[u][0] % 2]
        )

    def hop_three(k):
        return rcopy(f3.at[k], a3.at[k], fsend.at[3, k], frecv.at[3, k], znb)

    def send_one(u):
        k, h = units[u]
        zz = plane(h)
        pair(u).wait_recv()
        for n in range(2):
            g = group(zz, n, 1 - y) if k % 2 == 0 else group(zz, 1 - r, n)
            f1[u, n] = summed_pair(k, g).astype(jnp.bfloat16)
        hop_one(u).start()

    def send_two(u):
        k, h = units[u]
        zz = plane(h)
        hop_one(u).wait_recv()
        g, n = (group(zz, 1 - r, y), 1 - r) if k % 2 == 0 else (group(zz, r, 1 - y), 1 - y)
        f2[u] = (summed_pair(k, g) + a1[u, n].astype(jnp.float32)).astype(jnp.bfloat16)
        hop_two(u).start()

    def own_sum(u):
        k, h = units[u]
        n = r if k % 2 == 0 else y
        hop_two(u).wait_recv()
        return (
            summed_pair(k, group(plane(h), r, y))
            + a1[u, n].astype(jnp.float32)
            + a2[u].astype(jnp.float32)
        )

    def send_three(u):
        k, h = units[u]
        if h == far_half:
            f3[k] = own_sum(u).astype(jnp.bfloat16)
            hop_three(k).start()

    for j in range(3):
        chunk(0, j).wait_recv()
    gathered(near)
    expand(z)
    done = set()

    def once(action, u):
        if 0 <= u < len(units) and (action, u) not in done:
            done.add((action, u))
            action(u)

    for u in range(len(units) + 5):
        if u == 4:
            once(send_one, 3)
            fourth(away)
            gathered(away)
            expand(1 - z)
            once(send_two, 0)
        if u == 8:
            once(send_one, 7)
        once(reduce, u)
        once(send_one, u - 1)
        if u != 3:
            once(send_two, u - 3)
        once(send_three, u - 5)
    for k, (from_slot, side) in enumerate(steps):
        at = span(order[from_slot] * piece + side * thin, thin)
        near_sum = own_sum(units.index((k, near_half)))
        hop_three(k).wait_recv()
        out_ref[:, at] = (
            mid[:, at].astype(jnp.float32) + near_sum + a3[k].astype(jnp.float32)
        ).astype(jnp.bfloat16)

    for i in range(3):
        for way in range(2):
            for d in range(3):

                @pl.when(jnp.logical_and(comes(way, d), goes(way)))
                def _(i=i, way=way, d=d):
                    hop(i, way, d).wait_send()

                @pl.when(comes(way, d + 1))
                def _(i=i, way=way, d=d):
                    over(i, way, d + 1).wait_send()

        for j in range(3):
            chunk(i, j).wait_send()
    for copy in gather + tuple(stats) + near + away + (over_fs,):
        copy.wait_send()
    for k in range(4):
        merge_pair(k).wait_send()
        merge_far(k).wait_send()
    for u in range(len(units)):
        pair(u).wait_send()
        hop_one(u).wait_send()
        hop_two(u).wait_send()
    for k in range(len(steps)):
        hop_three(k).wait_send()


def fused_body(
    tokens,
    mixer_gain,
    direct_weight,
    direct_scale,
    value_weight,
    value_scale,
    value_gain,
    value_shift,
    spatial_weight,
    spatial_bias,
    merge_weight,
    merge_scale,
    channel_gain,
    expand_weight,
    expand_scale,
    reduce_weight,
    reduce_scale,
):
    bf = jnp.bfloat16
    rows, width = tokens.shape
    piece, local = direct_weight.shape
    unit = expand_weight.shape[1] // 4
    thin = piece // 2
    seq = 4 * rows
    vm = pltpu.VMEM
    dma = pltpu.SemaphoreType.DMA
    f32 = jnp.float32
    small = (
        tokens, mixer_gain[None], direct_scale[None], value_scale[None], value_gain[None],
        value_shift[None], spatial_weight, spatial_bias, merge_scale[None], channel_gain[None],
        expand_scale[None], reduce_scale[None],
    )
    large = (direct_weight, value_weight, merge_weight, expand_weight, reduce_weight)
    return pl.pallas_call(
        fused_kernel,
        out_shape=jax.ShapeDtypeStruct((rows, width), bf),
        in_specs=[pl.BlockSpec(memory_space=pltpu.VMEM)] * len(small)
        + [pl.BlockSpec(memory_space=pl.ANY)] * len(large),
        out_specs=pl.BlockSpec(memory_space=pltpu.VMEM),
        scratch_shapes=[
            vm((2, piece, local), f32),
            vm((local, piece), f32),
            vm((2, piece, unit), f32),
            vm((2, unit, piece), f32),
            vm((4, piece, 2 * local), bf),
            vm((4, local, piece), bf),
            vm((4 * piece, unit), bf),
            vm((piece, unit), bf),
            vm((4, 2, unit, thin), bf),
            vm((2, unit, thin), bf),
            vm((seq, width), bf),
            vm((seq, 2 * local), f32),
            vm((4, 4, 8, rows), f32),
            vm((seq, local), bf),
            vm((4, seq, piece), bf),
            vm((4, 2 * rows, piece), bf),
            vm((4, rows, piece), bf),
            vm((4, rows, piece), bf),
            vm((rows, width), bf),
            vm((8, 2, rows, width), bf),
            vm((8, 2 * rows, unit), bf),
            vm((8, 8, 2, rows, thin), bf),
            vm((8, 8, rows, thin), bf),
            vm((16, 2, rows, thin), bf),
            vm((16, 2, rows, thin), bf),
            vm((16, rows, thin), bf),
            vm((16, rows, thin), bf),
            vm((8, rows, thin), bf),
            vm((8, rows, thin), bf),
            dma((7,)),
            dma((3, 2, 3)), dma((3, 2, 3)),
            dma((3, 2, 3)), dma((3, 2, 3)),
            dma((3, 3)), dma((3, 3)),
            dma((3,)), dma((3,)),
            dma((3,)), dma((3,)),
            dma((4, 2)), dma((4, 2)),
            dma((21,)), dma((21,)),
            dma((4, 16)), dma((4, 16)),
        ],
        compiler_params=pltpu.CompilerParams(
            collective_id=0, has_side_effects=True, vmem_limit_bytes=62 * 1024 * 1024
        ),
    )(*small, *large)


def solution(mesh):
    sizes = mesh.shape
    fused = sizes["rep"] == 2 and sizes["fs"] == 4 and sizes["tp"] == 4
    return jax.shard_map(
        fused_body if fused else body,
        mesh=mesh,
        in_specs=(
            P(("rep", "fs", "tp"), None),
            P(),
            P("fs", "tp"),
            P("tp"),
            P("fs", "tp"),
            P("tp"),
            P("tp"),
            P("tp"),
            P("tp", None, None),
            P("tp", None),
            P("tp", "fs"),
            P("fs"),
            P(),
            P("fs", "tp"),
            P("tp"),
            P("tp", "fs"),
            P("fs"),
        ),
        out_specs=P(("rep", "fs", "tp"), None),
        check_vma=False,
    )
```

```python
import jax
import jax.numpy as jnp
from jax import lax
from jax.experimental import pallas as pl
from jax.experimental.pallas import tpu as pltpu
from jax.sharding import PartitionSpec as P

GDIM = 64
BLOCK = 128


epsilon = 1e-06


def rms_rows(rows, gain):
    floats = rows.astype(jnp.float32)
    scaled = floats * lax.rsqrt(jnp.mean(floats * floats, axis=-1, keepdims=True) + epsilon)
    return (scaled * gain).astype(jnp.bfloat16)


def body(
    tokens,
    mixer_gain,
    direct_weight,
    direct_scale,
    value_weight,
    value_scale,
    value_gain,
    value_shift,
    spatial_weight,
    spatial_bias,
    merge_weight,
    merge_scale,
    channel_gain,
    expand_weight,
    expand_scale,
    reduce_weight,
    reduce_scale,
):
    direct_half = direct_weight.astype(jnp.bfloat16)
    value_half = value_weight.astype(jnp.bfloat16)
    merge_half = merge_weight.astype(jnp.bfloat16)
    expand_half = expand_weight.astype(jnp.bfloat16)
    reduce_half = reduce_weight.astype(jnp.bfloat16)
    full_expand, full_reduce, reduce_full_scale = (
        lax.all_gather(expand_half, "fs", axis=0, tiled=True),
        lax.all_gather(reduce_half, "fs", axis=1, tiled=True),
        lax.all_gather(reduce_scale.astype(jnp.bfloat16), "fs", axis=0, tiled=True).astype(
            reduce_scale.dtype
        ),
    )
    normed = rms_rows(tokens, mixer_gain)
    whole = lax.all_gather(normed, "tp", axis=0, tiled=True)
    seq_rows = whole.shape[0]
    local_width = direct_weight.shape[1]
    direct_pre = jnp.dot(
        whole,
        lax.all_gather(direct_half, "fs", axis=0, tiled=True),
        preferred_element_type=jnp.float32,
    )
    value_pre = jnp.dot(
        whole,
        lax.all_gather(value_half, "fs", axis=0, tiled=True),
        preferred_element_type=jnp.float32,
    )
    full_merge, merge_full_scale = (
        lax.all_gather(merge_half, "fs", axis=1, tiled=True),
        lax.all_gather(merge_scale.astype(jnp.bfloat16), "fs", axis=0, tiled=True).astype(
            merge_scale.dtype
        ),
    )
    direct = jax.nn.gelu(direct_pre * direct_scale)
    value = jax.nn.gelu(value_pre * value_scale)
    total, squares = lax.psum((jnp.sum(value, axis=1), jnp.sum(value * value, axis=1)), "tp")
    branch_width = local_width * lax.axis_size("tp")
    mean = (total / branch_width)[:, None]
    var = (squares / branch_width)[:, None] - mean * mean
    gated_value = ((value - mean) * lax.rsqrt(var + epsilon) * value_gain + value_shift).astype(
        jnp.bfloat16
    )
    local_groups = spatial_weight.shape[0]
    blocks = gated_value.reshape(seq_rows // BLOCK, BLOCK, local_groups, GDIM)
    mixed = jnp.einsum("gpq,nqgc->npgc", spatial_weight, blocks, preferred_element_type=jnp.float32)
    mixed = mixed + jnp.transpose(spatial_bias)[None, :, :, None]
    gated = (direct * mixed.reshape(seq_rows, local_width)).astype(jnp.bfloat16)
    rows = gated
    mix = lax.psum_scatter(
        (jnp.dot(rows, full_merge, preferred_element_type=jnp.float32) * merge_full_scale).astype(
            jnp.bfloat16
        ),
        "tp",
        scatter_dimension=0,
        tiled=True,
    ).astype(jnp.float32)
    middle = (tokens.astype(jnp.float32) + mix).astype(jnp.bfloat16)
    normed_mid = rms_rows(middle, channel_gain)
    whole_mid = lax.all_gather(normed_mid, "tp", axis=0, tiled=True)
    upper = jnp.dot(whole_mid, full_expand, preferred_element_type=jnp.float32)
    hidden = jnp.square(jax.nn.relu(upper * expand_scale)).astype(jnp.bfloat16)
    rows = hidden
    lower = lax.psum_scatter(
        (jnp.dot(rows, full_reduce, preferred_element_type=jnp.float32) * reduce_full_scale).astype(
            jnp.bfloat16
        ),
        "tp",
        scatter_dimension=0,
        tiled=True,
    ).astype(jnp.float32)
    return (middle.astype(jnp.float32) + lower).astype(jnp.bfloat16)


MESH = pl.DeviceIdType.MESH


def fused_kernel(
    tok_ref, mgain_ref, dscale_ref, vscale_ref, vgain_ref, vshift_ref, sw_ref, sbias_ref,
    mscale_ref, cgain_ref, exscale_ref, rscale_ref,
    dw_ref, vw_ref, mw_ref, ew_ref, rw_ref,
    out_ref,
    dv_f32, mg_f32, ex_f32, rd_f32,
    dv_all, mg_all, ex_all, ex_own, rd_all, rd_own,
    xg, act, stat, gated, p1, r1, s1, x1, mid,
    nm, hid, p2, r2, f1, a1, f2, a2, f3, a3,
    load_sem, wsend, wrecv, xsend, xrecv, csend, crecv, gsend, grecv, tsend, trecv, msend, mrecv,
    nsend, nrecv, fsend, frecv,
):
    rows, width = tok_ref.shape
    piece, local = dw_ref.shape
    big = hid.shape[2]
    wide = ex_own.shape[1]
    small = wide - big
    half = rows // 2
    thin = piece // 2
    r = lax.axis_index("rep")
    f = lax.axis_index("fs")
    t = lax.axis_index("tp")
    y, c = t // 2, t % 2
    z = f % 2
    mate = f + 1 - 2 * z
    peers = (mate, (f + 2) % 4, (mate + 2) % 4)
    sib = {"tp": y * 2 + (1 - c)}
    ynb = {"tp": (1 - y) * 2 + c}
    xnb = {"rep": 1 - r}
    znb = {"fs": mate}

    barrier = pltpu.get_barrier_semaphore()
    for dev in (sib, ynb, xnb) + tuple({"fs": peer} for peer in peers):
        pl.semaphore_signal(barrier, inc=1, device_id=dev, device_id_type=MESH)

    def span(start, size):
        return pl.ds(pl.multiple_of(start, size), size)

    loads = [
        pltpu.make_async_copy(source, target, load_sem.at[i])
        for i, (source, target) in enumerate(
            (
                (dw_ref, dv_f32.at[0]),
                (vw_ref, dv_f32.at[1]),
                (mw_ref, mg_f32),
                (ew_ref.at[:, span(r * wide, wide)], ex_f32),
                (rw_ref.at[span(r * wide, wide)], rd_f32),
            )
        )
    ]
    for load in loads:
        load.start()

    def rcopy(src, dst, ssem, rsem, dev):
        return pltpu.make_async_remote_copy(
            src_ref=src, dst_ref=dst, send_sem=ssem, recv_sem=rsem,
            device_id=dev, device_id_type=MESH,
        )

    def item(i, slot, q):
        if i < 2:
            return dv_all.at[slot, span(q * 2 * rows + i * rows, rows)]
        return mg_all.at[slot, span(q * rows, rows)]

    def origin(way, d):
        return lax.rem(f + (4 - d if way == 0 else d), 4)

    def comes(way, d):
        return f >= d if way == 0 else f + d <= 3

    def goes(way):
        return f < 3 if way == 0 else f > 0

    def inward(way):
        return f < 2 if way == 0 else f >= 2

    def hop(i, way, d):
        ref = item(i, origin(way, d), r)
        to = lax.rem(f + (1 if way == 0 else 3), 4)
        return rcopy(ref, ref, wsend.at[i, way, d], wrecv.at[i, way, d], {"fs": to})

    def over(i, way, d):
        ref = item(i, origin(way, d), r)
        return rcopy(ref, ref, xsend.at[i, way, d - 1], xrecv.at[i, way, d - 1], xnb)

    def relay(i, d):
        for way in range(2):

            @pl.when(comes(way, d))
            def _(way=way):
                hop(i, way, d - 1).wait_recv()
                over(i, way, d).start()

            if d < 3:

                @pl.when(jnp.logical_and(comes(way, d), goes(way)))
                def _(way=way):
                    hop(i, way, d).start()

    def over_wait(i, d):
        for way in range(2):

            @pl.when(comes(way, d))
            def _(way=way):
                over(i, way, d).wait_recv()

    inner = jnp.logical_or(f == 1, f == 2)
    outer = jnp.logical_not(inner)

    def part(to_inner):
        return (0, big) if to_inner else (big, small)

    def ex_copy(j, to_inner, h=None):
        first, size = part(to_inner)
        start, count = (0, piece) if h is None else (h * thin, thin)
        n = j + 1 if h is None else h
        return rcopy(
            ex_own.at[pl.ds(start, count), pl.ds(first, size)],
            ex_all.at[pl.ds(pl.multiple_of(f * piece + start, thin), count), pl.ds(0, size)],
            csend.at[n], crecv.at[n], {"fs": peers[j]},
        )

    def rd_copy(side, j, to_inner, index=None):
        first, size = part(to_inner)
        n = 4 + side * 3 + (j if index is None else index)
        return rcopy(
            rd_own.at[side, pl.ds(first, size)], rd_all.at[f, side, pl.ds(0, size)],
            csend.at[n], crecv.at[n], {"fs": peers[j]},
        )

    def both(action):
        @pl.when(inner)
        def _():
            action(True)

        @pl.when(outer)
        def _():
            action(False)

    def ex_copies(to_inner):
        return [ex_copy(0, to_inner[0], 0), ex_copy(0, to_inner[0], 1)] + [
            ex_copy(j, to_inner[j]) for j in range(1, 3)
        ]

    def norm(x, gain):
        return (
            x * lax.rsqrt(jnp.mean(x * x, axis=-1, keepdims=True) + epsilon) * gain
        ).astype(jnp.bfloat16)

    def block(n, size=1):
        return pl.ds(pl.multiple_of(n * rows, rows), size * rows)

    def columns(slot):
        return span(slot * piece, piece)

    for i in range(2):
        loads[i].wait()
        dv_all[f, :, i * local : (i + 1) * local] = dv_f32[i].astype(jnp.bfloat16)
    mine = xg.at[block(c * 2 + y)]
    mine[...] = norm(tok_ref[...].astype(jnp.float32), mgain_ref[...])
    far = xg.at[block(c * 2 + 1 - y)]
    gather = (
        rcopy(mine, mine, gsend.at[0], grecv.at[0], sib),
        rcopy(mine, mine, gsend.at[1], grecv.at[1], ynb),
        rcopy(far, far, gsend.at[2], grecv.at[2], sib),
    )
    pl.semaphore_wait(barrier, 6)
    for i in range(2):
        for way in range(2):

            @pl.when(goes(way))
            def _(i=i, way=way):
                hop(i, way, 0).start()

    gather[1].start()
    gather[0].start()
    loads[2].wait()
    mg_all[f] = (mg_f32[...] * mscale_ref[...]).astype(jnp.bfloat16)
    loads[3].wait()
    ex_own[...] = ex_f32[...].astype(jnp.bfloat16)

    relay(0, 1)
    relay(1, 1)
    for way in range(2):

        @pl.when(inward(way))
        def _(way=way):
            hop(2, way, 0).start()

    @pl.when(outer)
    def _():
        for h in range(2):
            ex_copy(0, True, h).start()

    relay(0, 2)
    relay(1, 2)
    for way in range(2):

        @pl.when(jnp.logical_and(jnp.logical_not(inward(way)), goes(way)))
        def _(way=way):
            hop(2, way, 0).start()

    gather[1].wait_recv()
    gather[2].start()

    @pl.when(inner)
    def _():
        relay(2, 1)
        relay(2, 2)
        for h in range(2):
            ex_copy(0, False, h).start()

    @pl.when(outer)
    def _():
        relay(0, 3)
        relay(1, 3)

    loads[4].wait()
    for side in range(2):
        cut = slice(side * thin, (side + 1) * thin)
        rd_own[side] = (rd_f32[:, cut] * rscale_ref[:, cut]).astype(jnp.bfloat16)

    @pl.when(outer)
    def _():
        ex_all[:, small:] = jnp.zeros((width, big - small), jnp.bfloat16)
        for slot in range(4):
            for side in range(2):
                rd_all[slot, side, small:] = jnp.zeros((big - small, thin), jnp.bfloat16)

    def place_own(is_inner):
        first, size = part(is_inner)
        ex_all[columns(f), :size] = ex_own[:, first : first + size]
        for side in range(2):
            rd_all[f, side, :size] = rd_own[side, first : first + size]

    both(place_own)

    def project(slot):
        return jnp.dot(xg[:, columns(slot)], dv_all[slot], preferred_element_type=jnp.float32)

    gather[0].wait_recv()
    gather[2].wait_recv()
    act[...] = project(f)

    def project_more(d):
        for i in range(2):
            over_wait(i, d)
        for way in range(2):

            @pl.when(comes(way, d))
            def _(way=way):
                act[...] += project(origin(way, d))

    project_more(1)
    project_more(2)
    project_more(3)

    @pl.when(outer)
    def _():
        ex_copy(1, True).start()
        ex_copy(2, False).start()
        relay(2, 1)
        relay(2, 2)

    @pl.when(inner)
    def _():
        ex_copy(2, True).start()
        ex_copy(1, False).start()

    dvscale = jnp.concatenate([dscale_ref[...], vscale_ref[...]], axis=1)
    act[...] = jax.nn.gelu(act[...] * dvscale)

    lane = lax.broadcasted_iota(jnp.int32, (rows, rows), 1)
    for n in range(4):
        value = act[n * rows : (n + 1) * rows, local:]
        total = jnp.sum(value, axis=1, keepdims=True)
        squares = jnp.sum(value * value, axis=1, keepdims=True)
        table = jnp.where(lane == 0, total, jnp.where(lane == 1, squares, 0.0))
        stat[t, n] = jnp.transpose(table)[:8]
    stats = [
        rcopy(stat.at[t], stat.at[t], tsend.at[0], trecv.at[0], sib),
        rcopy(stat.at[t], stat.at[t], tsend.at[1], trecv.at[1], ynb),
        rcopy(
            stat.at[(1 - y) * 2 + c], stat.at[(1 - y) * 2 + c], tsend.at[2], trecv.at[2], sib
        ),
    ]
    stats[1].start()
    stats[0].start()
    groups = sbias_ref.shape[0]
    down = lax.broadcasted_iota(jnp.int32, (rows, rows), 0)
    bias = jnp.zeros((rows, rows), jnp.float32)
    for n in range(groups):
        bias = jnp.where(down == n, sbias_ref[n : n + 1, :], bias)
    bias = jnp.transpose(bias)
    stats[1].wait_recv()
    stats[2].start()
    stats[0].wait_recv()
    stats[2].wait_recv()

    @pl.when(outer)
    def _():
        relay(2, 3)

    inverse = 1.0 / (local * 4)
    group_lane = lax.broadcasted_iota(jnp.int32, (rows, 128), 1) // GDIM
    for n in range(4):
        here = slice(n * rows, (n + 1) * rows)
        summed = stat[0, n] + stat[1, n] + stat[2, n] + stat[3, n]
        table = jnp.transpose(jnp.concatenate([summed] * (rows // 8), axis=0))
        mean = table[:, 0:1] * inverse
        var = table[:, 1:2] * inverse - mean * mean
        gv = (
            (act[here, local:] - mean) * lax.rsqrt(var + epsilon) * vgain_ref[...]
            + vshift_ref[...]
        ).astype(jnp.bfloat16)
        per = 128 // GDIM
        for j in range(local // 128):
            at = slice(j * 128, (j + 1) * 128)
            mixed = jnp.dot(sw_ref[j * per], gv[:, at], preferred_element_type=jnp.float32)
            mixed = mixed + bias[:, j * per : j * per + 1]
            for k in range(1, per):
                n_group = j * per + k
                other = jnp.dot(sw_ref[n_group], gv[:, at], preferred_element_type=jnp.float32)
                other = other + bias[:, n_group : n_group + 1]
                mixed = jnp.where(group_lane == k, other, mixed)
            gated[here, at] = (act[here, at] * mixed).astype(jnp.bfloat16)

    closer, farther = jnp.where(inner, 2, 1), jnp.where(inner, 1, 2)
    second_slot = jnp.where(inner, peers[2], peers[1])
    last_slot = jnp.where(inner, peers[1], peers[2])
    merge_order = (f, mate, second_slot, last_slot)

    def merge_pair(k):
        return rcopy(
            p1.at[k, block((1 - c) * 2, 2)], r1.at[k], msend.at[k, 0], mrecv.at[k, 0], sib
        )

    def merge_far(k):
        return rcopy(s1.at[k], x1.at[k], msend.at[k, 1], mrecv.at[k, 1], ynb)

    def merge_send(k):
        merge_pair(k).wait_recv()
        s1[k] = (
            p1[k, block(c * 2 + 1 - y)].astype(jnp.float32)
            + r1[k, block(1 - y)].astype(jnp.float32)
        ).astype(jnp.bfloat16)
        merge_far(k).start()

    for k, slot in enumerate(merge_order):
        if k == 1:
            over_wait(2, 1)
        if k == 2:

            @pl.when(outer)
            def _():
                over_wait(2, 2)

        if k == 3:

            @pl.when(inner)
            def _():
                over_wait(2, 2)

            over_wait(2, 3)
        p1[k] = jnp.dot(gated[...], mg_all[slot], preferred_element_type=jnp.float32).astype(
            jnp.bfloat16
        )
        merge_pair(k).start()
        if k > 0:
            merge_send(k - 1)
    merge_send(3)
    for k, slot in enumerate(merge_order):
        merge_far(k).wait_recv()
        mid[:, columns(slot)] = (
            tok_ref[:, columns(slot)].astype(jnp.float32)
            + p1[k, block(c * 2 + y)].astype(jnp.float32)
            + r1[k, block(y)].astype(jnp.float32)
            + x1[k].astype(jnp.float32)
        ).astype(jnp.bfloat16)

    def group(zz, rr, yy):
        return zz * 4 + rr * 2 + yy

    def place(zz, rr, yy):
        return nm.at[group(zz, rr, yy), c]

    mine = place(z, r, y)
    mine[...] = norm(mid[...].astype(jnp.float32), cgain_ref[...])
    over_fs = rcopy(mine, mine, nsend.at[20], nrecv.at[20], znb)

    def spreading(b, zz):
        here, from_x = place(zz, r, y), place(zz, 1 - r, y)
        from_y, from_xy = place(zz, r, 1 - y), place(zz, 1 - r, 1 - y)

        def low(ref):
            return ref.at[pl.ds(0, half)]

        def high(ref):
            return ref.at[pl.ds(half, half)]

        routes = (
            (low(here), xnb), (high(here), xnb), (high(here), ynb), (low(here), ynb), (here, sib),
            (low(from_x), ynb), (high(from_y), xnb),
            (from_x, sib), (from_y, sib), (from_xy, sib),
        )
        return tuple(
            rcopy(ref, ref, nsend.at[10 * b + k], nrecv.at[10 * b + k], dev)
            for k, (ref, dev) in enumerate(routes)
        )

    near, away = spreading(0, z), spreading(1, 1 - z)

    def first(spread):
        for k in (0, 2, 1, 3, 4):
            spread[k].start()

    def second(spread):
        spread[0].wait_recv()
        spread[5].start()
        spread[2].wait_recv()
        spread[6].start()

    def third(spread):
        spread[1].wait_recv()
        spread[7].start()
        spread[3].wait_recv()
        spread[8].start()

    def fourth(spread):
        spread[5].wait_recv()
        spread[6].wait_recv()
        spread[9].start()

    def gathered(spread):
        for k in (4, 7, 8, 9):
            spread[k].wait_recv()

    over_fs.start()
    first(near)

    @pl.when(outer)
    def _():
        for side in range(2):
            rd_copy(side, 0, True).start()
        for side in range(2):
            rd_copy(side, 2, False).start()
            rd_copy(side, 1, True).start()

    @pl.when(inner)
    def _():
        for side in range(2):
            rd_copy(side, 0, False).start()
            rd_copy(side, 2, True).start()
            rd_copy(side, 1, False).start()

    second(near)
    third(near)
    over_fs.wait_recv()
    first(away)
    fourth(near)

    tall = 2 * rows
    start = pl.multiple_of(r * wide, wide)
    exscale = jnp.where(
        inner,
        exscale_ref[:, pl.ds(start, big)],
        jnp.concatenate(
            [
                exscale_ref[:, pl.ds(pl.multiple_of(start + big, 2 * GDIM), small)],
                jnp.zeros((1, big - small), jnp.float32),
            ],
            axis=1,
        ),
    )

    def expand(count, group_of):
        def step(i, _):
            g = group_of(i)
            upper = jnp.dot(
                nm[g].reshape(tall, width), ex_all[...], preferred_element_type=jnp.float32
            ) * exscale
            hid[g] = jnp.square(jax.nn.relu(upper)).astype(jnp.bfloat16)

        lax.fori_loop(0, count, step, None)

    def pick(if_inner, if_outer):
        return jnp.where(inner, if_inner, if_outer)

    slots = (f, f, mate, mate, last_slot, last_slot, second_slot, second_slot)
    sides = (0, 1) * 4
    came = (None, None, 0, 0) + (pick(1, 2),) * 2 + (pick(2, 1),) * 2
    near_half, far_half = 0, 1
    units = ((0, 0), (1, 0), (2, 0), (0, 1), (1, 1), (2, 1))
    units += tuple((k, h) for k in range(3, 8) for h in range(2))

    def plane(h):
        return z if h == near_half else 1 - z

    def arrived(side, j):
        both(lambda is_inner: rd_copy(side, 0, is_inner, j).wait_recv())

    def reduce(u):
        k, h = units[u]
        slot, side = slots[k], sides[k]
        if h == near_half and k > 1:
            arrived(side, came[k])
        zz = plane(h)

        def step(i, _):
            g = zz * 4 + i * 2
            p2[k, pl.ds(g, 2)] = (
                jnp.dot(
                    hid[pl.ds(g, 2)].reshape(2 * tall, big), rd_all[slot, side],
                    preferred_element_type=jnp.float32,
                )
                .astype(jnp.bfloat16)
                .reshape(2, 2, rows, thin)
            )

        lax.fori_loop(0, 2, step, None)
        pair(u).start()

    def pair(u):
        k, h = units[u]
        at = pl.ds(plane(h) * 4, 4)
        return rcopy(p2.at[k, at, 1 - c], r2.at[k, at], fsend.at[0, u], frecv.at[0, u], sib)

    def summed_pair(k, g):
        return p2[k, g, c].astype(jnp.float32) + r2[k, g].astype(jnp.float32)

    def hop_one(u):
        return rcopy(
            f1.at[u], a1.at[u], fsend.at[1, u], frecv.at[1, u], (ynb, xnb)[u % 2]
        )

    def hop_two(u):
        return rcopy(
            f2.at[u], a2.at[u], fsend.at[2, u], frecv.at[2, u], (xnb, ynb)[u % 2]
        )

    def hop_three(k):
        q = slots[k] * 2 + sides[k]
        return rcopy(f3.at[k], a3.at[q], fsend.at[3, k], frecv.at[3, q], znb)

    def send_one(u):
        k, h = units[u]
        zz = plane(h)
        pair(u).wait_recv()
        for n in range(2):
            g = group(zz, n, 1 - y) if u % 2 == 0 else group(zz, 1 - r, n)
            f1[u, n] = summed_pair(k, g).astype(jnp.bfloat16)
        hop_one(u).start()

    def send_two(u):
        k, h = units[u]
        zz = plane(h)
        hop_one(u).wait_recv()
        g, n = (group(zz, 1 - r, y), 1 - r) if u % 2 == 0 else (group(zz, r, 1 - y), 1 - y)
        f2[u] = (summed_pair(k, g) + a1[u, n].astype(jnp.float32)).astype(jnp.bfloat16)
        hop_two(u).start()

    def own_sum(u):
        k, h = units[u]
        n = r if u % 2 == 0 else y
        hop_two(u).wait_recv()
        return (
            summed_pair(k, group(plane(h), r, y))
            + a1[u, n].astype(jnp.float32)
            + a2[u].astype(jnp.float32)
        )

    def send_three(u):
        k, h = units[u]
        if h == far_half:
            f3[k] = own_sum(u).astype(jnp.bfloat16)
            hop_three(k).start()

    def ex_arrived(is_inner):
        for copy in ex_copies((is_inner,) * 3):
            copy.wait_recv()

    done = set()

    def once(action, u):
        if 0 <= u < len(units) and (action, u) not in done:
            done.add((action, u))
            action(u)

    gathered(near)
    both(ex_arrived)
    expand(4, lambda i: z * 4 + i)
    second(away)
    away[4].wait_recv()
    expand(1, lambda i: group(1 - z, r, y) + i)
    once(reduce, 0)
    once(reduce, 1)
    third(away)
    once(send_one, 0)
    once(send_one, 1)
    once(reduce, 2)
    away[7].wait_recv()
    away[8].wait_recv()
    expand(2, lambda i: jnp.where(i == 0, group(1 - z, 1 - r, y), group(1 - z, r, 1 - y)))
    once(send_one, 2)
    fourth(away)
    away[9].wait_recv()
    expand(1, lambda i: group(1 - z, 1 - r, 1 - y) + i)
    for u in range(3, len(units) + 8):
        if u == 14:
            once(send_one, 13)
            for n in range(10, 14):
                once(send_two, n)
        once(reduce, u)
        once(send_one, u - 1)
        once(send_two, u - 4)
        once(send_three, u - 8)
    for k, (slot, side) in enumerate(zip(slots, sides)):
        at = span(slot * piece + side * thin, thin)
        near_sum = own_sum(units.index((k, near_half)))
        hop_three(k).wait_recv()
        q = slot * 2 + side
        out_ref[:, at] = (
            mid[:, at].astype(jnp.float32) + near_sum + a3[q].astype(jnp.float32)
        ).astype(jnp.bfloat16)

    for i in range(3):
        for way in range(2):
            for d in range(3):

                @pl.when(jnp.logical_and(comes(way, d), goes(way)))
                def _(i=i, way=way, d=d):
                    hop(i, way, d).wait_send()

                @pl.when(comes(way, d + 1))
                def _(i=i, way=way, d=d):
                    over(i, way, d + 1).wait_send()

    def own_sends(is_inner):
        to_inner = (not is_inner, not is_inner, is_inner)
        for copy in ex_copies(to_inner):
            copy.wait_send()
        for side in range(2):
            for j in range(3):
                rd_copy(side, j, to_inner[j]).wait_send()

    both(own_sends)
    for copy in gather + tuple(stats) + near + away + (over_fs,):
        copy.wait_send()
    for k in range(4):
        merge_pair(k).wait_send()
        merge_far(k).wait_send()
    for u in range(len(units)):
        pair(u).wait_send()
        hop_one(u).wait_send()
        hop_two(u).wait_send()
    for k in range(len(slots)):
        hop_three(k).wait_send()


def fused_body(
    tokens,
    mixer_gain,
    direct_weight,
    direct_scale,
    value_weight,
    value_scale,
    value_gain,
    value_shift,
    spatial_weight,
    spatial_bias,
    merge_weight,
    merge_scale,
    channel_gain,
    expand_weight,
    expand_scale,
    reduce_weight,
    reduce_scale,
):
    bf = jnp.bfloat16
    rows, width = tokens.shape
    piece, local = direct_weight.shape
    wide = expand_weight.shape[1] // 2
    big = wide * 5 // 8
    thin = piece // 2
    seq = 4 * rows
    vm = pltpu.VMEM
    dma = pltpu.SemaphoreType.DMA
    f32 = jnp.float32
    small = (
        tokens, mixer_gain[None], direct_scale[None], value_scale[None], value_gain[None],
        value_shift[None], spatial_weight, spatial_bias, merge_scale[None], channel_gain[None],
        expand_scale[None], reduce_scale[None],
    )
    large = (direct_weight, value_weight, merge_weight, expand_weight, reduce_weight)
    return pl.pallas_call(
        fused_kernel,
        out_shape=jax.ShapeDtypeStruct((rows, width), bf),
        in_specs=[pl.BlockSpec(memory_space=pltpu.VMEM)] * len(small)
        + [pl.BlockSpec(memory_space=pl.ANY)] * len(large),
        out_specs=pl.BlockSpec(memory_space=pltpu.VMEM),
        scratch_shapes=[
            vm((2, piece, local), f32),
            vm((local, piece), f32),
            vm((piece, wide), f32),
            vm((wide, piece), f32),
            vm((4, piece, 2 * local), bf),
            vm((4, local, piece), bf),
            vm((4 * piece, big), bf),
            vm((piece, wide), bf),
            vm((4, 2, big, thin), bf),
            vm((2, wide, thin), bf),
            vm((seq, width), bf),
            vm((seq, 2 * local), f32),
            vm((4, 4, 8, rows), f32),
            vm((seq, local), bf),
            vm((4, seq, piece), bf),
            vm((4, 2 * rows, piece), bf),
            vm((4, rows, piece), bf),
            vm((4, rows, piece), bf),
            vm((rows, width), bf),
            vm((8, 2, rows, width), bf),
            vm((8, 2 * rows, big), bf),
            vm((8, 8, 2, rows, thin), bf),
            vm((8, 8, rows, thin), bf),
            vm((16, 2, rows, thin), bf),
            vm((16, 2, rows, thin), bf),
            vm((16, rows, thin), bf),
            vm((16, rows, thin), bf),
            vm((8, rows, thin), bf),
            vm((8, rows, thin), bf),
            dma((5,)),
            dma((3, 2, 3)), dma((3, 2, 3)),
            dma((3, 2, 3)), dma((3, 2, 3)),
            dma((10,)), dma((10,)),
            dma((3,)), dma((3,)),
            dma((3,)), dma((3,)),
            dma((4, 2)), dma((4, 2)),
            dma((21,)), dma((21,)),
            dma((4, 16)), dma((4, 16)),
        ],
        compiler_params=pltpu.CompilerParams(
            collective_id=0, has_side_effects=True, vmem_limit_bytes=62 * 1024 * 1024
        ),
    )(*small, *large)


def solution(mesh):
    sizes = mesh.shape
    fused = sizes["rep"] == 2 and sizes["fs"] == 4 and sizes["tp"] == 4
    return jax.shard_map(
        fused_body if fused else body,
        mesh=mesh,
        in_specs=(
            P(("rep", "fs", "tp"), None),
            P(),
            P("fs", "tp"),
            P("tp"),
            P("fs", "tp"),
            P("tp"),
            P("tp"),
            P("tp"),
            P("tp", None, None),
            P("tp", None),
            P("tp", "fs"),
            P("fs"),
            P(),
            P("fs", "tp"),
            P("tp"),
            P("tp", "fs"),
            P("fs"),
        ),
        out_specs=P(("rep", "fs", "tp"), None),
        check_vma=False,
    )
```

```python
import jax
import jax.numpy as jnp
from jax import lax
from jax.experimental import pallas as pl
from jax.experimental.pallas import tpu as pltpu
from jax.sharding import PartitionSpec as P

GDIM = 64
BLOCK = 128


epsilon = 1e-06


def rms_rows(rows, gain):
    floats = rows.astype(jnp.float32)
    scaled = floats * lax.rsqrt(jnp.mean(floats * floats, axis=-1, keepdims=True) + epsilon)
    return (scaled * gain).astype(jnp.bfloat16)


def body(
    tokens,
    mixer_gain,
    direct_weight,
    direct_scale,
    value_weight,
    value_scale,
    value_gain,
    value_shift,
    spatial_weight,
    spatial_bias,
    merge_weight,
    merge_scale,
    channel_gain,
    expand_weight,
    expand_scale,
    reduce_weight,
    reduce_scale,
):
    direct_half = direct_weight.astype(jnp.bfloat16)
    value_half = value_weight.astype(jnp.bfloat16)
    merge_half = merge_weight.astype(jnp.bfloat16)
    expand_half = expand_weight.astype(jnp.bfloat16)
    reduce_half = reduce_weight.astype(jnp.bfloat16)
    full_expand, full_reduce, reduce_full_scale = (
        lax.all_gather(expand_half, "fs", axis=0, tiled=True),
        lax.all_gather(reduce_half, "fs", axis=1, tiled=True),
        lax.all_gather(reduce_scale.astype(jnp.bfloat16), "fs", axis=0, tiled=True).astype(
            reduce_scale.dtype
        ),
    )
    normed = rms_rows(tokens, mixer_gain)
    whole = lax.all_gather(normed, "tp", axis=0, tiled=True)
    seq_rows = whole.shape[0]
    local_width = direct_weight.shape[1]
    direct_pre = jnp.dot(
        whole,
        lax.all_gather(direct_half, "fs", axis=0, tiled=True),
        preferred_element_type=jnp.float32,
    )
    value_pre = jnp.dot(
        whole,
        lax.all_gather(value_half, "fs", axis=0, tiled=True),
        preferred_element_type=jnp.float32,
    )
    full_merge, merge_full_scale = (
        lax.all_gather(merge_half, "fs", axis=1, tiled=True),
        lax.all_gather(merge_scale.astype(jnp.bfloat16), "fs", axis=0, tiled=True).astype(
            merge_scale.dtype
        ),
    )
    direct = jax.nn.gelu(direct_pre * direct_scale)
    value = jax.nn.gelu(value_pre * value_scale)
    total, squares = lax.psum((jnp.sum(value, axis=1), jnp.sum(value * value, axis=1)), "tp")
    branch_width = local_width * lax.axis_size("tp")
    mean = (total / branch_width)[:, None]
    var = (squares / branch_width)[:, None] - mean * mean
    gated_value = ((value - mean) * lax.rsqrt(var + epsilon) * value_gain + value_shift).astype(
        jnp.bfloat16
    )
    local_groups = spatial_weight.shape[0]
    blocks = gated_value.reshape(seq_rows // BLOCK, BLOCK, local_groups, GDIM)
    mixed = jnp.einsum("gpq,nqgc->npgc", spatial_weight, blocks, preferred_element_type=jnp.float32)
    mixed = mixed + jnp.transpose(spatial_bias)[None, :, :, None]
    gated = (direct * mixed.reshape(seq_rows, local_width)).astype(jnp.bfloat16)
    rows = gated
    mix = lax.psum_scatter(
        (jnp.dot(rows, full_merge, preferred_element_type=jnp.float32) * merge_full_scale).astype(
            jnp.bfloat16
        ),
        "tp",
        scatter_dimension=0,
        tiled=True,
    ).astype(jnp.float32)
    middle = (tokens.astype(jnp.float32) + mix).astype(jnp.bfloat16)
    normed_mid = rms_rows(middle, channel_gain)
    whole_mid = lax.all_gather(normed_mid, "tp", axis=0, tiled=True)
    upper = jnp.dot(whole_mid, full_expand, preferred_element_type=jnp.float32)
    hidden = jnp.square(jax.nn.relu(upper * expand_scale)).astype(jnp.bfloat16)
    rows = hidden
    lower = lax.psum_scatter(
        (jnp.dot(rows, full_reduce, preferred_element_type=jnp.float32) * reduce_full_scale).astype(
            jnp.bfloat16
        ),
        "tp",
        scatter_dimension=0,
        tiled=True,
    ).astype(jnp.float32)
    return (middle.astype(jnp.float32) + lower).astype(jnp.bfloat16)


MESH = pl.DeviceIdType.MESH


def fused_kernel(
    tok_hbm, mgain_hbm, dscale_hbm, vscale_hbm, vgain_hbm, vshift_hbm, sw_hbm, sbias_hbm,
    mscale_hbm, cgain_hbm, exscale_hbm, rscale_hbm,
    dw_ref, vw_ref, mw_ref, ew_ref, rw_ref,
    out_ref,
    tok_ref, mgain_ref, dscale_ref, vscale_ref, vgain_ref, vshift_ref, sw_ref, sbias_ref,
    mscale_ref, cgain_ref, exscale_ref, rscale_ref,
    dv_f32, mg_f32, ex_f32, rd_f32,
    dv_all, mg_all, ex_all, ex_own, rd_all, rd_own,
    xg, act, stat, gated, p1, r1, s1, x1, mid,
    nm, hid, p2, r2, f1, a1, f2, a2, f3, a3, result,
    load_sem, out_sem, wsend, wrecv, xsend, xrecv, csend, crecv, gsend, grecv, trecv, msend, mrecv,
    nsend, nrecv, fsend, frecv,
):
    rows, width = tok_ref.shape
    piece, local = dw_ref.shape
    big = hid.shape[2]
    wide = ex_own.shape[1]
    small = wide - big
    half = rows // 2
    thin = piece // 2
    r = lax.axis_index("rep")
    f = lax.axis_index("fs")
    t = lax.axis_index("tp")
    y, c = t // 2, t % 2
    z = f % 2
    mate = f + 1 - 2 * z
    peers = (mate, (f + 2) % 4, (mate + 2) % 4)
    sib = {"tp": y * 2 + (1 - c)}
    ynb = {"tp": (1 - y) * 2 + c}
    xnb = {"rep": 1 - r}
    znb = {"fs": mate}

    barrier = pltpu.get_barrier_semaphore()
    for dev in (sib, ynb, xnb) + tuple({"fs": peer} for peer in peers):
        pl.semaphore_signal(barrier, inc=1, device_id=dev, device_id_type=MESH)

    def span(start, size):
        return pl.ds(pl.multiple_of(start, size), size)

    loads = [
        pltpu.make_async_copy(source, target, load_sem.at[i])
        for i, (source, target) in enumerate(
            (
                (dw_ref, dv_f32.at[0]),
                (vw_ref, dv_f32.at[1]),
                (tok_hbm, tok_ref),
                (mgain_hbm, mgain_ref),
                (mscale_hbm, mscale_ref),
                (mw_ref, mg_f32),
                (ew_ref.at[:, span(r * wide, wide)], ex_f32),
                (rscale_hbm, rscale_ref),
                (rw_ref.at[span(r * wide, wide)], rd_f32),
                (dscale_hbm, dscale_ref),
                (vscale_hbm, vscale_ref),
                (vgain_hbm, vgain_ref),
                (vshift_hbm, vshift_ref),
                (sw_hbm, sw_ref),
                (sbias_hbm, sbias_ref),
                (cgain_hbm, cgain_ref),
                (exscale_hbm, exscale_ref),
            )
        )
    ]
    for load in loads:
        load.start()

    def rcopy(src, dst, ssem, rsem, dev):
        return pltpu.make_async_remote_copy(
            src_ref=src, dst_ref=dst, send_sem=ssem, recv_sem=rsem,
            device_id=dev, device_id_type=MESH,
        )

    def item(i, slot, q):
        if i < 2:
            return dv_all.at[slot, span(q * 2 * rows + i * rows, rows)]
        return mg_all.at[slot, span(q * rows, rows)]

    def origin(way, d):
        return lax.rem(f + (4 - d if way == 0 else d), 4)

    def comes(way, d):
        return f >= d if way == 0 else f + d <= 3

    def goes(way):
        return f < 3 if way == 0 else f > 0

    def inward(way):
        return f < 2 if way == 0 else f >= 2

    def hop(i, way, d):
        ref = item(i, origin(way, d), r)
        to = lax.rem(f + (1 if way == 0 else 3), 4)
        return rcopy(
            ref, ref, wsend.at[min(d, 1)], wrecv.at[i, origin(way, d)], {"fs": to}
        )

    def over(i, way, d):
        slot = origin(way, d)
        ref = item(i, slot, r)
        return rcopy(ref, ref, xsend.at[i // 2], xrecv.at[i, slot], xnb)

    def relay(i, d):
        for way in range(2):

            @pl.when(comes(way, d))
            def _(way=way):
                hop(i, way, d).wait_recv()
                over(i, way, d).start()

            if d < 3:

                @pl.when(jnp.logical_and(comes(way, d), goes(way)))
                def _(way=way):
                    hop(i, way, d).start()

    def over_wait(i, d):
        for way in range(2):

            @pl.when(comes(way, d))
            def _(way=way):
                over(i, way, d).wait_recv()

    inner = jnp.logical_or(f == 1, f == 2)
    outer = jnp.logical_not(inner)

    def part(to_inner):
        return (0, big) if to_inner else (big, small)

    cuts = ((0, thin // 2), (thin // 2, thin // 2), (thin, thin))

    def ex_copy(j, to_inner, h):
        first, size = part(to_inner)
        start, count = cuts[h]
        return rcopy(
            ex_own.at[pl.ds(start, count), pl.ds(first, size)],
            ex_all.at[span(f * piece + start, count), pl.ds(0, size)],
            csend.at[int(to_inner)], crecv.at[0], {"fs": peers[j]},
        )

    def ex_start(j, to_inner, which=(0, 1, 2)):
        for h in which:
            ex_copy(j, to_inner, h).start()

    def rd_copy(side, j, to_inner, index=None):
        first, size = part(to_inner)
        n = 1 + side * 3 + (j if index is None else index)
        return rcopy(
            rd_own.at[side, pl.ds(first, size)], rd_all.at[f, side, pl.ds(0, size)],
            csend.at[2 + int(to_inner)], crecv.at[n], {"fs": peers[j]},
        )

    def both(action):
        @pl.when(inner)
        def _():
            action(True)

        @pl.when(outer)
        def _():
            action(False)

    def norm(x, gain):
        return (
            x * lax.rsqrt(jnp.mean(x * x, axis=-1, keepdims=True) + epsilon) * gain
        ).astype(jnp.bfloat16)

    def block(n, size=1):
        return pl.ds(pl.multiple_of(n * rows, rows), size * rows)

    def columns(slot):
        return span(slot * piece, piece)

    for i in range(2):
        loads[i].wait()
        dv_all[f, :, i * local : (i + 1) * local] = dv_f32[i].astype(jnp.bfloat16)
    for i in range(2, 4):
        loads[i].wait()
    mine = xg.at[block(c * 2 + y)]
    mine[...] = norm(tok_ref[...].astype(jnp.float32), mgain_ref[...])
    far = xg.at[block(c * 2 + 1 - y)]
    gather = (
        rcopy(mine, mine, gsend.at[0], grecv.at[0], sib),
        rcopy(mine, mine, gsend.at[0], grecv.at[1], ynb),
        rcopy(far, far, gsend.at[0], grecv.at[2], sib),
    )
    pl.semaphore_wait(barrier, 6)
    for i in range(2):
        for way in range(2):

            @pl.when(goes(way))
            def _(i=i, way=way):
                hop(i, way, 0).start()

    gather[1].start()
    gather[0].start()
    for i in range(4, 6):
        loads[i].wait()
    mg_all[f] = (mg_f32[...] * mscale_ref[...]).astype(jnp.bfloat16)
    loads[6].wait()
    ex_own[...] = ex_f32[...].astype(jnp.bfloat16)

    relay(0, 1)
    relay(1, 1)
    for way in range(2):

        @pl.when(inward(way))
        def _(way=way):
            hop(2, way, 0).start()

    @pl.when(outer)
    def _():
        ex_start(0, True)

    relay(0, 2)
    relay(1, 2)
    for way in range(2):

        @pl.when(jnp.logical_and(jnp.logical_not(inward(way)), goes(way)))
        def _(way=way):
            hop(2, way, 0).start()

    gather[1].wait_recv()
    gather[2].start()

    @pl.when(inner)
    def _():
        relay(2, 1)
        relay(2, 2)
        ex_start(2, True, (0,))

    @pl.when(outer)
    def _():
        relay(0, 3)
        relay(1, 3)

    for load in loads[7:]:
        load.wait()
    for side in range(2):
        cut = slice(side * thin, (side + 1) * thin)
        rd_own[side] = (rd_f32[:, cut] * rscale_ref[:, cut]).astype(jnp.bfloat16)

    @pl.when(outer)
    def _():
        ex_all[:, small:] = jnp.zeros((width, big - small), jnp.bfloat16)
        for slot in range(4):
            for side in range(2):
                rd_all[slot, side, small:] = jnp.zeros((big - small, thin), jnp.bfloat16)

    def place_own(is_inner):
        first, size = part(is_inner)
        ex_all[columns(f), :size] = ex_own[:, first : first + size]
        for side in range(2):
            rd_all[f, side, :size] = rd_own[side, first : first + size]

    both(place_own)

    def project(slot):
        return jnp.dot(xg[:, columns(slot)], dv_all[slot], preferred_element_type=jnp.float32)

    gather[0].wait_recv()
    gather[2].wait_recv()
    act[...] = project(f)

    def project_more(d):
        for i in range(2):
            over_wait(i, d)
        for way in range(2):

            @pl.when(comes(way, d))
            def _(way=way):
                act[...] += project(origin(way, d))

    project_more(1)
    project_more(2)
    project_more(3)

    @pl.when(outer)
    def _():
        ex_start(1, True, (0, 1))
        relay(2, 1)
        relay(2, 2)

    dvscale = jnp.concatenate([dscale_ref[...], vscale_ref[...]], axis=1)
    act[...] = jax.nn.gelu(act[...] * dvscale)

    lane = lax.broadcasted_iota(jnp.int32, (rows, rows), 1)
    for n in range(4):
        value = act[n * rows : (n + 1) * rows, local:]
        total = jnp.sum(value, axis=1, keepdims=True)
        squares = jnp.sum(value * value, axis=1, keepdims=True)
        table = jnp.where(lane == 0, total, jnp.where(lane == 1, squares, 0.0))
        stat[t, n] = jnp.transpose(table)[:8]
    stats = [
        rcopy(stat.at[t], stat.at[t], gsend.at[1], trecv.at[0], sib),
        rcopy(stat.at[t], stat.at[t], gsend.at[1], trecv.at[1], ynb),
        rcopy(
            stat.at[(1 - y) * 2 + c], stat.at[(1 - y) * 2 + c], gsend.at[1], trecv.at[2], sib
        ),
    ]
    stats[1].start()
    stats[0].start()
    groups = sbias_ref.shape[0]
    down = lax.broadcasted_iota(jnp.int32, (rows, rows), 0)
    bias = jnp.zeros((rows, rows), jnp.float32)
    for n in range(groups):
        bias = jnp.where(down == n, sbias_ref[n : n + 1, :], bias)
    bias = jnp.transpose(bias)
    stats[1].wait_recv()
    stats[2].start()
    stats[0].wait_recv()
    stats[2].wait_recv()

    @pl.when(inner)
    def _():
        ex_start(1, False)
        ex_start(2, True, (1, 2))

    @pl.when(outer)
    def _():
        ex_start(2, False)
        relay(2, 3)

    inverse = 1.0 / (local * 4)
    group_lane = lax.broadcasted_iota(jnp.int32, (rows, 128), 1) // GDIM
    for n in range(4):
        here = slice(n * rows, (n + 1) * rows)
        summed = stat[0, n] + stat[1, n] + stat[2, n] + stat[3, n]
        table = jnp.transpose(jnp.concatenate([summed] * (rows // 8), axis=0))
        mean = table[:, 0:1] * inverse
        var = table[:, 1:2] * inverse - mean * mean
        gv = (
            (act[here, local:] - mean) * lax.rsqrt(var + epsilon) * vgain_ref[...]
            + vshift_ref[...]
        ).astype(jnp.bfloat16)
        per = 128 // GDIM
        for j in range(local // 128):
            at = slice(j * 128, (j + 1) * 128)
            mixed = jnp.dot(sw_ref[j * per], gv[:, at], preferred_element_type=jnp.float32)
            mixed = mixed + bias[:, j * per : j * per + 1]
            for k in range(1, per):
                n_group = j * per + k
                other = jnp.dot(sw_ref[n_group], gv[:, at], preferred_element_type=jnp.float32)
                other = other + bias[:, n_group : n_group + 1]
                mixed = jnp.where(group_lane == k, other, mixed)
            gated[here, at] = (act[here, at] * mixed).astype(jnp.bfloat16)

    closer, farther = jnp.where(inner, 2, 1), jnp.where(inner, 1, 2)
    second_slot = jnp.where(inner, peers[2], peers[1])
    last_slot = jnp.where(inner, peers[1], peers[2])
    merge_order = (f, mate, second_slot, last_slot)

    def merge_pair(k):
        return rcopy(
            p1.at[k, block((1 - c) * 2, 2)], r1.at[k], msend.at[0], mrecv.at[k, 0], sib
        )

    def merge_far(k):
        return rcopy(s1.at[k], x1.at[k], msend.at[1], mrecv.at[k, 1], ynb)

    def merge_send(k):
        merge_pair(k).wait_recv()
        s1[k] = (
            p1[k, block(c * 2 + 1 - y)].astype(jnp.float32)
            + r1[k, block(1 - y)].astype(jnp.float32)
        ).astype(jnp.bfloat16)
        merge_far(k).start()

    for k, slot in enumerate(merge_order):
        if k == 1:
            over_wait(2, 1)
        if k == 2:

            @pl.when(outer)
            def _():
                over_wait(2, 2)

        if k == 3:

            @pl.when(inner)
            def _():
                over_wait(2, 2)

            over_wait(2, 3)
        p1[k] = jnp.dot(gated[...], mg_all[slot], preferred_element_type=jnp.float32).astype(
            jnp.bfloat16
        )
        merge_pair(k).start()
        if k > 0:
            merge_send(k - 1)
    merge_send(3)
    for k, slot in enumerate(merge_order):
        merge_far(k).wait_recv()
        mid[:, columns(slot)] = (
            tok_ref[:, columns(slot)].astype(jnp.float32)
            + p1[k, block(c * 2 + y)].astype(jnp.float32)
            + r1[k, block(y)].astype(jnp.float32)
            + x1[k].astype(jnp.float32)
        ).astype(jnp.bfloat16)

    def group(zz, rr, yy):
        return zz * 4 + rr * 2 + yy

    def place(zz, rr, yy):
        return nm.at[group(zz, rr, yy), c]

    mine = place(z, r, y)
    mine[...] = norm(mid[...].astype(jnp.float32), cgain_ref[...])
    over_fs = rcopy(mine, mine, nsend.at[1], nrecv.at[20], znb)

    def spreading(b, zz):
        here, from_x = place(zz, r, y), place(zz, 1 - r, y)
        from_y, from_xy = place(zz, r, 1 - y), place(zz, 1 - r, 1 - y)

        def low(ref):
            return ref.at[pl.ds(0, half)]

        def high(ref):
            return ref.at[pl.ds(half, half)]

        routes = (
            (low(here), xnb), (high(here), xnb), (high(here), ynb), (low(here), ynb), (here, sib),
            (low(from_x), ynb), (high(from_y), xnb),
            (from_x, sib), (from_y, sib), (from_xy, sib),
        )
        return tuple(
            rcopy(ref, ref, nsend.at[0], nrecv.at[10 * b + k], dev)
            for k, (ref, dev) in enumerate(routes)
        )

    near, away = spreading(0, z), spreading(1, 1 - z)

    def first(spread):
        for k in (0, 2, 1, 3, 4):
            spread[k].start()

    def second(spread):
        spread[0].wait_recv()
        spread[5].start()
        spread[2].wait_recv()
        spread[6].start()

    def third(spread):
        spread[1].wait_recv()
        spread[7].start()
        spread[3].wait_recv()
        spread[8].start()

    def fourth(spread):
        spread[5].wait_recv()
        spread[6].wait_recv()
        spread[9].start()

    def gathered(spread):
        for k in (4, 7, 8, 9):
            spread[k].wait_recv()

    over_fs.start()

    @pl.when(outer)
    def _():
        ex_start(1, True, (2,))

    first(near)

    second(near)

    @pl.when(inner)
    def _():
        ex_start(0, False)

    third(near)
    over_fs.wait_recv()
    first(away)

    def rd_start(side, j, to_inner):
        rd_copy(side, j, to_inner).start()

    @pl.when(inner)
    def _():
        for side in range(2):
            rd_start(side, 0, False)
        for side in range(2):
            rd_start(side, 2, True)
            rd_start(side, 1, False)

    @pl.when(outer)
    def _():
        for side in range(2):
            rd_start(side, 0, True)

    fourth(near)

    tall = 2 * rows
    start = pl.multiple_of(r * wide, wide)
    exscale = jnp.where(
        inner,
        exscale_ref[:, pl.ds(start, big)],
        jnp.concatenate(
            [
                exscale_ref[:, pl.ds(pl.multiple_of(start + big, 2 * GDIM), small)],
                jnp.zeros((1, big - small), jnp.float32),
            ],
            axis=1,
        ),
    )

    def expand(count, group_of):
        def step(i, _):
            g = group_of(i)
            upper = jnp.dot(
                nm[g].reshape(tall, width), ex_all[...], preferred_element_type=jnp.float32
            ) * exscale
            hid[g] = jnp.square(jax.nn.relu(upper)).astype(jnp.bfloat16)

        lax.fori_loop(0, count, step, None)

    def pick(if_inner, if_outer):
        return jnp.where(inner, if_inner, if_outer)

    slots = (f, f, mate, mate, second_slot, last_slot, last_slot, second_slot)
    sides = (0, 1, 0, 1, 0, 0, 1, 1)
    came = (None, None, 0, 0, pick(2, 1), pick(1, 2), pick(1, 2), pick(2, 1))
    near_half, far_half = 0, 1
    units = tuple((k, h) for h in range(2) for k in range(4))
    units += tuple((k, h) for k in range(4, 8) for h in (1, 0))

    def plane(h):
        return z if h == near_half else 1 - z

    def arrived(side, j):
        both(lambda is_inner: rd_copy(side, 0, is_inner, j).wait_recv())

    def reduce(u):
        k, h = units[u]
        slot, side = slots[k], sides[k]
        if k > 1 and h == (near_half if k < 4 else far_half):
            arrived(side, came[k])
        zz = plane(h)

        def step(i, _):
            g = zz * 4 + i * 2
            p2[k, pl.ds(g, 2)] = (
                jnp.dot(
                    hid[pl.ds(g, 2)].reshape(2 * tall, big), rd_all[slot, side],
                    preferred_element_type=jnp.float32,
                )
                .astype(jnp.bfloat16)
                .reshape(2, 2, rows, thin)
            )

        lax.fori_loop(0, 2, step, None)
        pair(u).start()

    def pair(u):
        k, h = units[u]
        at = pl.ds(plane(h) * 4, 4)
        return rcopy(p2.at[k, at, 1 - c], r2.at[k, at], fsend.at[0], frecv.at[0, u], sib)

    def summed_pair(k, g):
        return p2[k, g, c].astype(jnp.float32) + r2[k, g].astype(jnp.float32)

    def hop_one(u):
        return rcopy(
            f1.at[u], a1.at[u], fsend.at[1], frecv.at[1, u], (ynb, xnb)[u % 2]
        )

    def hop_two(u):
        return rcopy(
            f2.at[u], a2.at[u], fsend.at[2], frecv.at[2, u], (xnb, ynb)[u % 2]
        )

    def hop_three(k):
        q = slots[k] * 2 + sides[k]
        return rcopy(f3.at[k], a3.at[q], fsend.at[3], frecv.at[3, q], znb)

    def send_one(u):
        k, h = units[u]
        zz = plane(h)
        pair(u).wait_recv()
        for n in range(2):
            g = group(zz, n, 1 - y) if u % 2 == 0 else group(zz, 1 - r, n)
            f1[u, n] = summed_pair(k, g).astype(jnp.bfloat16)
        hop_one(u).start()

    def send_two(u):
        k, h = units[u]
        zz = plane(h)
        hop_one(u).wait_recv()
        g, n = (group(zz, 1 - r, y), 1 - r) if u % 2 == 0 else (group(zz, r, 1 - y), 1 - y)
        f2[u] = (summed_pair(k, g) + a1[u, n].astype(jnp.float32)).astype(jnp.bfloat16)
        hop_two(u).start()

    def own_sum(u):
        k, h = units[u]
        n = r if u % 2 == 0 else y
        hop_two(u).wait_recv()
        return (
            summed_pair(k, group(plane(h), r, y))
            + a1[u, n].astype(jnp.float32)
            + a2[u].astype(jnp.float32)
        )

    def send_three(u):
        k, h = units[u]
        if h == far_half:
            f3[k] = own_sum(u).astype(jnp.bfloat16)
            hop_three(k).start()

    def ex_arrived(is_inner):
        ref = ex_all.at[pl.ds(0, 3 * piece), pl.ds(0, part(is_inner)[1])]
        rcopy(ref, ref, csend.at[0], crecv.at[0], znb).wait_recv()

    done = set()

    def once(action, u):
        if 0 <= u < len(units) and (action, u) not in done:
            done.add((action, u))
            action(u)

    gathered(near)
    both(ex_arrived)
    expand(4, lambda i: z * 4 + i)
    second(away)
    away[4].wait_recv()
    expand(1, lambda i: group(1 - z, r, y) + i)
    once(reduce, 0)
    once(reduce, 1)
    third(away)
    once(send_one, 0)
    once(send_one, 1)
    once(reduce, 2)
    away[7].wait_recv()
    away[8].wait_recv()
    expand(2, lambda i: jnp.where(i == 0, group(1 - z, 1 - r, y), group(1 - z, r, 1 - y)))
    once(send_one, 2)
    fourth(away)

    @pl.when(outer)
    def _():
        for side in range(2):
            rd_start(side, 2, False)
            rd_start(side, 1, True)

    away[9].wait_recv()
    expand(1, lambda i: group(1 - z, 1 - r, 1 - y) + i)
    turn = (0, 1, 2, 4, 5, 3) + tuple(range(6, len(units)))

    def late(action, n):
        if n >= 0:
            once(action, turn[n])

    for n in range(3, len(turn)):
        if n in (12, 14):
            late(send_one, n - 1)
            late(send_two, n - 4)
            late(send_two, n - 3)
        late(reduce, n)
        late(send_one, n - 1)
        late(send_two, n - 4)
        late(send_three, n - 8)
    once(send_one, 15)
    once(send_two, 12)
    once(send_three, 8)
    once(send_two, 13)
    once(send_three, 10)
    once(send_two, 14)
    once(send_three, 12)
    once(send_two, 15)
    once(send_three, 14)

    def stored(k):
        at = span(slots[k] * piece + sides[k] * thin, thin)
        return pltpu.make_async_copy(result.at[:, at], out_ref.at[:, at], out_sem)

    for k, (slot, side) in enumerate(zip(slots, sides)):
        at = span(slot * piece + side * thin, thin)
        near_sum = own_sum(units.index((k, near_half)))
        hop_three(k).wait_recv()
        q = slot * 2 + side
        result[:, at] = (
            mid[:, at].astype(jnp.float32) + near_sum + a3[q].astype(jnp.float32)
        ).astype(jnp.bfloat16)
        stored(k).start()

    def sent(ref, sem):
        rcopy(ref, ref, sem, crecv.at[0], znb).wait_send()

    def few_sent(is_inner):
        own = rows * (2 if is_inner else 1)
        sent(dv_all.at[pl.ds(0, 3), pl.ds(0, own)], wsend.at[0])
        if is_inner:
            sent(dv_all.at[pl.ds(0, 3), pl.ds(0, 3 * rows)], wsend.at[1])
        for to_inner in (False, True):
            size = part(to_inner)[1]
            count = piece * (1 if to_inner == is_inner else 2)
            for n in (0, 2):
                sent(ex_all.at[pl.ds(0, count), pl.ds(0, size)], csend.at[n + int(to_inner)])

    both(few_sent)
    sent(dv_all.at[pl.ds(0, 3), pl.ds(0, 2 * rows)], xsend.at[0])
    sent(mg_all.at[pl.ds(0, 3), pl.ds(0, rows)], xsend.at[1])
    sent(xg.at[pl.ds(0, 3 * rows)], gsend.at[0])
    sent(stat.at[pl.ds(0, 3)], gsend.at[1])
    sent(r1, msend.at[0])
    sent(s1, msend.at[1])
    sent(nm.at[pl.ds(0, 7)], nsend.at[0])
    over_fs.wait_send()
    for n, ref in enumerate((r2, f1, f2, f3)):
        sent(ref, fsend.at[n])
    pltpu.make_async_copy(result, out_ref, out_sem).wait()


def fused_body(
    tokens,
    mixer_gain,
    direct_weight,
    direct_scale,
    value_weight,
    value_scale,
    value_gain,
    value_shift,
    spatial_weight,
    spatial_bias,
    merge_weight,
    merge_scale,
    channel_gain,
    expand_weight,
    expand_scale,
    reduce_weight,
    reduce_scale,
):
    bf = jnp.bfloat16
    rows, width = tokens.shape
    piece, local = direct_weight.shape
    wide = expand_weight.shape[1] // 2
    big = wide * 5 // 8
    thin = piece // 2
    seq = 4 * rows
    vm = pltpu.VMEM
    dma = pltpu.SemaphoreType.DMA
    f32 = jnp.float32
    small = (
        tokens, mixer_gain[None], direct_scale[None], value_scale[None], value_gain[None],
        value_shift[None], spatial_weight, spatial_bias, merge_scale[None], channel_gain[None],
        expand_scale[None], reduce_scale[None],
    )
    large = (direct_weight, value_weight, merge_weight, expand_weight, reduce_weight)
    return pl.pallas_call(
        fused_kernel,
        out_shape=jax.ShapeDtypeStruct((rows, width), bf),
        in_specs=[pl.BlockSpec(memory_space=pl.ANY)] * len(small + large),
        out_specs=pl.BlockSpec(memory_space=pl.ANY),
        scratch_shapes=[vm(a.shape, a.dtype) for a in small]
        + [
            vm((2, piece, local), f32),
            vm((local, piece), f32),
            vm((piece, wide), f32),
            vm((wide, piece), f32),
            vm((4, piece, 2 * local), bf),
            vm((4, local, piece), bf),
            vm((4 * piece, big), bf),
            vm((piece, wide), bf),
            vm((4, 2, big, thin), bf),
            vm((2, wide, thin), bf),
            vm((seq, width), bf),
            vm((seq, 2 * local), f32),
            vm((4, 4, 8, rows), f32),
            vm((seq, local), bf),
            vm((4, seq, piece), bf),
            vm((4, 2 * rows, piece), bf),
            vm((4, rows, piece), bf),
            vm((4, rows, piece), bf),
            vm((rows, width), bf),
            vm((8, 2, rows, width), bf),
            vm((8, 2 * rows, big), bf),
            vm((8, 8, 2, rows, thin), bf),
            vm((8, 8, rows, thin), bf),
            vm((16, 2, rows, thin), bf),
            vm((16, 2, rows, thin), bf),
            vm((16, rows, thin), bf),
            vm((16, rows, thin), bf),
            vm((8, rows, thin), bf),
            vm((8, rows, thin), bf),
            vm((rows, width), bf),
            dma((17,)), dma,
            dma((2,)), dma((3, 4)),
            dma((2,)), dma((3, 4)),
            dma((4,)), dma((7,)),
            dma((2,)), dma((3,)), dma((3,)),
            dma((2,)), dma((4, 2)),
            dma((2,)), dma((21,)),
            dma((4,)), dma((4, 16)),
        ],
        compiler_params=pltpu.CompilerParams(
            collective_id=0, has_side_effects=True, vmem_limit_bytes=62 * 1024 * 1024
        ),
    )(*small, *large)


def solution(mesh):
    sizes = mesh.shape
    fused = sizes["rep"] == 2 and sizes["fs"] == 4 and sizes["tp"] == 4
    return jax.shard_map(
        fused_body if fused else body,
        mesh=mesh,
        in_specs=(
            P(("rep", "fs", "tp"), None),
            P(),
            P("fs", "tp"),
            P("tp"),
            P("fs", "tp"),
            P("tp"),
            P("tp"),
            P("tp"),
            P("tp", None, None),
            P("tp", None),
            P("tp", "fs"),
            P("fs"),
            P(),
            P("fs", "tp"),
            P("tp"),
            P("tp", "fs"),
            P("fs"),
        ),
        out_specs=P(("rep", "fs", "tp"), None),
        check_vma=False,
    )
```

```python
import jax
import jax.numpy as jnp
from jax import lax
from jax.experimental import pallas as pl
from jax.experimental.pallas import tpu as pltpu
from jax.sharding import PartitionSpec as P

GDIM = 64
BLOCK = 128


epsilon = 1e-06


def rms_rows(rows, gain):
    floats = rows.astype(jnp.float32)
    scaled = floats * lax.rsqrt(jnp.mean(floats * floats, axis=-1, keepdims=True) + epsilon)
    return (scaled * gain).astype(jnp.bfloat16)


def body(
    tokens,
    mixer_gain,
    direct_weight,
    direct_scale,
    value_weight,
    value_scale,
    value_gain,
    value_shift,
    spatial_weight,
    spatial_bias,
    merge_weight,
    merge_scale,
    channel_gain,
    expand_weight,
    expand_scale,
    reduce_weight,
    reduce_scale,
):
    direct_half = direct_weight.astype(jnp.bfloat16)
    value_half = value_weight.astype(jnp.bfloat16)
    merge_half = merge_weight.astype(jnp.bfloat16)
    expand_half = expand_weight.astype(jnp.bfloat16)
    reduce_half = reduce_weight.astype(jnp.bfloat16)
    full_expand, full_reduce, reduce_full_scale = (
        lax.all_gather(expand_half, "fs", axis=0, tiled=True),
        lax.all_gather(reduce_half, "fs", axis=1, tiled=True),
        lax.all_gather(reduce_scale.astype(jnp.bfloat16), "fs", axis=0, tiled=True).astype(
            reduce_scale.dtype
        ),
    )
    normed = rms_rows(tokens, mixer_gain)
    whole = lax.all_gather(normed, "tp", axis=0, tiled=True)
    seq_rows = whole.shape[0]
    local_width = direct_weight.shape[1]
    direct_pre = jnp.dot(
        whole,
        lax.all_gather(direct_half, "fs", axis=0, tiled=True),
        preferred_element_type=jnp.float32,
    )
    value_pre = jnp.dot(
        whole,
        lax.all_gather(value_half, "fs", axis=0, tiled=True),
        preferred_element_type=jnp.float32,
    )
    full_merge, merge_full_scale = (
        lax.all_gather(merge_half, "fs", axis=1, tiled=True),
        lax.all_gather(merge_scale.astype(jnp.bfloat16), "fs", axis=0, tiled=True).astype(
            merge_scale.dtype
        ),
    )
    direct = jax.nn.gelu(direct_pre * direct_scale)
    value = jax.nn.gelu(value_pre * value_scale)
    total, squares = lax.psum((jnp.sum(value, axis=1), jnp.sum(value * value, axis=1)), "tp")
    branch_width = local_width * lax.axis_size("tp")
    mean = (total / branch_width)[:, None]
    var = (squares / branch_width)[:, None] - mean * mean
    gated_value = ((value - mean) * lax.rsqrt(var + epsilon) * value_gain + value_shift).astype(
        jnp.bfloat16
    )
    local_groups = spatial_weight.shape[0]
    blocks = gated_value.reshape(seq_rows // BLOCK, BLOCK, local_groups, GDIM)
    mixed = jnp.einsum("gpq,nqgc->npgc", spatial_weight, blocks, preferred_element_type=jnp.float32)
    mixed = mixed + jnp.transpose(spatial_bias)[None, :, :, None]
    gated = (direct * mixed.reshape(seq_rows, local_width)).astype(jnp.bfloat16)
    rows = gated
    mix = lax.psum_scatter(
        (jnp.dot(rows, full_merge, preferred_element_type=jnp.float32) * merge_full_scale).astype(
            jnp.bfloat16
        ),
        "tp",
        scatter_dimension=0,
        tiled=True,
    ).astype(jnp.float32)
    middle = (tokens.astype(jnp.float32) + mix).astype(jnp.bfloat16)
    normed_mid = rms_rows(middle, channel_gain)
    whole_mid = lax.all_gather(normed_mid, "tp", axis=0, tiled=True)
    upper = jnp.dot(whole_mid, full_expand, preferred_element_type=jnp.float32)
    hidden = jnp.square(jax.nn.relu(upper * expand_scale)).astype(jnp.bfloat16)
    rows = hidden
    lower = lax.psum_scatter(
        (jnp.dot(rows, full_reduce, preferred_element_type=jnp.float32) * reduce_full_scale).astype(
            jnp.bfloat16
        ),
        "tp",
        scatter_dimension=0,
        tiled=True,
    ).astype(jnp.float32)
    return (middle.astype(jnp.float32) + lower).astype(jnp.bfloat16)


MESH = pl.DeviceIdType.MESH


def fused_kernel(
    tok_hbm, mgain_hbm, dscale_hbm, vscale_hbm, vgain_hbm, vshift_hbm, sw_hbm, sbias_hbm,
    mscale_hbm, cgain_hbm, exscale_hbm, rscale_hbm,
    dw_ref, vw_ref, mw_ref, ew_ref, rw_ref,
    out_ref,
    tok_ref, mgain_ref, dscale_ref, vscale_ref, vgain_ref, vshift_ref, sw_ref, sbias_ref,
    mscale_ref, cgain_ref, exscale_ref, rscale_ref,
    dv_f32, mg_f32, ex_f32, rd_f32,
    dv_all, mg_all, ex_all, ex_own, rd_all, rd_own,
    xg, act, stat, gated, p1, r1, s1, x1, mid,
    nm, hid, p2, r2, f1, a1, f2, a2, f3, a3, result,
    load_sem, out_sem, wsend, wrecv, xsend, xrecv, csend, crecv, gsend, grecv, trecv, msend, mrecv,
    nsend, nrecv, fsend, frecv,
):
    rows, width = tok_ref.shape
    piece, local = dw_ref.shape
    big = hid.shape[2]
    wide = ex_own.shape[1]
    small = wide - big
    half = rows // 2
    thin = piece // 2
    r = lax.axis_index("rep")
    f = lax.axis_index("fs")
    t = lax.axis_index("tp")
    y, c = t // 2, t % 2
    z = f % 2
    mate = f + 1 - 2 * z
    peers = (mate, (f + 2) % 4, (mate + 2) % 4)
    sib = {"tp": y * 2 + (1 - c)}
    ynb = {"tp": (1 - y) * 2 + c}
    xnb = {"rep": 1 - r}
    znb = {"fs": mate}

    barrier = pltpu.get_barrier_semaphore()
    for dev in (sib, ynb, xnb) + tuple({"fs": peer} for peer in peers):
        pl.semaphore_signal(barrier, inc=1, device_id=dev, device_id_type=MESH)

    def span(start, size):
        return pl.ds(pl.multiple_of(start, size), size)

    loads = [
        pltpu.make_async_copy(source, target, load_sem.at[i])
        for i, (source, target) in enumerate(
            (
                (dw_ref, dv_f32.at[0]),
                (vw_ref, dv_f32.at[1]),
                (tok_hbm, tok_ref),
                (mgain_hbm, mgain_ref),
                (mscale_hbm, mscale_ref),
                (mw_ref, mg_f32),
                (ew_ref.at[:, span(r * wide, wide)], ex_f32),
                (rscale_hbm, rscale_ref),
                (rw_ref.at[span(r * wide, wide)], rd_f32),
                (dscale_hbm, dscale_ref),
                (vscale_hbm, vscale_ref),
                (vgain_hbm, vgain_ref),
                (vshift_hbm, vshift_ref),
                (sw_hbm, sw_ref),
                (sbias_hbm, sbias_ref),
                (cgain_hbm, cgain_ref),
                (exscale_hbm, exscale_ref),
            )
        )
    ]
    for load in loads:
        load.start()

    def rcopy(src, dst, ssem, rsem, dev):
        return pltpu.make_async_remote_copy(
            src_ref=src, dst_ref=dst, send_sem=ssem, recv_sem=rsem,
            device_id=dev, device_id_type=MESH,
        )

    quarters = 2 * rows // half
    merge_item = quarters

    def item(i, slot, q):
        if i < quarters:
            return dv_all.at[slot, span(q * 2 * rows + i * half, half)]
        return mg_all.at[slot, span(q * rows, rows)]

    def origin(way, d):
        return lax.rem(f + (4 - d if way == 0 else d), 4)

    def comes(way, d):
        return f >= d if way == 0 else f + d <= 3

    def goes(way):
        return f < 3 if way == 0 else f > 0

    def inward(way):
        return f < 2 if way == 0 else f >= 2

    def hop(i, way, d):
        ref = item(i, origin(way, d), r)
        to = lax.rem(f + (1 if way == 0 else 3), 4)
        return rcopy(
            ref, ref, wsend.at[min(d, 1)], wrecv.at[i, origin(way, d)], {"fs": to}
        )

    def over(i, way, d):
        slot = origin(way, d)
        ref = item(i, slot, r)
        return rcopy(ref, ref, xsend.at[i // quarters], xrecv.at[i, slot], xnb)

    def relay(i, d):
        for way in range(2):

            @pl.when(comes(way, d))
            def _(way=way):
                hop(i, way, d).wait_recv()
                over(i, way, d).start()

            if d < 3:

                @pl.when(jnp.logical_and(comes(way, d), goes(way)))
                def _(way=way):
                    hop(i, way, d).start()

    def relay_all(d):
        for i in range(quarters):
            relay(i, d)

    def over_wait(i, d):
        for way in range(2):

            @pl.when(comes(way, d))
            def _(way=way):
                over(i, way, d).wait_recv()

    inner = jnp.logical_or(f == 1, f == 2)
    outer = jnp.logical_not(inner)

    def part(to_inner):
        return (0, big) if to_inner else (big, small)

    cuts = ((0, thin // 2), (thin // 2, thin // 2), (thin, thin))

    def ex_copy(j, to_inner, h):
        first, size = part(to_inner)
        start, count = cuts[h]
        return rcopy(
            ex_own.at[pl.ds(start, count), pl.ds(first, size)],
            ex_all.at[span(f * piece + start, count), pl.ds(0, size)],
            csend.at[int(to_inner)], crecv.at[0], {"fs": peers[j]},
        )

    def ex_start(j, to_inner, which=(0, 1, 2)):
        for h in which:
            ex_copy(j, to_inner, h).start()

    left, right, third_lanes, fourth_lanes = range(4)
    lane_cuts = ((0, thin), (thin, thin), (thin, thin // 2), (thin + thin // 2, thin // 2))

    def rd_copy(side, j, to_inner, index=None):
        first, size = part(to_inner)
        cut = pl.ds(*lane_cuts[side])
        n = 1 + side * 3 + (j if index is None else index)
        return rcopy(
            rd_own.at[pl.ds(first, size), cut], rd_all.at[f, pl.ds(0, size), cut],
            csend.at[2 + int(to_inner)], crecv.at[n], {"fs": peers[j]},
        )

    def both(action):
        @pl.when(inner)
        def _():
            action(True)

        @pl.when(outer)
        def _():
            action(False)

    def norm(x, gain):
        return (
            x * lax.rsqrt(jnp.mean(x * x, axis=-1, keepdims=True) + epsilon) * gain
        ).astype(jnp.bfloat16)

    def block(n, size=1):
        return pl.ds(pl.multiple_of(n * rows, rows), size * rows)

    def columns(slot):
        return span(slot * piece, piece)

    for i in range(2):
        loads[i].wait()
        dv_all[f, :, i * local : (i + 1) * local] = dv_f32[i].astype(jnp.bfloat16)
    for i in range(2, 4):
        loads[i].wait()
    mine = xg.at[block(c * 2 + y)]
    mine[...] = norm(tok_ref[...].astype(jnp.float32), mgain_ref[...])
    far = xg.at[block(c * 2 + 1 - y)]
    gather = (
        rcopy(mine, mine, gsend.at[0], grecv.at[0], sib),
        rcopy(mine, mine, gsend.at[0], grecv.at[1], ynb),
        rcopy(far, far, gsend.at[0], grecv.at[2], sib),
    )
    pl.semaphore_wait(barrier, 6)
    for i in range(quarters):
        for way in range(2):

            @pl.when(goes(way))
            def _(i=i, way=way):
                hop(i, way, 0).start()

    gather[1].start()
    gather[0].start()
    for i in range(4, 6):
        loads[i].wait()
    mg_all[f] = (mg_f32[...] * mscale_ref[...]).astype(jnp.bfloat16)
    loads[6].wait()
    ex_own[...] = ex_f32[...].astype(jnp.bfloat16)

    relay_all(1)
    for way in range(2):

        @pl.when(inward(way))
        def _(way=way):
            hop(merge_item, way, 0).start()

    @pl.when(outer)
    def _():
        ex_start(0, True)

    relay_all(2)
    for way in range(2):

        @pl.when(jnp.logical_and(jnp.logical_not(inward(way)), goes(way)))
        def _(way=way):
            hop(merge_item, way, 0).start()

    gather[1].wait_recv()
    gather[2].start()

    @pl.when(inner)
    def _():
        relay(merge_item, 1)
        relay(merge_item, 2)
        ex_start(2, True, (0,))

    @pl.when(outer)
    def _():
        relay_all(3)

    for load in loads[7:]:
        load.wait()
    rd_own[...] = (rd_f32[...] * rscale_ref[...]).astype(jnp.bfloat16)

    @pl.when(outer)
    def _():
        ex_all[:, small:] = jnp.zeros((width, big - small), jnp.bfloat16)
        for slot in range(4):
            rd_all[slot, small:] = jnp.zeros((big - small, piece), jnp.bfloat16)

    def place_own(is_inner):
        first, size = part(is_inner)
        ex_all[columns(f), :size] = ex_own[:, first : first + size]
        rd_all[f, :size] = rd_own[first : first + size]

    both(place_own)

    def project(slot):
        return jnp.dot(xg[:, columns(slot)], dv_all[slot], preferred_element_type=jnp.float32)

    gather[0].wait_recv()
    gather[2].wait_recv()
    act[...] = project(f)

    def project_more(d):
        for i in range(quarters):
            over_wait(i, d)
        for way in range(2):

            @pl.when(comes(way, d))
            def _(way=way):
                act[...] += project(origin(way, d))

    project_more(1)
    project_more(2)
    project_more(3)

    @pl.when(outer)
    def _():
        ex_start(1, True, (0, 1))
        relay(merge_item, 1)
        relay(merge_item, 2)

    dvscale = jnp.concatenate([dscale_ref[...], vscale_ref[...]], axis=1)
    act[...] = jax.nn.gelu(act[...] * dvscale)

    lane = lax.broadcasted_iota(jnp.int32, (rows, rows), 1)
    for n in range(4):
        value = act[n * rows : (n + 1) * rows, local:]
        total = jnp.sum(value, axis=1, keepdims=True)
        squares = jnp.sum(value * value, axis=1, keepdims=True)
        table = jnp.where(lane == 0, total, jnp.where(lane == 1, squares, 0.0))
        stat[t, n] = jnp.transpose(table)[:8]
    stats = [
        rcopy(stat.at[t], stat.at[t], gsend.at[1], trecv.at[0], sib),
        rcopy(stat.at[t], stat.at[t], gsend.at[1], trecv.at[1], ynb),
        rcopy(
            stat.at[(1 - y) * 2 + c], stat.at[(1 - y) * 2 + c], gsend.at[1], trecv.at[2], sib
        ),
    ]
    stats[1].start()
    stats[0].start()
    groups = sbias_ref.shape[0]
    down = lax.broadcasted_iota(jnp.int32, (rows, rows), 0)
    bias = jnp.zeros((rows, rows), jnp.float32)
    for n in range(groups):
        bias = jnp.where(down == n, sbias_ref[n : n + 1, :], bias)
    bias = jnp.transpose(bias)
    stats[1].wait_recv()
    stats[2].start()
    stats[0].wait_recv()
    stats[2].wait_recv()

    @pl.when(inner)
    def _():
        ex_start(1, False)
        ex_start(2, True, (1, 2))

    @pl.when(outer)
    def _():
        ex_start(2, False)
        relay(merge_item, 3)

    inverse = 1.0 / (local * 4)
    group_lane = lax.broadcasted_iota(jnp.int32, (rows, 128), 1) // GDIM
    for n in range(4):
        here = slice(n * rows, (n + 1) * rows)
        summed = stat[0, n] + stat[1, n] + stat[2, n] + stat[3, n]
        table = jnp.transpose(jnp.concatenate([summed] * (rows // 8), axis=0))
        mean = table[:, 0:1] * inverse
        var = table[:, 1:2] * inverse - mean * mean
        gv = (
            (act[here, local:] - mean) * lax.rsqrt(var + epsilon) * vgain_ref[...]
            + vshift_ref[...]
        ).astype(jnp.bfloat16)
        per = 128 // GDIM
        for j in range(local // 128):
            at = slice(j * 128, (j + 1) * 128)
            mixed = jnp.dot(sw_ref[j * per], gv[:, at], preferred_element_type=jnp.float32)
            mixed = mixed + bias[:, j * per : j * per + 1]
            for k in range(1, per):
                n_group = j * per + k
                other = jnp.dot(sw_ref[n_group], gv[:, at], preferred_element_type=jnp.float32)
                other = other + bias[:, n_group : n_group + 1]
                mixed = jnp.where(group_lane == k, other, mixed)
            gated[here, at] = (act[here, at] * mixed).astype(jnp.bfloat16)

    closer, farther = jnp.where(inner, 2, 1), jnp.where(inner, 1, 2)
    second_slot = jnp.where(inner, peers[2], peers[1])
    last_slot = jnp.where(inner, peers[1], peers[2])
    merge_order = (f, mate, second_slot, last_slot)

    def merge_pair(k):
        return rcopy(
            p1.at[k, block((1 - c) * 2, 2)], r1.at[k], msend.at[0], mrecv.at[k, 0], sib
        )

    def merge_far(k):
        return rcopy(s1.at[k], x1.at[k], msend.at[1], mrecv.at[k, 1], ynb)

    def merge_send(k):
        merge_pair(k).wait_recv()
        s1[k] = (
            p1[k, block(c * 2 + 1 - y)].astype(jnp.float32)
            + r1[k, block(1 - y)].astype(jnp.float32)
        ).astype(jnp.bfloat16)
        merge_far(k).start()

    for k, slot in enumerate(merge_order):
        if k == 1:
            over_wait(merge_item, 1)
        if k == 2:

            @pl.when(outer)
            def _():
                over_wait(merge_item, 2)

        if k == 3:

            @pl.when(inner)
            def _():
                over_wait(merge_item, 2)

            over_wait(merge_item, 3)
        p1[k] = jnp.dot(gated[...], mg_all[slot], preferred_element_type=jnp.float32).astype(
            jnp.bfloat16
        )
        merge_pair(k).start()
        if k > 0:
            merge_send(k - 1)
    merge_send(3)
    for k, slot in enumerate(merge_order):
        merge_far(k).wait_recv()
        mid[:, columns(slot)] = (
            tok_ref[:, columns(slot)].astype(jnp.float32)
            + p1[k, block(c * 2 + y)].astype(jnp.float32)
            + r1[k, block(y)].astype(jnp.float32)
            + x1[k].astype(jnp.float32)
        ).astype(jnp.bfloat16)

    def group(zz, rr, yy):
        return zz * 4 + rr * 2 + yy

    def place(zz, rr, yy):
        return nm.at[group(zz, rr, yy), c]

    mine = place(z, r, y)
    mine[...] = norm(mid[...].astype(jnp.float32), cgain_ref[...])
    over_fs = rcopy(mine, mine, nsend.at[1], nrecv.at[20], znb)

    def spreading(b, zz):
        here, from_x = place(zz, r, y), place(zz, 1 - r, y)
        from_y, from_xy = place(zz, r, 1 - y), place(zz, 1 - r, 1 - y)

        def low(ref):
            return ref.at[pl.ds(0, half)]

        def high(ref):
            return ref.at[pl.ds(half, half)]

        routes = (
            (low(here), xnb), (high(here), xnb), (high(here), ynb), (low(here), ynb), (here, sib),
            (low(from_x), ynb), (high(from_y), xnb),
            (from_x, sib), (from_y, sib), (from_xy, sib),
        )
        return tuple(
            rcopy(ref, ref, nsend.at[0], nrecv.at[10 * b + k], dev)
            for k, (ref, dev) in enumerate(routes)
        )

    near, away = spreading(0, z), spreading(1, 1 - z)

    def first(spread):
        for k in (0, 2, 1, 3, 4):
            spread[k].start()

    def second(spread):
        spread[0].wait_recv()
        spread[5].start()
        spread[2].wait_recv()
        spread[6].start()

    def third(spread):
        spread[1].wait_recv()
        spread[7].start()
        spread[3].wait_recv()
        spread[8].start()

    def fourth(spread):
        spread[5].wait_recv()
        spread[6].wait_recv()
        spread[9].start()

    def gathered(spread):
        for k in (4, 7, 8, 9):
            spread[k].wait_recv()

    over_fs.start()

    @pl.when(outer)
    def _():
        ex_start(1, True, (2,))

    first(near)

    second(near)

    @pl.when(inner)
    def _():
        ex_start(0, False)

    third(near)
    over_fs.wait_recv()
    first(away)

    def rd_start(side, j, to_inner):
        rd_copy(side, j, to_inner).start()

    @pl.when(inner)
    def _():
        for side in (left, right):
            rd_start(side, 0, False)
        for side in (left, third_lanes, fourth_lanes):
            rd_start(side, 2, True)
            rd_start(side, 1, False)

    @pl.when(outer)
    def _():
        for side in (left, right):
            rd_start(side, 0, True)

    fourth(near)

    tall = 2 * rows
    start = pl.multiple_of(r * wide, wide)
    exscale = jnp.where(
        inner,
        exscale_ref[:, pl.ds(start, big)],
        jnp.concatenate(
            [
                exscale_ref[:, pl.ds(pl.multiple_of(start + big, 2 * GDIM), small)],
                jnp.zeros((1, big - small), jnp.float32),
            ],
            axis=1,
        ),
    )

    def expand(count, group_of):
        def step(i, _):
            g = group_of(i)
            upper = jnp.dot(
                nm[g].reshape(tall, width), ex_all[...], preferred_element_type=jnp.float32
            ) * exscale
            hid[g] = jnp.square(jax.nn.relu(upper)).astype(jnp.bfloat16)

        lax.fori_loop(0, count, step, None)

    def pick(if_inner, if_outer):
        return jnp.where(inner, if_inner, if_outer)

    slots = (f, f, mate, mate, second_slot, last_slot, last_slot, second_slot, second_slot)
    sides = (left, right, left, right, left, left, right, third_lanes, fourth_lanes)
    runs = (0, 0, 1, 1, 2, 3, 3, 2, 2)
    came = (None, None, 0, 0, pick(2, 1), pick(1, 2), pick(1, 2), pick(2, 1), pick(2, 1))
    near_half, far_half = 0, 1
    units = tuple((k, h) for h in range(2) for k in range(4))
    units += tuple((k, h) for k in range(4, len(slots)) for h in (1, 0))

    def plane(h):
        return z if h == near_half else 1 - z

    def arrived(side, j):
        both(lambda is_inner: rd_copy(side, 0, is_inner, j).wait_recv())

    starts = tuple(run * piece + lane_cuts[side][0] for run, side in zip(runs, sides))

    def lanes(k):
        return slice(starts[k], starts[k] + lane_cuts[sides[k]][1])

    def reduce(u):
        k, h = units[u]
        slot, side = slots[k], sides[k]
        first, size = lane_cuts[side]
        if k > 1 and h == (near_half if k < 4 else far_half):
            arrived(side, came[k])
        zz = plane(h)

        def step(i, _):
            g = zz * 4 + i * 2
            p2[pl.ds(g, 2), :, :, lanes(k)] = (
                jnp.dot(
                    hid[pl.ds(g, 2)].reshape(2 * tall, big),
                    rd_all[slot, :, first : first + size],
                    preferred_element_type=jnp.float32,
                )
                .astype(jnp.bfloat16)
                .reshape(2, 2, rows, size)
            )

        lax.fori_loop(0, 2, step, None)
        pair(u).start()

    y_first = tuple(u % 2 == 0 for u in range(len(units)))

    def cols(k):
        return pl.ds(lanes(k).start, lanes(k).stop - lanes(k).start)

    def pair(u):
        k, h = units[u]
        at = pl.ds(plane(h) * 4, 4)
        return rcopy(
            p2.at[at, 1 - c, :, cols(k)], r2.at[at, :, cols(k)], fsend.at[0], frecv.at[0, u], sib
        )

    def summed_pair(k, g):
        return p2[g, c, :, lanes(k)].astype(jnp.float32) + r2[g, :, lanes(k)].astype(jnp.float32)

    def hop_one(u):
        k, h = units[u]
        at = (h, slice(None), slice(None), cols(k))
        return rcopy(
            f1.at[at], a1.at[at], fsend.at[1], frecv.at[1, u], ynb if y_first[u] else xnb
        )

    def hop_two(u):
        k, h = units[u]
        at = (h, slice(None), cols(k))
        return rcopy(
            f2.at[at], a2.at[at], fsend.at[2], frecv.at[2, u], xnb if y_first[u] else ynb
        )

    def lane_span(k):
        first, size = lane_cuts[sides[k]]
        return pl.ds(pl.multiple_of(slots[k] * piece + first, rows), size)

    def hop_three(k):
        q = slots[k] * 4 + sides[k]
        return rcopy(
            f3.at[:, cols(k)], a3.at[:, lane_span(k)], fsend.at[3], frecv.at[3, q], znb
        )

    def send_one(u):
        k, h = units[u]
        zz = plane(h)
        pair(u).wait_recv()
        for n in range(2):
            g = group(zz, n, 1 - y) if y_first[u] else group(zz, 1 - r, n)
            f1[h, n, :, lanes(k)] = summed_pair(k, g).astype(jnp.bfloat16)
        hop_one(u).start()

    def send_two(u):
        k, h = units[u]
        zz = plane(h)
        hop_one(u).wait_recv()
        g, n = (group(zz, 1 - r, y), 1 - r) if y_first[u] else (group(zz, r, 1 - y), 1 - y)
        f2[h, :, lanes(k)] = (
            summed_pair(k, g) + a1[h, n, :, lanes(k)].astype(jnp.float32)
        ).astype(jnp.bfloat16)
        hop_two(u).start()

    def own_sum(u):
        k, h = units[u]
        n = r if y_first[u] else y
        hop_two(u).wait_recv()
        return (
            summed_pair(k, group(plane(h), r, y))
            + a1[h, n, :, lanes(k)].astype(jnp.float32)
            + a2[h, :, lanes(k)].astype(jnp.float32)
        )

    def send_three(u):
        k, h = units[u]
        if h == far_half:
            f3[:, lanes(k)] = own_sum(u).astype(jnp.bfloat16)
            hop_three(k).start()

    def ex_arrived(is_inner):
        ref = ex_all.at[pl.ds(0, 3 * piece), pl.ds(0, part(is_inner)[1])]
        rcopy(ref, ref, csend.at[0], crecv.at[0], znb).wait_recv()

    done = set()

    def once(action, u):
        if 0 <= u < len(units) and (action, u) not in done:
            done.add((action, u))
            action(u)

    gathered(near)
    both(ex_arrived)
    expand(4, lambda i: z * 4 + i)
    second(away)
    away[4].wait_recv()
    expand(1, lambda i: group(1 - z, r, y) + i)
    once(reduce, 0)
    once(reduce, 1)
    third(away)
    once(send_one, 0)
    once(send_one, 1)
    once(reduce, 2)
    away[7].wait_recv()
    away[8].wait_recv()
    expand(2, lambda i: jnp.where(i == 0, group(1 - z, 1 - r, y), group(1 - z, r, 1 - y)))
    once(send_one, 2)

    @pl.when(outer)
    def _():
        rd_start(left, 2, False)
        rd_start(left, 1, True)
        rd_start(right, 1, True)
        rd_start(right, 2, False)

    fourth(away)
    away[9].wait_recv()
    expand(1, lambda i: group(1 - z, 1 - r, 1 - y) + i)
    turn = (0, 1, 2, 4, 5, 3) + tuple(range(6, len(units)))

    def late(action, n):
        if n >= 0:
            once(action, turn[n])

    for n in range(3, len(turn)):
        if n in (12, 14, 16):
            late(send_one, n - 1)
            late(send_two, n - 4)
            late(send_two, n - 3)
        late(reduce, n)
        late(send_one, n - 1)
        late(send_two, n - 4)
        late(send_three, n - 8)
    count = len(units)
    once(send_one, count - 1)
    for u in range(count - 4, count):
        once(send_two, u)
        once(send_three, 2 * (u - 9))
    once(send_three, count - 2)

    def stored(k):
        at = lane_span(k)
        return pltpu.make_async_copy(result.at[:, at], out_ref.at[:, at], out_sem)

    for k in range(len(slots)):
        at = lane_span(k)
        near_sum = own_sum(units.index((k, near_half)))
        hop_three(k).wait_recv()
        result[:, at] = (
            mid[:, at].astype(jnp.float32) + near_sum + a3[:, at].astype(jnp.float32)
        ).astype(jnp.bfloat16)
        stored(k).start()

    def sent(ref, sem):
        rcopy(ref, ref, sem, crecv.at[0], znb).wait_send()

    def few_sent(is_inner):
        own = rows * (2 if is_inner else 1)
        sent(dv_all.at[pl.ds(0, 3), pl.ds(0, own)], wsend.at[0])
        if is_inner:
            sent(dv_all.at[pl.ds(0, 3), pl.ds(0, 3 * rows)], wsend.at[1])
        for to_inner in (False, True):
            size = part(to_inner)[1]
            count = piece * (1 if to_inner == is_inner else 2)
            for n in (0, 2):
                sent(ex_all.at[pl.ds(0, count), pl.ds(0, size)], csend.at[n + int(to_inner)])

    both(few_sent)
    sent(dv_all.at[pl.ds(0, 3), pl.ds(0, 2 * rows)], xsend.at[0])
    sent(mg_all.at[pl.ds(0, 3), pl.ds(0, rows)], xsend.at[1])
    sent(xg.at[pl.ds(0, 3 * rows)], gsend.at[0])
    sent(stat.at[pl.ds(0, 3)], gsend.at[1])
    sent(r1, msend.at[0])
    sent(s1, msend.at[1])
    sent(nm.at[pl.ds(0, 7)], nsend.at[0])
    over_fs.wait_send()
    for n, ref in enumerate((r2, f1, f2, f3)):
        sent(ref, fsend.at[n])
    pltpu.make_async_copy(result, out_ref, out_sem).wait()


def fused_body(
    tokens,
    mixer_gain,
    direct_weight,
    direct_scale,
    value_weight,
    value_scale,
    value_gain,
    value_shift,
    spatial_weight,
    spatial_bias,
    merge_weight,
    merge_scale,
    channel_gain,
    expand_weight,
    expand_scale,
    reduce_weight,
    reduce_scale,
):
    bf = jnp.bfloat16
    rows, width = tokens.shape
    piece, local = direct_weight.shape
    wide = expand_weight.shape[1] // 2
    big = wide * 5 // 8
    thin = piece // 2
    seq = 4 * rows
    vm = pltpu.VMEM
    dma = pltpu.SemaphoreType.DMA
    f32 = jnp.float32
    small = (
        tokens, mixer_gain[None], direct_scale[None], value_scale[None], value_gain[None],
        value_shift[None], spatial_weight, spatial_bias, merge_scale[None], channel_gain[None],
        expand_scale[None], reduce_scale[None],
    )
    large = (direct_weight, value_weight, merge_weight, expand_weight, reduce_weight)
    return pl.pallas_call(
        fused_kernel,
        out_shape=jax.ShapeDtypeStruct((rows, width), bf),
        in_specs=[pl.BlockSpec(memory_space=pl.ANY)] * len(small + large),
        out_specs=pl.BlockSpec(memory_space=pl.ANY),
        scratch_shapes=[vm(a.shape, a.dtype) for a in small]
        + [
            vm((2, piece, local), f32),
            vm((local, piece), f32),
            vm((piece, wide), f32),
            vm((wide, piece), f32),
            vm((4, piece, 2 * local), bf),
            vm((4, local, piece), bf),
            vm((4 * piece, big), bf),
            vm((piece, wide), bf),
            vm((4, big, piece), bf),
            vm((wide, piece), bf),
            vm((seq, width), bf),
            vm((seq, 2 * local), f32),
            vm((4, 4, 8, rows), f32),
            vm((seq, local), bf),
            vm((4, seq, piece), bf),
            vm((4, 2 * rows, piece), bf),
            vm((4, rows, piece), bf),
            vm((4, rows, piece), bf),
            vm((rows, width), bf),
            vm((8, 2, rows, width), bf),
            vm((8, 2 * rows, big), bf),
            vm((8, 2, rows, width), bf),
            vm((8, rows, width), bf),
            vm((2, 2, rows, width), bf),
            vm((2, 2, rows, width), bf),
            vm((2, rows, width), bf),
            vm((2, rows, width), bf),
            vm((rows, width), bf),
            vm((rows, width), bf),
            vm((rows, width), bf),
            dma((17,)), dma,
            dma((2,)), dma((5, 4)),
            dma((2,)), dma((5, 4)),
            dma((4,)), dma((13,)),
            dma((2,)), dma((3,)), dma((3,)),
            dma((2,)), dma((4, 2)),
            dma((2,)), dma((21,)),
            dma((4,)), dma((4, 18)),
        ],
        compiler_params=pltpu.CompilerParams(
            collective_id=0, has_side_effects=True, vmem_limit_bytes=62 * 1024 * 1024
        ),
    )(*small, *large)


def solution(mesh):
    sizes = mesh.shape
    fused = sizes["rep"] == 2 and sizes["fs"] == 4 and sizes["tp"] == 4
    return jax.shard_map(
        fused_body if fused else body,
        mesh=mesh,
        in_specs=(
            P(("rep", "fs", "tp"), None),
            P(),
            P("fs", "tp"),
            P("tp"),
            P("fs", "tp"),
            P("tp"),
            P("tp"),
            P("tp"),
            P("tp", None, None),
            P("tp", None),
            P("tp", "fs"),
            P("fs"),
            P(),
            P("fs", "tp"),
            P("tp"),
            P("tp", "fs"),
            P("fs"),
        ),
        out_specs=P(("rep", "fs", "tp"), None),
        check_vma=False,
    )
```

```python
import jax
import jax.numpy as jnp
from jax import lax
from jax.experimental import pallas as pl
from jax.experimental.pallas import tpu as pltpu
from jax.sharding import PartitionSpec as P

GDIM = 64
BLOCK = 128


epsilon = 1e-06


def rms_rows(rows, gain):
    floats = rows.astype(jnp.float32)
    scaled = floats * lax.rsqrt(jnp.mean(floats * floats, axis=-1, keepdims=True) + epsilon)
    return (scaled * gain).astype(jnp.bfloat16)


def body(
    tokens,
    mixer_gain,
    direct_weight,
    direct_scale,
    value_weight,
    value_scale,
    value_gain,
    value_shift,
    spatial_weight,
    spatial_bias,
    merge_weight,
    merge_scale,
    channel_gain,
    expand_weight,
    expand_scale,
    reduce_weight,
    reduce_scale,
):
    direct_half = direct_weight.astype(jnp.bfloat16)
    value_half = value_weight.astype(jnp.bfloat16)
    merge_half = merge_weight.astype(jnp.bfloat16)
    expand_half = expand_weight.astype(jnp.bfloat16)
    reduce_half = reduce_weight.astype(jnp.bfloat16)
    full_expand, full_reduce, reduce_full_scale = (
        lax.all_gather(expand_half, "fs", axis=0, tiled=True),
        lax.all_gather(reduce_half, "fs", axis=1, tiled=True),
        lax.all_gather(reduce_scale.astype(jnp.bfloat16), "fs", axis=0, tiled=True).astype(
            reduce_scale.dtype
        ),
    )
    normed = rms_rows(tokens, mixer_gain)
    whole = lax.all_gather(normed, "tp", axis=0, tiled=True)
    seq_rows = whole.shape[0]
    local_width = direct_weight.shape[1]
    direct_pre = jnp.dot(
        whole,
        lax.all_gather(direct_half, "fs", axis=0, tiled=True),
        preferred_element_type=jnp.float32,
    )
    value_pre = jnp.dot(
        whole,
        lax.all_gather(value_half, "fs", axis=0, tiled=True),
        preferred_element_type=jnp.float32,
    )
    full_merge, merge_full_scale = (
        lax.all_gather(merge_half, "fs", axis=1, tiled=True),
        lax.all_gather(merge_scale.astype(jnp.bfloat16), "fs", axis=0, tiled=True).astype(
            merge_scale.dtype
        ),
    )
    direct = jax.nn.gelu(direct_pre * direct_scale)
    value = jax.nn.gelu(value_pre * value_scale)
    total, squares = lax.psum((jnp.sum(value, axis=1), jnp.sum(value * value, axis=1)), "tp")
    branch_width = local_width * lax.axis_size("tp")
    mean = (total / branch_width)[:, None]
    var = (squares / branch_width)[:, None] - mean * mean
    gated_value = ((value - mean) * lax.rsqrt(var + epsilon) * value_gain + value_shift).astype(
        jnp.bfloat16
    )
    local_groups = spatial_weight.shape[0]
    blocks = gated_value.reshape(seq_rows // BLOCK, BLOCK, local_groups, GDIM)
    mixed = jnp.einsum("gpq,nqgc->npgc", spatial_weight, blocks, preferred_element_type=jnp.float32)
    mixed = mixed + jnp.transpose(spatial_bias)[None, :, :, None]
    gated = (direct * mixed.reshape(seq_rows, local_width)).astype(jnp.bfloat16)
    rows = gated
    mix = lax.psum_scatter(
        (jnp.dot(rows, full_merge, preferred_element_type=jnp.float32) * merge_full_scale).astype(
            jnp.bfloat16
        ),
        "tp",
        scatter_dimension=0,
        tiled=True,
    ).astype(jnp.float32)
    middle = (tokens.astype(jnp.float32) + mix).astype(jnp.bfloat16)
    normed_mid = rms_rows(middle, channel_gain)
    whole_mid = lax.all_gather(normed_mid, "tp", axis=0, tiled=True)
    upper = jnp.dot(whole_mid, full_expand, preferred_element_type=jnp.float32)
    hidden = jnp.square(jax.nn.relu(upper * expand_scale)).astype(jnp.bfloat16)
    rows = hidden
    lower = lax.psum_scatter(
        (jnp.dot(rows, full_reduce, preferred_element_type=jnp.float32) * reduce_full_scale).astype(
            jnp.bfloat16
        ),
        "tp",
        scatter_dimension=0,
        tiled=True,
    ).astype(jnp.float32)
    return (middle.astype(jnp.float32) + lower).astype(jnp.bfloat16)


MESH = pl.DeviceIdType.MESH


def fused_kernel(
    tok_hbm, mgain_hbm, dscale_hbm, vscale_hbm, vgain_hbm, vshift_hbm, sw_hbm, sbias_hbm,
    mscale_hbm, cgain_hbm, exscale_hbm, rscale_hbm,
    dw_ref, vw_ref, mw_ref, ew_ref, rw_ref,
    out_ref,
    tok_ref, mgain_ref, dscale_ref, vscale_ref, vgain_ref, vshift_ref, sw_ref, sbias_ref,
    mscale_ref, cgain_ref, exscale_ref, rscale_ref,
    dv_f32, mg_f32, ex_f32, rd_f32,
    dv_all, mg_all, ex_all, ex_own, rd_all, rd_own,
    xg, act, stat, gated, p1, r1, s1, x1, mid,
    nm, hid, p2, r2, f1, a1, f2, a2, f3, a3, result,
    load_sem, out_sem, wsend, wrecv, xsend, xrecv, csend, crecv, gsend, grecv, trecv, msend, mrecv,
    nsend, nrecv, fsend, frecv,
):
    rows, width = tok_ref.shape
    piece, local = dw_ref.shape
    big = hid.shape[2]
    wide = ex_own.shape[1]
    small = wide - big
    half = rows // 2
    thin = piece // 2
    r = lax.axis_index("rep")
    f = lax.axis_index("fs")
    t = lax.axis_index("tp")
    y, c = t // 2, t % 2
    z = f % 2
    mate = f + 1 - 2 * z
    peers = (mate, (f + 2) % 4, (mate + 2) % 4)
    sib = {"tp": y * 2 + (1 - c)}
    ynb = {"tp": (1 - y) * 2 + c}
    xnb = {"rep": 1 - r}
    znb = {"fs": mate}

    barrier = pltpu.get_barrier_semaphore()
    for dev in (sib, ynb, xnb) + tuple({"fs": peer} for peer in peers):
        pl.semaphore_signal(barrier, inc=1, device_id=dev, device_id_type=MESH)

    def span(start, size):
        return pl.ds(pl.multiple_of(start, size), size)

    loads = [
        pltpu.make_async_copy(source, target, load_sem.at[i])
        for i, (source, target) in enumerate(
            (
                (dw_ref, dv_f32.at[0]),
                (vw_ref, dv_f32.at[1]),
                (tok_hbm, tok_ref),
                (mgain_hbm, mgain_ref),
                (mscale_hbm, mscale_ref),
                (mw_ref, mg_f32),
                (ew_ref.at[:, span(r * wide, wide)], ex_f32),
                (rscale_hbm, rscale_ref),
                (rw_ref.at[span(r * wide, wide)], rd_f32),
                (dscale_hbm, dscale_ref),
                (vscale_hbm, vscale_ref),
                (vgain_hbm, vgain_ref),
                (vshift_hbm, vshift_ref),
                (sw_hbm, sw_ref),
                (sbias_hbm, sbias_ref),
                (cgain_hbm, cgain_ref),
                (exscale_hbm, exscale_ref),
            )
        )
    ]
    for load in loads:
        load.start()

    def rcopy(src, dst, ssem, rsem, dev):
        return pltpu.make_async_remote_copy(
            src_ref=src, dst_ref=dst, send_sem=ssem, recv_sem=rsem,
            device_id=dev, device_id_type=MESH,
        )

    quarters = 2 * rows // half
    merge_item = quarters

    def item(i, slot, q):
        if i < quarters:
            return dv_all.at[slot, span(q * 2 * rows + i * half, half)]
        return mg_all.at[slot, span(q * rows, rows)]

    def origin(way, d):
        return lax.rem(f + (4 - d if way == 0 else d), 4)

    def comes(way, d):
        return f >= d if way == 0 else f + d <= 3

    def goes(way):
        return f < 3 if way == 0 else f > 0

    def inward(way):
        return f < 2 if way == 0 else f >= 2

    def hop(i, way, d):
        ref = item(i, origin(way, d), r)
        to = lax.rem(f + (1 if way == 0 else 3), 4)
        return rcopy(
            ref, ref, wsend.at[min(d, 1)], wrecv.at[i, origin(way, d)], {"fs": to}
        )

    def over(i, way, d):
        slot = origin(way, d)
        ref = item(i, slot, r)
        return rcopy(ref, ref, xsend.at[i // quarters], xrecv.at[i, slot], xnb)

    def relay(i, d):
        for way in range(2):

            @pl.when(comes(way, d))
            def _(way=way):
                hop(i, way, d).wait_recv()
                over(i, way, d).start()

            if d < 3:

                @pl.when(jnp.logical_and(comes(way, d), goes(way)))
                def _(way=way):
                    hop(i, way, d).start()

    def relay_all(d):
        for i in range(quarters):
            relay(i, d)

    def over_wait(i, d):
        for way in range(2):

            @pl.when(comes(way, d))
            def _(way=way):
                over(i, way, d).wait_recv()

    inner = jnp.logical_or(f == 1, f == 2)
    outer = jnp.logical_not(inner)

    def part(to_inner):
        return (0, big) if to_inner else (big, small)

    cuts = ((0, thin // 2), (thin // 2, thin // 2), (thin, thin))

    def ex_copy(j, to_inner, h):
        first, size = part(to_inner)
        start, count = cuts[h]
        return rcopy(
            ex_own.at[pl.ds(start, count), pl.ds(first, size)],
            ex_all.at[span(f * piece + start, count), pl.ds(0, size)],
            csend.at[int(to_inner)], crecv.at[0], {"fs": peers[j]},
        )

    def ex_start(j, to_inner, which=(0, 1, 2)):
        for h in which:
            ex_copy(j, to_inner, h).start()

    left, right, third_lanes, fourth_lanes = range(4)
    lane_cuts = ((0, thin), (thin, thin), (thin, thin // 2), (thin + thin // 2, thin // 2))

    def rd_copy(side, j, to_inner, index=None):
        first, size = part(to_inner)
        cut = pl.ds(*lane_cuts[side])
        n = 1 + side * 3 + (j if index is None else index)
        return rcopy(
            rd_own.at[pl.ds(first, size), cut], rd_all.at[f, pl.ds(0, size), cut],
            csend.at[2 + int(to_inner)], crecv.at[n], {"fs": peers[j]},
        )

    def both(action):
        @pl.when(inner)
        def _():
            action(True)

        @pl.when(outer)
        def _():
            action(False)

    def norm(x, gain):
        return (
            x * lax.rsqrt(jnp.mean(x * x, axis=-1, keepdims=True) + epsilon) * gain
        ).astype(jnp.bfloat16)

    def block(n, size=1):
        return pl.ds(pl.multiple_of(n * rows, rows), size * rows)

    def columns(slot):
        return span(slot * piece, piece)

    for i in range(2):
        loads[i].wait()
        dv_all[f, :, i * local : (i + 1) * local] = dv_f32[i].astype(jnp.bfloat16)
    for i in range(2, 4):
        loads[i].wait()
    mine = xg.at[block(c * 2 + y)]
    mine[...] = norm(tok_ref[...].astype(jnp.float32), mgain_ref[...])
    far = xg.at[block(c * 2 + 1 - y)]
    gather = (
        rcopy(mine, mine, gsend.at[0], grecv.at[0], sib),
        rcopy(mine, mine, gsend.at[0], grecv.at[1], ynb),
        rcopy(far, far, gsend.at[0], grecv.at[2], sib),
    )
    pl.semaphore_wait(barrier, 6)
    for i in range(quarters):
        for way in range(2):

            @pl.when(goes(way))
            def _(i=i, way=way):
                hop(i, way, 0).start()

    gather[1].start()
    gather[0].start()
    for i in range(4, 6):
        loads[i].wait()
    mg_all[f] = (mg_f32[...] * mscale_ref[...]).astype(jnp.bfloat16)
    loads[6].wait()
    ex_own[...] = ex_f32[...].astype(jnp.bfloat16)

    relay_all(1)
    for way in range(2):

        @pl.when(inward(way))
        def _(way=way):
            hop(merge_item, way, 0).start()

    @pl.when(outer)
    def _():
        ex_start(0, True)

    relay_all(2)
    for way in range(2):

        @pl.when(jnp.logical_and(jnp.logical_not(inward(way)), goes(way)))
        def _(way=way):
            hop(merge_item, way, 0).start()

    gather[1].wait_recv()
    gather[2].start()

    @pl.when(inner)
    def _():
        relay(merge_item, 1)
        ex_start(2, True, (0, 1))
        relay(merge_item, 2)
        ex_start(0, False, (0,))

    @pl.when(outer)
    def _():
        relay_all(3)

    for load in loads[7:]:
        load.wait()
    rd_own[...] = (rd_f32[...] * rscale_ref[...]).astype(jnp.bfloat16)

    @pl.when(outer)
    def _():
        ex_all[:, small:] = jnp.zeros((width, big - small), jnp.bfloat16)
        for slot in range(4):
            rd_all[slot, small:] = jnp.zeros((big - small, piece), jnp.bfloat16)

    def place_own(is_inner):
        first, size = part(is_inner)
        ex_all[columns(f), :size] = ex_own[:, first : first + size]
        rd_all[f, :size] = rd_own[first : first + size]

    both(place_own)

    def project(slot):
        return jnp.dot(xg[:, columns(slot)], dv_all[slot], preferred_element_type=jnp.float32)

    gather[0].wait_recv()
    gather[2].wait_recv()
    act[...] = project(f)

    def project_more(d):
        for i in range(quarters):
            over_wait(i, d)
        for way in range(2):

            @pl.when(comes(way, d))
            def _(way=way):
                act[...] += project(origin(way, d))

    project_more(1)
    project_more(2)
    project_more(3)

    @pl.when(outer)
    def _():
        ex_start(1, True, (0, 1))

    dvscale = jnp.concatenate([dscale_ref[...], vscale_ref[...]], axis=1)
    act[...] = jax.nn.gelu(act[...] * dvscale)

    lane = lax.broadcasted_iota(jnp.int32, (rows, rows), 1)
    for n in range(4):
        value = act[n * rows : (n + 1) * rows, local:]
        total = jnp.sum(value, axis=1, keepdims=True)
        squares = jnp.sum(value * value, axis=1, keepdims=True)
        table = jnp.where(lane == 0, total, jnp.where(lane == 1, squares, 0.0))
        stat[t, n] = jnp.transpose(table)[:8]
    stats = [
        rcopy(stat.at[t], stat.at[t], gsend.at[1], trecv.at[0], sib),
        rcopy(stat.at[t], stat.at[t], gsend.at[1], trecv.at[1], ynb),
        rcopy(
            stat.at[(1 - y) * 2 + c], stat.at[(1 - y) * 2 + c], gsend.at[1], trecv.at[2], sib
        ),
    ]
    stats[1].start()
    stats[0].start()

    @pl.when(outer)
    def _():
        relay(merge_item, 1)
        relay(merge_item, 2)

    groups = sbias_ref.shape[0]
    down = lax.broadcasted_iota(jnp.int32, (rows, rows), 0)
    bias = jnp.zeros((rows, rows), jnp.float32)
    for n in range(groups):
        bias = jnp.where(down == n, sbias_ref[n : n + 1, :], bias)
    bias = jnp.transpose(bias)
    stats[1].wait_recv()
    stats[2].start()
    stats[0].wait_recv()
    stats[2].wait_recv()

    @pl.when(inner)
    def _():
        ex_start(1, False)
        ex_start(2, True, (2,))

    @pl.when(outer)
    def _():
        ex_start(2, False)
        relay(merge_item, 3)

    inverse = 1.0 / (local * 4)
    group_lane = lax.broadcasted_iota(jnp.int32, (rows, 128), 1) // GDIM
    for n in range(4):
        here = slice(n * rows, (n + 1) * rows)
        summed = stat[0, n] + stat[1, n] + stat[2, n] + stat[3, n]
        table = jnp.transpose(jnp.concatenate([summed] * (rows // 8), axis=0))
        mean = table[:, 0:1] * inverse
        var = table[:, 1:2] * inverse - mean * mean
        gv = (
            (act[here, local:] - mean) * lax.rsqrt(var + epsilon) * vgain_ref[...]
            + vshift_ref[...]
        ).astype(jnp.bfloat16)
        per = 128 // GDIM
        for j in range(local // 128):
            at = slice(j * 128, (j + 1) * 128)
            mixed = jnp.dot(sw_ref[j * per], gv[:, at], preferred_element_type=jnp.float32)
            mixed = mixed + bias[:, j * per : j * per + 1]
            for k in range(1, per):
                n_group = j * per + k
                other = jnp.dot(sw_ref[n_group], gv[:, at], preferred_element_type=jnp.float32)
                other = other + bias[:, n_group : n_group + 1]
                mixed = jnp.where(group_lane == k, other, mixed)
            gated[here, at] = (act[here, at] * mixed).astype(jnp.bfloat16)

    closer, farther = jnp.where(inner, 2, 1), jnp.where(inner, 1, 2)
    second_slot = jnp.where(inner, peers[2], peers[1])
    last_slot = jnp.where(inner, peers[1], peers[2])
    merge_order = (f, mate, second_slot, last_slot)

    def merge_pair(k):
        return rcopy(
            p1.at[k, block((1 - c) * 2, 2)], r1.at[k], msend.at[0], mrecv.at[k, 0], sib
        )

    def merge_far(k):
        return rcopy(s1.at[k], x1.at[k], msend.at[1], mrecv.at[k, 1], ynb)

    def merge_send(k):
        merge_pair(k).wait_recv()
        s1[k] = (
            p1[k, block(c * 2 + 1 - y)].astype(jnp.float32)
            + r1[k, block(1 - y)].astype(jnp.float32)
        ).astype(jnp.bfloat16)
        merge_far(k).start()

    for k, slot in enumerate(merge_order):
        if k == 1:
            over_wait(merge_item, 1)
        if k == 2:

            @pl.when(outer)
            def _():
                over_wait(merge_item, 2)

        if k == 3:

            @pl.when(inner)
            def _():
                over_wait(merge_item, 2)

            over_wait(merge_item, 3)
        p1[k] = jnp.dot(gated[...], mg_all[slot], preferred_element_type=jnp.float32).astype(
            jnp.bfloat16
        )
        merge_pair(k).start()
        if k > 0:
            merge_send(k - 1)
    merge_send(3)
    for k, slot in enumerate(merge_order):
        merge_far(k).wait_recv()
        mid[:, columns(slot)] = (
            tok_ref[:, columns(slot)].astype(jnp.float32)
            + p1[k, block(c * 2 + y)].astype(jnp.float32)
            + r1[k, block(y)].astype(jnp.float32)
            + x1[k].astype(jnp.float32)
        ).astype(jnp.bfloat16)

    def group(zz, rr, yy):
        return zz * 4 + rr * 2 + yy

    def place(zz, rr, yy):
        return nm.at[group(zz, rr, yy), c]

    mine = place(z, r, y)
    mine[...] = norm(mid[...].astype(jnp.float32), cgain_ref[...])
    over_fs = rcopy(mine, mine, nsend.at[1], nrecv.at[20], znb)

    def spreading(b, zz):
        here, from_x = place(zz, r, y), place(zz, 1 - r, y)
        from_y, from_xy = place(zz, r, 1 - y), place(zz, 1 - r, 1 - y)

        def low(ref):
            return ref.at[pl.ds(0, half)]

        def high(ref):
            return ref.at[pl.ds(half, half)]

        routes = (
            (low(here), xnb), (high(here), xnb), (high(here), ynb), (low(here), ynb), (here, sib),
            (low(from_x), ynb), (high(from_y), xnb),
            (from_x, sib), (from_y, sib), (from_xy, sib),
        )
        return tuple(
            rcopy(ref, ref, nsend.at[0], nrecv.at[10 * b + k], dev)
            for k, (ref, dev) in enumerate(routes)
        )

    near, away = spreading(0, z), spreading(1, 1 - z)

    def first(spread):
        for k in (0, 2, 1, 3, 4):
            spread[k].start()

    def second(spread):
        spread[0].wait_recv()
        spread[5].start()
        spread[2].wait_recv()
        spread[6].start()

    def third(spread):
        spread[1].wait_recv()
        spread[7].start()
        spread[3].wait_recv()
        spread[8].start()

    def fourth(spread):
        spread[5].wait_recv()
        spread[6].wait_recv()
        spread[9].start()

    def gathered(spread):
        for k in (4, 7, 8, 9):
            spread[k].wait_recv()

    over_fs.start()

    @pl.when(outer)
    def _():
        ex_start(1, True, (2,))

    first(near)

    second(near)

    @pl.when(inner)
    def _():
        ex_start(0, False, (1, 2))

    third(near)
    over_fs.wait_recv()
    first(away)

    def rd_start(side, j, to_inner):
        rd_copy(side, j, to_inner).start()

    @pl.when(inner)
    def _():
        for side in (left, right):
            rd_start(side, 0, False)
        for side in (left, third_lanes, fourth_lanes):
            rd_start(side, 2, True)
            rd_start(side, 1, False)

    @pl.when(outer)
    def _():
        for side in (left, right):
            rd_start(side, 0, True)

    fourth(near)

    tall = 2 * rows
    start = pl.multiple_of(r * wide, wide)
    exscale = jnp.where(
        inner,
        exscale_ref[:, pl.ds(start, big)],
        jnp.concatenate(
            [
                exscale_ref[:, pl.ds(pl.multiple_of(start + big, 2 * GDIM), small)],
                jnp.zeros((1, big - small), jnp.float32),
            ],
            axis=1,
        ),
    )

    def expand(count, group_of):
        def step(i, _):
            g = group_of(i)
            upper = jnp.dot(
                nm[g].reshape(tall, width), ex_all[...], preferred_element_type=jnp.float32
            ) * exscale
            hid[g] = jnp.square(jax.nn.relu(upper)).astype(jnp.bfloat16)

        lax.fori_loop(0, count, step, None)

    def pick(if_inner, if_outer):
        return jnp.where(inner, if_inner, if_outer)

    slots = (f, f, mate, mate, second_slot) + (last_slot,) * 3 + (second_slot,) * 2
    sides = (left, right, left, right, left, left) + (third_lanes, fourth_lanes) * 2
    runs = (0, 0, 1, 1, 2, 3, 3, 3, 2, 2)
    came = (None, None, 0, 0, pick(2, 1)) + (pick(1, 2),) * 3 + (pick(2, 1),) * 2
    near_half, far_half = 0, 1
    units = tuple((k, h) for h in range(2) for k in range(4))
    units += tuple((k, h) for k in range(4, len(slots)) for h in (1, 0))

    def plane(h):
        return z if h == near_half else 1 - z

    def arrived(side, j):
        both(lambda is_inner: rd_copy(side, 0, is_inner, j).wait_recv())

    starts = tuple(run * piece + lane_cuts[side][0] for run, side in zip(runs, sides))

    def lanes(k):
        return slice(starts[k], starts[k] + lane_cuts[sides[k]][1])

    def reduce(u):
        k, h = units[u]
        slot, side = slots[k], sides[k]
        first, size = lane_cuts[side]
        if k > 1 and h == (near_half if k < 5 else far_half):
            arrived(side, came[k])
        zz = plane(h)

        def step(i, _):
            g = zz * 4 + i * 2
            p2[pl.ds(g, 2), :, :, lanes(k)] = (
                jnp.dot(
                    hid[pl.ds(g, 2)].reshape(2 * tall, big),
                    rd_all[slot, :, first : first + size],
                    preferred_element_type=jnp.float32,
                )
                .astype(jnp.bfloat16)
                .reshape(2, 2, rows, size)
            )

        lax.fori_loop(0, 2, step, None)
        pair(u).start()

    y_first = tuple(u % 2 == 0 for u in range(len(units)))

    def cols(k):
        return pl.ds(lanes(k).start, lanes(k).stop - lanes(k).start)

    def pair(u):
        k, h = units[u]
        at = pl.ds(plane(h) * 4, 4)
        return rcopy(
            p2.at[at, 1 - c, :, cols(k)], r2.at[at, :, cols(k)], fsend.at[0], frecv.at[0, u], sib
        )

    def summed_pair(k, g):
        return p2[g, c, :, lanes(k)].astype(jnp.float32) + r2[g, :, lanes(k)].astype(jnp.float32)

    def hop_one(u):
        k, h = units[u]
        at = (h, slice(None), slice(None), cols(k))
        return rcopy(
            f1.at[at], a1.at[at], fsend.at[1], frecv.at[1, u], ynb if y_first[u] else xnb
        )

    def hop_two(u):
        k, h = units[u]
        at = (h, slice(None), cols(k))
        return rcopy(
            f2.at[at], a2.at[at], fsend.at[2], frecv.at[2, u], xnb if y_first[u] else ynb
        )

    def lane_span(k):
        first, size = lane_cuts[sides[k]]
        return pl.ds(pl.multiple_of(slots[k] * piece + first, rows), size)

    def hop_three(k):
        q = slots[k] * 4 + sides[k]
        return rcopy(
            f3.at[:, cols(k)], a3.at[:, lane_span(k)], fsend.at[3], frecv.at[3, q], znb
        )

    def send_one(u):
        k, h = units[u]
        zz = plane(h)
        pair(u).wait_recv()
        for n in range(2):
            g = group(zz, n, 1 - y) if y_first[u] else group(zz, 1 - r, n)
            f1[h, n, :, lanes(k)] = summed_pair(k, g).astype(jnp.bfloat16)
        hop_one(u).start()

    def send_two(u):
        k, h = units[u]
        zz = plane(h)
        hop_one(u).wait_recv()
        g, n = (group(zz, 1 - r, y), 1 - r) if y_first[u] else (group(zz, r, 1 - y), 1 - y)
        f2[h, :, lanes(k)] = (
            summed_pair(k, g) + a1[h, n, :, lanes(k)].astype(jnp.float32)
        ).astype(jnp.bfloat16)
        hop_two(u).start()

    def own_sum(u):
        k, h = units[u]
        n = r if y_first[u] else y
        hop_two(u).wait_recv()
        return (
            summed_pair(k, group(plane(h), r, y))
            + a1[h, n, :, lanes(k)].astype(jnp.float32)
            + a2[h, :, lanes(k)].astype(jnp.float32)
        )

    def send_three(u):
        k, h = units[u]
        if h == far_half:
            f3[:, lanes(k)] = own_sum(u).astype(jnp.bfloat16)
            hop_three(k).start()

    def ex_arrived(is_inner):
        ref = ex_all.at[pl.ds(0, 3 * piece), pl.ds(0, part(is_inner)[1])]
        rcopy(ref, ref, csend.at[0], crecv.at[0], znb).wait_recv()

    done = set()

    def once(action, u):
        if 0 <= u < len(units) and (action, u) not in done:
            done.add((action, u))
            action(u)

    gathered(near)
    both(ex_arrived)

    @pl.when(outer)
    def _():
        second(away)

    expand(4, lambda i: z * 4 + i)

    @pl.when(inner)
    def _():
        second(away)

    away[4].wait_recv()
    expand(1, lambda i: group(1 - z, r, y) + i)
    once(reduce, 0)
    once(reduce, 1)
    third(away)
    once(send_one, 0)
    once(send_one, 1)

    @pl.when(outer)
    def _():
        for side in (left, third_lanes, fourth_lanes):
            rd_start(side, 2, False)
            rd_start(side, 1, True)

    once(reduce, 2)
    away[7].wait_recv()
    away[8].wait_recv()
    expand(2, lambda i: jnp.where(i == 0, group(1 - z, 1 - r, y), group(1 - z, r, 1 - y)))
    once(send_one, 2)
    fourth(away)
    once(reduce, 9)
    away[9].wait_recv()
    once(send_one, 9)
    expand(1, lambda i: group(1 - z, 1 - r, 1 - y) + i)
    turn = (0, 1, 2, 9, 4, 5, 3, 6, 7, 8) + tuple(range(10, len(units)))

    def late(action, n):
        if n >= 0:
            once(action, turn[n])

    for n in range(4, len(turn)):
        if n in (10, 12, 14, 16, 18):
            late(send_one, n - 1)
            late(send_two, n - 4)
            late(send_two, n - 3)
        late(reduce, n)
        if n == 5:
            late(send_two, 1)
        late(send_one, n - 1)
        late(send_two, n - 4)
        late(send_three, n - 8)
    count = len(units)
    once(send_one, count - 1)
    for u in range(count - 4, count):
        once(send_two, u)
        once(send_three, 2 * (u - count // 2))

    def stored(k):
        at = lane_span(k)
        return pltpu.make_async_copy(result.at[:, at], out_ref.at[:, at], out_sem)

    for k in range(len(slots)):
        at = lane_span(k)
        near_sum = own_sum(units.index((k, near_half)))
        hop_three(k).wait_recv()
        result[:, at] = (
            mid[:, at].astype(jnp.float32) + near_sum + a3[:, at].astype(jnp.float32)
        ).astype(jnp.bfloat16)
        stored(k).start()

    def sent(ref, sem):
        rcopy(ref, ref, sem, crecv.at[0], znb).wait_send()

    def few_sent(is_inner):
        own = rows * (2 if is_inner else 1)
        sent(dv_all.at[pl.ds(0, 3), pl.ds(0, own)], wsend.at[0])
        if is_inner:
            sent(dv_all.at[pl.ds(0, 3), pl.ds(0, 3 * rows)], wsend.at[1])
        for to_inner in (False, True):
            size = part(to_inner)[1]
            count = piece * (1 if to_inner == is_inner else 2)
            for n in (0, 2):
                sent(ex_all.at[pl.ds(0, count), pl.ds(0, size)], csend.at[n + int(to_inner)])

    both(few_sent)
    sent(dv_all.at[pl.ds(0, 3), pl.ds(0, 2 * rows)], xsend.at[0])
    sent(mg_all.at[pl.ds(0, 3), pl.ds(0, rows)], xsend.at[1])
    sent(xg.at[pl.ds(0, 3 * rows)], gsend.at[0])
    sent(stat.at[pl.ds(0, 3)], gsend.at[1])
    sent(r1, msend.at[0])
    sent(s1, msend.at[1])
    sent(nm.at[pl.ds(0, 7)], nsend.at[0])
    over_fs.wait_send()
    for n, ref in enumerate((r2, f1, f2, f3)):
        sent(ref, fsend.at[n])
    pltpu.make_async_copy(result, out_ref, out_sem).wait()


def fused_body(
    tokens,
    mixer_gain,
    direct_weight,
    direct_scale,
    value_weight,
    value_scale,
    value_gain,
    value_shift,
    spatial_weight,
    spatial_bias,
    merge_weight,
    merge_scale,
    channel_gain,
    expand_weight,
    expand_scale,
    reduce_weight,
    reduce_scale,
):
    bf = jnp.bfloat16
    rows, width = tokens.shape
    piece, local = direct_weight.shape
    wide = expand_weight.shape[1] // 2
    big = wide * 5 // 8
    thin = piece // 2
    seq = 4 * rows
    vm = pltpu.VMEM
    dma = pltpu.SemaphoreType.DMA
    f32 = jnp.float32
    small = (
        tokens, mixer_gain[None], direct_scale[None], value_scale[None], value_gain[None],
        value_shift[None], spatial_weight, spatial_bias, merge_scale[None], channel_gain[None],
        expand_scale[None], reduce_scale[None],
    )
    large = (direct_weight, value_weight, merge_weight, expand_weight, reduce_weight)
    return pl.pallas_call(
        fused_kernel,
        out_shape=jax.ShapeDtypeStruct((rows, width), bf),
        in_specs=[pl.BlockSpec(memory_space=pl.ANY)] * len(small + large),
        out_specs=pl.BlockSpec(memory_space=pl.ANY),
        scratch_shapes=[vm(a.shape, a.dtype) for a in small]
        + [
            vm((2, piece, local), f32),
            vm((local, piece), f32),
            vm((piece, wide), f32),
            vm((wide, piece), f32),
            vm((4, piece, 2 * local), bf),
            vm((4, local, piece), bf),
            vm((4 * piece, big), bf),
            vm((piece, wide), bf),
            vm((4, big, piece), bf),
            vm((wide, piece), bf),
            vm((seq, width), bf),
            vm((seq, 2 * local), f32),
            vm((4, 4, 8, rows), f32),
            vm((seq, local), bf),
            vm((4, seq, piece), bf),
            vm((4, 2 * rows, piece), bf),
            vm((4, rows, piece), bf),
            vm((4, rows, piece), bf),
            vm((rows, width), bf),
            vm((8, 2, rows, width), bf),
            vm((8, 2 * rows, big), bf),
            vm((8, 2, rows, width), bf),
            vm((8, rows, width), bf),
            vm((2, 2, rows, width), bf),
            vm((2, 2, rows, width), bf),
            vm((2, rows, width), bf),
            vm((2, rows, width), bf),
            vm((rows, width), bf),
            vm((rows, width), bf),
            vm((rows, width), bf),
            dma((17,)), dma,
            dma((2,)), dma((5, 4)),
            dma((2,)), dma((5, 4)),
            dma((4,)), dma((13,)),
            dma((2,)), dma((3,)), dma((3,)),
            dma((2,)), dma((4, 2)),
            dma((2,)), dma((21,)),
            dma((4,)), dma((4, 20)),
        ],
        compiler_params=pltpu.CompilerParams(
            collective_id=0, has_side_effects=True, vmem_limit_bytes=62 * 1024 * 1024
        ),
    )(*small, *large)


def solution(mesh):
    sizes = mesh.shape
    fused = sizes["rep"] == 2 and sizes["fs"] == 4 and sizes["tp"] == 4
    return jax.shard_map(
        fused_body if fused else body,
        mesh=mesh,
        in_specs=(
            P(("rep", "fs", "tp"), None),
            P(),
            P("fs", "tp"),
            P("tp"),
            P("fs", "tp"),
            P("tp"),
            P("tp"),
            P("tp"),
            P("tp", None, None),
            P("tp", None),
            P("tp", "fs"),
            P("fs"),
            P(),
            P("fs", "tp"),
            P("tp"),
            P("tp", "fs"),
            P("fs"),
        ),
        out_specs=P(("rep", "fs", "tp"), None),
        check_vma=False,
    )
```

```python
import jax
import jax.numpy as jnp
from jax import lax
from jax.experimental import pallas as pl
from jax.experimental.pallas import tpu as pltpu
from jax.sharding import PartitionSpec as P

GDIM = 64
BLOCK = 128


epsilon = 1e-06


def rms_rows(rows, gain):
    floats = rows.astype(jnp.float32)
    scaled = floats * lax.rsqrt(jnp.mean(floats * floats, axis=-1, keepdims=True) + epsilon)
    return (scaled * gain).astype(jnp.bfloat16)


def body(
    tokens,
    mixer_gain,
    direct_weight,
    direct_scale,
    value_weight,
    value_scale,
    value_gain,
    value_shift,
    spatial_weight,
    spatial_bias,
    merge_weight,
    merge_scale,
    channel_gain,
    expand_weight,
    expand_scale,
    reduce_weight,
    reduce_scale,
):
    direct_half = direct_weight.astype(jnp.bfloat16)
    value_half = value_weight.astype(jnp.bfloat16)
    merge_half = merge_weight.astype(jnp.bfloat16)
    expand_half = expand_weight.astype(jnp.bfloat16)
    reduce_half = reduce_weight.astype(jnp.bfloat16)
    full_expand, full_reduce, reduce_full_scale = (
        lax.all_gather(expand_half, "fs", axis=0, tiled=True),
        lax.all_gather(reduce_half, "fs", axis=1, tiled=True),
        lax.all_gather(reduce_scale.astype(jnp.bfloat16), "fs", axis=0, tiled=True).astype(
            reduce_scale.dtype
        ),
    )
    normed = rms_rows(tokens, mixer_gain)
    whole = lax.all_gather(normed, "tp", axis=0, tiled=True)
    seq_rows = whole.shape[0]
    local_width = direct_weight.shape[1]
    direct_pre = jnp.dot(
        whole,
        lax.all_gather(direct_half, "fs", axis=0, tiled=True),
        preferred_element_type=jnp.float32,
    )
    value_pre = jnp.dot(
        whole,
        lax.all_gather(value_half, "fs", axis=0, tiled=True),
        preferred_element_type=jnp.float32,
    )
    full_merge, merge_full_scale = (
        lax.all_gather(merge_half, "fs", axis=1, tiled=True),
        lax.all_gather(merge_scale.astype(jnp.bfloat16), "fs", axis=0, tiled=True).astype(
            merge_scale.dtype
        ),
    )
    direct = jax.nn.gelu(direct_pre * direct_scale)
    value = jax.nn.gelu(value_pre * value_scale)
    total, squares = lax.psum((jnp.sum(value, axis=1), jnp.sum(value * value, axis=1)), "tp")
    branch_width = local_width * lax.axis_size("tp")
    mean = (total / branch_width)[:, None]
    var = (squares / branch_width)[:, None] - mean * mean
    gated_value = ((value - mean) * lax.rsqrt(var + epsilon) * value_gain + value_shift).astype(
        jnp.bfloat16
    )
    local_groups = spatial_weight.shape[0]
    blocks = gated_value.reshape(seq_rows // BLOCK, BLOCK, local_groups, GDIM)
    mixed = jnp.einsum("gpq,nqgc->npgc", spatial_weight, blocks, preferred_element_type=jnp.float32)
    mixed = mixed + jnp.transpose(spatial_bias)[None, :, :, None]
    gated = (direct * mixed.reshape(seq_rows, local_width)).astype(jnp.bfloat16)
    rows = gated
    mix = lax.psum_scatter(
        (jnp.dot(rows, full_merge, preferred_element_type=jnp.float32) * merge_full_scale).astype(
            jnp.bfloat16
        ),
        "tp",
        scatter_dimension=0,
        tiled=True,
    ).astype(jnp.float32)
    middle = (tokens.astype(jnp.float32) + mix).astype(jnp.bfloat16)
    normed_mid = rms_rows(middle, channel_gain)
    whole_mid = lax.all_gather(normed_mid, "tp", axis=0, tiled=True)
    upper = jnp.dot(whole_mid, full_expand, preferred_element_type=jnp.float32)
    hidden = jnp.square(jax.nn.relu(upper * expand_scale)).astype(jnp.bfloat16)
    rows = hidden
    lower = lax.psum_scatter(
        (jnp.dot(rows, full_reduce, preferred_element_type=jnp.float32) * reduce_full_scale).astype(
            jnp.bfloat16
        ),
        "tp",
        scatter_dimension=0,
        tiled=True,
    ).astype(jnp.float32)
    return (middle.astype(jnp.float32) + lower).astype(jnp.bfloat16)


MESH = pl.DeviceIdType.MESH


def fused_kernel(
    tok_hbm, mgain_hbm, dscale_hbm, vscale_hbm, vgain_hbm, vshift_hbm, sw_hbm, sbias_hbm,
    mscale_hbm, cgain_hbm, exscale_hbm, rscale_hbm,
    dw_ref, vw_ref, mw_ref, ew_ref, rw_ref,
    out_ref,
    tok_ref, mgain_ref, dscale_ref, vscale_ref, vgain_ref, vshift_ref, sw_ref, sbias_ref,
    mscale_ref, cgain_ref, exscale_ref, rscale_ref,
    dv_f32, mg_f32, ex_f32, rd_f32,
    dv_all, mg_all, ex_all, ex_own, rd_all, rd_own,
    xg, act, stat, gated, p1, r1, s1, x1, mid,
    nm, hid, p2, r2, f1, a1, f2, a2, f3, a3,
    load_sem, wsend, wrecv, xsend, xrecv, csend, crecv, gsend, grecv, trecv, msend, mrecv,
    nsend, nrecv, fsend, frecv,
):
    rows, width = tok_ref.shape
    piece, local = dw_ref.shape
    big = hid.shape[2]
    wide = ex_own.shape[1]
    small = wide - big
    half = rows // 2
    thin = piece // 2
    r = lax.axis_index("rep")
    f = lax.axis_index("fs")
    t = lax.axis_index("tp")
    y, c = t // 2, t % 2
    z = f % 2
    mate = f + 1 - 2 * z
    peers = (mate, (f + 2) % 4, (mate + 2) % 4)
    sib = {"tp": y * 2 + (1 - c)}
    ynb = {"tp": (1 - y) * 2 + c}
    xnb = {"rep": 1 - r}
    znb = {"fs": mate}

    barrier = pltpu.get_barrier_semaphore()
    for dev in (sib, ynb, xnb) + tuple({"fs": peer} for peer in peers):
        pl.semaphore_signal(barrier, inc=1, device_id=dev, device_id_type=MESH)

    def span(start, size):
        return pl.ds(pl.multiple_of(start, size), size)

    loads = [
        pltpu.make_async_copy(source, target, load_sem.at[i])
        for i, (source, target) in enumerate(
            (
                (dw_ref, dv_f32.at[0]),
                (vw_ref, dv_f32.at[1]),
                (tok_hbm, tok_ref),
                (mgain_hbm, mgain_ref),
                (mscale_hbm, mscale_ref),
                (mw_ref, mg_f32),
                (ew_ref.at[:, span(r * wide, wide)], ex_f32),
                (rscale_hbm, rscale_ref),
                (rw_ref.at[span(r * wide, wide)], rd_f32),
                (dscale_hbm, dscale_ref),
                (vscale_hbm, vscale_ref),
                (vgain_hbm, vgain_ref),
                (vshift_hbm, vshift_ref),
                (sw_hbm, sw_ref),
                (sbias_hbm, sbias_ref),
                (cgain_hbm, cgain_ref),
                (exscale_hbm, exscale_ref),
            )
        )
    ]
    for load in loads:
        load.start()

    def rcopy(src, dst, ssem, rsem, dev):
        return pltpu.make_async_remote_copy(
            src_ref=src, dst_ref=dst, send_sem=ssem, recv_sem=rsem,
            device_id=dev, device_id_type=MESH,
        )

    quarters = 2 * rows // half
    merge_item = quarters

    def item(i, slot, q):
        if i < quarters:
            return dv_all.at[slot, span(q * 2 * rows + i * half, half)]
        return mg_all.at[slot, span(q * rows, rows)]

    def origin(way, d):
        return lax.rem(f + (4 - d if way == 0 else d), 4)

    def comes(way, d):
        return f >= d if way == 0 else f + d <= 3

    def goes(way):
        return f < 3 if way == 0 else f > 0

    def inward(way):
        return f < 2 if way == 0 else f >= 2

    def hop(i, way, d):
        ref = item(i, origin(way, d), r)
        to = lax.rem(f + (1 if way == 0 else 3), 4)
        return rcopy(
            ref, ref, wsend.at[min(d, 1)], wrecv.at[i, origin(way, d)], {"fs": to}
        )

    def over(i, way, d):
        slot = origin(way, d)
        ref = item(i, slot, r)
        return rcopy(ref, ref, xsend.at[i // quarters], xrecv.at[i, slot], xnb)

    def relay(i, d):
        for way in range(2):

            @pl.when(comes(way, d))
            def _(way=way):
                hop(i, way, d).wait_recv()
                over(i, way, d).start()

            if d < 3:

                @pl.when(jnp.logical_and(comes(way, d), goes(way)))
                def _(way=way):
                    hop(i, way, d).start()

    def relay_all(d):
        for i in range(quarters):
            relay(i, d)

    def over_wait(i, d):
        for way in range(2):

            @pl.when(comes(way, d))
            def _(way=way):
                over(i, way, d).wait_recv()

    inner = jnp.logical_or(f == 1, f == 2)
    outer = jnp.logical_not(inner)

    def part(to_inner):
        return (0, big) if to_inner else (big, small)

    cuts = ((0, thin // 2), (thin // 2, thin // 2), (thin, thin))

    def ex_copy(j, to_inner, h):
        first, size = part(to_inner)
        start, count = cuts[h]
        return rcopy(
            ex_own.at[pl.ds(start, count), pl.ds(first, size)],
            ex_all.at[span(f * piece + start, count), pl.ds(0, size)],
            csend.at[int(to_inner)], crecv.at[0], {"fs": peers[j]},
        )

    def ex_start(j, to_inner, which=(0, 1, 2)):
        for h in which:
            ex_copy(j, to_inner, h).start()

    left, right, third_lanes, fourth_lanes = range(4)
    lane_cuts = ((0, thin), (thin, thin), (thin, thin // 2), (thin + thin // 2, thin // 2))

    def rd_copy(side, j, to_inner, index=None):
        first, size = part(to_inner)
        cut = pl.ds(*lane_cuts[side])
        n = 1 + side * 3 + (j if index is None else index)
        return rcopy(
            rd_own.at[pl.ds(first, size), cut], rd_all.at[f, pl.ds(0, size), cut],
            csend.at[2 + int(to_inner)], crecv.at[n], {"fs": peers[j]},
        )

    def both(action):
        @pl.when(inner)
        def _():
            action(True)

        @pl.when(outer)
        def _():
            action(False)

    def norm(x, gain):
        return (
            x * lax.rsqrt(jnp.mean(x * x, axis=-1, keepdims=True) + epsilon) * gain
        ).astype(jnp.bfloat16)

    def block(n, size=1):
        return pl.ds(pl.multiple_of(n * rows, rows), size * rows)

    def columns(slot):
        return span(slot * piece, piece)

    for i in range(2):
        loads[i].wait()
        dv_all[f, :, i * local : (i + 1) * local] = dv_f32[i].astype(jnp.bfloat16)
    for i in range(2, 4):
        loads[i].wait()
    mine = xg.at[block(c * 2 + y)]
    mine[...] = norm(tok_ref[...].astype(jnp.float32), mgain_ref[...])
    far = xg.at[block(c * 2 + 1 - y)]
    gather = (
        rcopy(mine, mine, gsend.at[0], grecv.at[0], sib),
        rcopy(mine, mine, gsend.at[0], grecv.at[1], ynb),
        rcopy(far, far, gsend.at[0], grecv.at[2], sib),
    )
    pl.semaphore_wait(barrier, 6)
    for i in range(quarters):
        for way in range(2):

            @pl.when(goes(way))
            def _(i=i, way=way):
                hop(i, way, 0).start()

    gather[1].start()
    gather[0].start()
    for i in range(4, 6):
        loads[i].wait()
    mg_all[f] = (mg_f32[...] * mscale_ref[...]).astype(jnp.bfloat16)
    loads[6].wait()
    ex_own[...] = ex_f32[...].astype(jnp.bfloat16)

    relay_all(1)
    for way in range(2):

        @pl.when(inward(way))
        def _(way=way):
            hop(merge_item, way, 0).start()

    @pl.when(outer)
    def _():
        ex_start(0, True)

    relay_all(2)
    for way in range(2):

        @pl.when(jnp.logical_and(jnp.logical_not(inward(way)), goes(way)))
        def _(way=way):
            hop(merge_item, way, 0).start()

    gather[1].wait_recv()
    gather[2].start()

    @pl.when(inner)
    def _():
        relay(merge_item, 1)
        ex_start(2, True, (0, 1))
        relay(merge_item, 2)
        ex_start(0, False, (0,))

    @pl.when(outer)
    def _():
        relay_all(3)

    for load in loads[7:]:
        load.wait()
    rd_own[...] = (rd_f32[...] * rscale_ref[...]).astype(jnp.bfloat16)

    @pl.when(outer)
    def _():
        ex_all[:, small:] = jnp.zeros((width, big - small), jnp.bfloat16)
        for slot in range(4):
            rd_all[slot, small:] = jnp.zeros((big - small, piece), jnp.bfloat16)

    def place_own(is_inner):
        first, size = part(is_inner)
        ex_all[columns(f), :size] = ex_own[:, first : first + size]
        rd_all[f, :size] = rd_own[first : first + size]

    both(place_own)

    def project(slot):
        return jnp.dot(xg[:, columns(slot)], dv_all[slot], preferred_element_type=jnp.float32)

    gather[0].wait_recv()
    gather[2].wait_recv()
    act[...] = project(f)

    def project_more(d):
        for i in range(quarters):
            over_wait(i, d)
        for way in range(2):

            @pl.when(comes(way, d))
            def _(way=way):
                act[...] += project(origin(way, d))

    project_more(1)
    project_more(2)
    project_more(3)

    @pl.when(outer)
    def _():
        ex_start(1, True, (0, 1))

    dvscale = jnp.concatenate([dscale_ref[...], vscale_ref[...]], axis=1)
    act[...] = jax.nn.gelu(act[...] * dvscale)

    lane = lax.broadcasted_iota(jnp.int32, (rows, rows), 1)
    for n in range(4):
        value = act[n * rows : (n + 1) * rows, local:]
        total = jnp.sum(value, axis=1, keepdims=True)
        squares = jnp.sum(value * value, axis=1, keepdims=True)
        table = jnp.where(lane == 0, total, jnp.where(lane == 1, squares, 0.0))
        stat[t, n] = jnp.transpose(table)[:8]
    stats = [
        rcopy(stat.at[t], stat.at[t], gsend.at[1], trecv.at[0], sib),
        rcopy(stat.at[t], stat.at[t], gsend.at[1], trecv.at[1], ynb),
        rcopy(
            stat.at[(1 - y) * 2 + c], stat.at[(1 - y) * 2 + c], gsend.at[1], trecv.at[2], sib
        ),
    ]
    stats[1].start()
    stats[0].start()

    @pl.when(outer)
    def _():
        relay(merge_item, 1)
        relay(merge_item, 2)

    groups = sbias_ref.shape[0]
    down = lax.broadcasted_iota(jnp.int32, (rows, rows), 0)
    bias = jnp.zeros((rows, rows), jnp.float32)
    for n in range(groups):
        bias = jnp.where(down == n, sbias_ref[n : n + 1, :], bias)
    bias = jnp.transpose(bias)
    stats[1].wait_recv()
    stats[2].start()
    stats[0].wait_recv()
    stats[2].wait_recv()

    @pl.when(inner)
    def _():
        ex_start(1, False)
        ex_start(2, True, (2,))

    @pl.when(outer)
    def _():
        ex_start(2, False)
        relay(merge_item, 3)

    inverse = 1.0 / (local * 4)
    group_lane = lax.broadcasted_iota(jnp.int32, (rows, 128), 1) // GDIM
    for n in range(4):
        here = slice(n * rows, (n + 1) * rows)
        summed = stat[0, n] + stat[1, n] + stat[2, n] + stat[3, n]
        table = jnp.transpose(jnp.concatenate([summed] * (rows // 8), axis=0))
        mean = table[:, 0:1] * inverse
        var = table[:, 1:2] * inverse - mean * mean
        gv = (
            (act[here, local:] - mean) * lax.rsqrt(var + epsilon) * vgain_ref[...]
            + vshift_ref[...]
        ).astype(jnp.bfloat16)
        per = 128 // GDIM
        for j in range(local // 128):
            at = slice(j * 128, (j + 1) * 128)
            mixed = jnp.dot(sw_ref[j * per], gv[:, at], preferred_element_type=jnp.float32)
            mixed = mixed + bias[:, j * per : j * per + 1]
            for k in range(1, per):
                n_group = j * per + k
                other = jnp.dot(sw_ref[n_group], gv[:, at], preferred_element_type=jnp.float32)
                other = other + bias[:, n_group : n_group + 1]
                mixed = jnp.where(group_lane == k, other, mixed)
            gated[here, at] = (act[here, at] * mixed).astype(jnp.bfloat16)

    closer, farther = jnp.where(inner, 2, 1), jnp.where(inner, 1, 2)
    second_slot = jnp.where(inner, peers[2], peers[1])
    last_slot = jnp.where(inner, peers[1], peers[2])
    merge_order = (f, mate, second_slot, last_slot)

    def merge_pair(k):
        return rcopy(
            p1.at[k, block((1 - c) * 2, 2)], r1.at[k], msend.at[0], mrecv.at[k, 0], sib
        )

    def merge_far(k):
        return rcopy(s1.at[k], x1.at[k], msend.at[1], mrecv.at[k, 1], ynb)

    def merge_send(k):
        merge_pair(k).wait_recv()
        s1[k] = (
            p1[k, block(c * 2 + 1 - y)].astype(jnp.float32)
            + r1[k, block(1 - y)].astype(jnp.float32)
        ).astype(jnp.bfloat16)
        merge_far(k).start()

    for k, slot in enumerate(merge_order):
        if k == 1:
            over_wait(merge_item, 1)
        if k == 2:

            @pl.when(outer)
            def _():
                over_wait(merge_item, 2)

        if k == 3:

            @pl.when(inner)
            def _():
                over_wait(merge_item, 2)

            over_wait(merge_item, 3)
        p1[k] = jnp.dot(gated[...], mg_all[slot], preferred_element_type=jnp.float32).astype(
            jnp.bfloat16
        )
        merge_pair(k).start()
        if k > 0:
            merge_send(k - 1)
    merge_send(3)
    for k, slot in enumerate(merge_order):
        merge_far(k).wait_recv()
        mid[:, columns(slot)] = (
            tok_ref[:, columns(slot)].astype(jnp.float32)
            + p1[k, block(c * 2 + y)].astype(jnp.float32)
            + r1[k, block(y)].astype(jnp.float32)
            + x1[k].astype(jnp.float32)
        ).astype(jnp.bfloat16)

    def group(zz, rr, yy):
        return zz * 4 + rr * 2 + yy

    def place(zz, rr, yy):
        return nm.at[group(zz, rr, yy), c]

    mine = place(z, r, y)
    mine[...] = norm(mid[...].astype(jnp.float32), cgain_ref[...])
    over_fs = rcopy(mine, mine, nsend.at[1], nrecv.at[20], znb)

    def spreading(b, zz):
        here, from_x = place(zz, r, y), place(zz, 1 - r, y)
        from_y, from_xy = place(zz, r, 1 - y), place(zz, 1 - r, 1 - y)

        def low(ref):
            return ref.at[pl.ds(0, half)]

        def high(ref):
            return ref.at[pl.ds(half, half)]

        routes = (
            (low(here), xnb), (high(here), xnb), (high(here), ynb), (low(here), ynb), (here, sib),
            (low(from_x), ynb), (high(from_y), xnb),
            (from_x, sib), (from_y, sib), (from_xy, sib),
        )
        return tuple(
            rcopy(ref, ref, nsend.at[0], nrecv.at[10 * b + k], dev)
            for k, (ref, dev) in enumerate(routes)
        )

    near, away = spreading(0, z), spreading(1, 1 - z)

    def first(spread):
        for k in (0, 2, 1, 3, 4):
            spread[k].start()

    def second(spread):
        spread[0].wait_recv()
        spread[5].start()
        spread[2].wait_recv()
        spread[6].start()

    def third(spread):
        spread[1].wait_recv()
        spread[7].start()
        spread[3].wait_recv()
        spread[8].start()

    def fourth(spread):
        spread[5].wait_recv()
        spread[6].wait_recv()
        spread[9].start()

    def gathered(spread):
        for k in (4, 7, 8, 9):
            spread[k].wait_recv()

    over_fs.start()

    @pl.when(outer)
    def _():
        ex_start(1, True, (2,))

    first(near)

    second(near)

    @pl.when(inner)
    def _():
        ex_start(0, False, (1, 2))

    third(near)
    over_fs.wait_recv()
    first(away)

    def rd_start(side, j, to_inner):
        rd_copy(side, j, to_inner).start()

    @pl.when(inner)
    def _():
        for side in (left, right):
            rd_start(side, 0, False)
        for side in (left, third_lanes, fourth_lanes):
            rd_start(side, 2, True)
            rd_start(side, 1, False)

    @pl.when(outer)
    def _():
        for side in (left, right):
            rd_start(side, 0, True)

    fourth(near)

    tall = 2 * rows
    start = pl.multiple_of(r * wide, wide)
    exscale = jnp.where(
        inner,
        exscale_ref[:, pl.ds(start, big)],
        jnp.concatenate(
            [
                exscale_ref[:, pl.ds(pl.multiple_of(start + big, 2 * GDIM), small)],
                jnp.zeros((1, big - small), jnp.float32),
            ],
            axis=1,
        ),
    )

    def expand(count, group_of):
        def step(i, _):
            g = group_of(i)
            upper = jnp.dot(
                nm[g].reshape(tall, width), ex_all[...], preferred_element_type=jnp.float32
            ) * exscale
            hid[g] = jnp.square(jax.nn.relu(upper)).astype(jnp.bfloat16)

        lax.fori_loop(0, count, step, None)

    def pick(if_inner, if_outer):
        return jnp.where(inner, if_inner, if_outer)

    slots = (f, f, mate, mate, second_slot) + (last_slot,) * 3 + (second_slot,) * 2
    sides = (left, right, left, right, left, left) + (third_lanes, fourth_lanes) * 2
    runs = (0, 0, 1, 1, 2, 3, 3, 3, 2, 2)
    came = (None, None, 0, 0, pick(2, 1)) + (pick(1, 2),) * 3 + (pick(2, 1),) * 2
    near_half, far_half = 0, 1
    units = tuple((k, h) for h in range(2) for k in range(4))
    units += tuple((k, h) for k in range(4, len(slots)) for h in (1, 0))

    def plane(h):
        return z if h == near_half else 1 - z

    def arrived(side, j):
        both(lambda is_inner: rd_copy(side, 0, is_inner, j).wait_recv())

    starts = tuple(run * piece + lane_cuts[side][0] for run, side in zip(runs, sides))

    def lanes(k):
        return slice(starts[k], starts[k] + lane_cuts[sides[k]][1])

    def reduce(u):
        k, h = units[u]
        slot, side = slots[k], sides[k]
        first, size = lane_cuts[side]
        if k > 1 and h == (near_half if k < 5 else far_half):
            arrived(side, came[k])
        zz = plane(h)

        def step(i, _):
            g = zz * 4 + i * 2
            p2[pl.ds(g, 2), :, :, lanes(k)] = (
                jnp.dot(
                    hid[pl.ds(g, 2)].reshape(2 * tall, big),
                    rd_all[slot, :, first : first + size],
                    preferred_element_type=jnp.float32,
                )
                .astype(jnp.bfloat16)
                .reshape(2, 2, rows, size)
            )

        lax.fori_loop(0, 2, step, None)
        pair(u).start()

    y_first = tuple(u % 2 == 0 for u in range(len(units)))

    def cols(k):
        return pl.ds(lanes(k).start, lanes(k).stop - lanes(k).start)

    def pair(u):
        k, h = units[u]
        at = pl.ds(plane(h) * 4, 4)
        return rcopy(
            p2.at[at, 1 - c, :, cols(k)], r2.at[at, :, cols(k)], fsend.at[0], frecv.at[0, u], sib
        )

    def summed_pair(k, g):
        return p2[g, c, :, lanes(k)].astype(jnp.float32) + r2[g, :, lanes(k)].astype(jnp.float32)

    def hop_one(u):
        k, h = units[u]
        at = (h, slice(None), slice(None), cols(k))
        return rcopy(
            f1.at[at], a1.at[at], fsend.at[1], frecv.at[1, u], ynb if y_first[u] else xnb
        )

    def hop_two(u):
        k, h = units[u]
        at = (h, slice(None), cols(k))
        return rcopy(
            f2.at[at], a2.at[at], fsend.at[2], frecv.at[2, u], xnb if y_first[u] else ynb
        )

    def lane_span(k):
        first, size = lane_cuts[sides[k]]
        return pl.ds(pl.multiple_of(slots[k] * piece + first, rows), size)

    def hop_three(k):
        q = slots[k] * 4 + sides[k]
        return rcopy(
            f3.at[:, cols(k)], a3.at[:, lane_span(k)], fsend.at[3], frecv.at[3, q], znb
        )

    def send_one(u):
        k, h = units[u]
        zz = plane(h)
        pair(u).wait_recv()
        for n in range(2):
            g = group(zz, n, 1 - y) if y_first[u] else group(zz, 1 - r, n)
            f1[h, n, :, lanes(k)] = summed_pair(k, g).astype(jnp.bfloat16)
        hop_one(u).start()

    def send_two(u):
        k, h = units[u]
        zz = plane(h)
        hop_one(u).wait_recv()
        g, n = (group(zz, 1 - r, y), 1 - r) if y_first[u] else (group(zz, r, 1 - y), 1 - y)
        f2[h, :, lanes(k)] = (
            summed_pair(k, g) + a1[h, n, :, lanes(k)].astype(jnp.float32)
        ).astype(jnp.bfloat16)
        hop_two(u).start()

    def own_sum(u):
        k, h = units[u]
        n = r if y_first[u] else y
        hop_two(u).wait_recv()
        return (
            summed_pair(k, group(plane(h), r, y))
            + a1[h, n, :, lanes(k)].astype(jnp.float32)
            + a2[h, :, lanes(k)].astype(jnp.float32)
        )

    def send_three(u):
        k, h = units[u]
        if h == far_half:
            f3[:, lanes(k)] = own_sum(u).astype(jnp.bfloat16)
            hop_three(k).start()

    def ex_arrived(is_inner):
        ref = ex_all.at[pl.ds(0, 3 * piece), pl.ds(0, part(is_inner)[1])]
        rcopy(ref, ref, csend.at[0], crecv.at[0], znb).wait_recv()

    done = set()

    def once(action, u):
        if 0 <= u < len(units) and (action, u) not in done:
            done.add((action, u))
            action(u)

    gathered(near)
    both(ex_arrived)

    @pl.when(outer)
    def _():
        second(away)

    expand(4, lambda i: z * 4 + i)

    @pl.when(inner)
    def _():
        second(away)

    away[4].wait_recv()
    expand(1, lambda i: group(1 - z, r, y) + i)
    once(reduce, 0)
    once(reduce, 1)
    third(away)
    once(send_one, 0)
    once(send_one, 1)

    @pl.when(outer)
    def _():
        for side in (left, third_lanes, fourth_lanes):
            rd_start(side, 2, False)
            rd_start(side, 1, True)

    once(reduce, 2)
    away[7].wait_recv()
    away[8].wait_recv()
    expand(2, lambda i: jnp.where(i == 0, group(1 - z, 1 - r, y), group(1 - z, r, 1 - y)))
    once(send_one, 2)
    fourth(away)
    once(reduce, 9)
    away[9].wait_recv()
    once(send_one, 9)
    expand(1, lambda i: group(1 - z, 1 - r, 1 - y) + i)
    turn = (0, 1, 2, 9, 4, 5, 3, 6, 7, 8) + tuple(range(10, len(units)))

    def late(action, n):
        if n >= 0:
            once(action, turn[n])

    for n in range(4, len(turn)):
        if n in (10, 12, 14, 16, 18):
            late(send_one, n - 1)
            late(send_two, n - 4)
            late(send_two, n - 3)
        late(reduce, n)
        if n == 5:
            late(send_two, 1)
        late(send_one, n - 1)
        late(send_two, n - 4)
        late(send_three, n - 8)
    count = len(units)
    once(send_one, count - 1)
    for u in range(count - 4, count):
        once(send_two, u)
        once(send_three, 2 * (u - count // 2))

    for k in range(len(slots)):
        at = lane_span(k)
        near_sum = own_sum(units.index((k, near_half)))
        hop_three(k).wait_recv()
        out_ref[:, at] = (
            mid[:, at].astype(jnp.float32) + near_sum + a3[:, at].astype(jnp.float32)
        ).astype(jnp.bfloat16)

    def sent(ref, sem):
        rcopy(ref, ref, sem, crecv.at[0], znb).wait_send()

    def few_sent(is_inner):
        own = rows * (2 if is_inner else 1)
        sent(dv_all.at[pl.ds(0, 3), pl.ds(0, own)], wsend.at[0])
        if is_inner:
            sent(dv_all.at[pl.ds(0, 3), pl.ds(0, 3 * rows)], wsend.at[1])
        for to_inner in (False, True):
            size = part(to_inner)[1]
            count = piece * (1 if to_inner == is_inner else 2)
            for n in (0, 2):
                sent(ex_all.at[pl.ds(0, count), pl.ds(0, size)], csend.at[n + int(to_inner)])

    both(few_sent)
    sent(dv_all.at[pl.ds(0, 3), pl.ds(0, 2 * rows)], xsend.at[0])
    sent(mg_all.at[pl.ds(0, 3), pl.ds(0, rows)], xsend.at[1])
    sent(xg.at[pl.ds(0, 3 * rows)], gsend.at[0])
    sent(stat.at[pl.ds(0, 3)], gsend.at[1])
    sent(r1, msend.at[0])
    sent(s1, msend.at[1])
    sent(nm.at[pl.ds(0, 7)], nsend.at[0])
    over_fs.wait_send()
    for n, ref in enumerate((r2, f1, f2, f3)):
        sent(ref, fsend.at[n])


def fused_body(
    tokens,
    mixer_gain,
    direct_weight,
    direct_scale,
    value_weight,
    value_scale,
    value_gain,
    value_shift,
    spatial_weight,
    spatial_bias,
    merge_weight,
    merge_scale,
    channel_gain,
    expand_weight,
    expand_scale,
    reduce_weight,
    reduce_scale,
):
    bf = jnp.bfloat16
    rows, width = tokens.shape
    piece, local = direct_weight.shape
    wide = expand_weight.shape[1] // 2
    big = wide * 5 // 8
    thin = piece // 2
    seq = 4 * rows
    vm = pltpu.VMEM
    dma = pltpu.SemaphoreType.DMA
    f32 = jnp.float32
    small = (
        tokens, mixer_gain[None], direct_scale[None], value_scale[None], value_gain[None],
        value_shift[None], spatial_weight, spatial_bias, merge_scale[None], channel_gain[None],
        expand_scale[None], reduce_scale[None],
    )
    large = (direct_weight, value_weight, merge_weight, expand_weight, reduce_weight)
    return pl.pallas_call(
        fused_kernel,
        out_shape=vm((rows, width), bf),
        in_specs=[pl.BlockSpec(memory_space=pl.ANY)] * len(small + large),
        out_specs=pl.BlockSpec(memory_space=vm),
        scratch_shapes=[vm(a.shape, a.dtype) for a in small]
        + [
            vm((2, piece, local), f32),
            vm((local, piece), f32),
            vm((piece, wide), f32),
            vm((wide, piece), f32),
            vm((4, piece, 2 * local), bf),
            vm((4, local, piece), bf),
            vm((4 * piece, big), bf),
            vm((piece, wide), bf),
            vm((4, big, piece), bf),
            vm((wide, piece), bf),
            vm((seq, width), bf),
            vm((seq, 2 * local), f32),
            vm((4, 4, 8, rows), f32),
            vm((seq, local), bf),
            vm((4, seq, piece), bf),
            vm((4, 2 * rows, piece), bf),
            vm((4, rows, piece), bf),
            vm((4, rows, piece), bf),
            vm((rows, width), bf),
            vm((8, 2, rows, width), bf),
            vm((8, 2 * rows, big), bf),
            vm((8, 2, rows, width), bf),
            vm((8, rows, width), bf),
            vm((2, 2, rows, width), bf),
            vm((2, 2, rows, width), bf),
            vm((2, rows, width), bf),
            vm((2, rows, width), bf),
            vm((rows, width), bf),
            vm((rows, width), bf),
            dma((17,)),
            dma((2,)), dma((5, 4)),
            dma((2,)), dma((5, 4)),
            dma((4,)), dma((13,)),
            dma((2,)), dma((3,)), dma((3,)),
            dma((2,)), dma((4, 2)),
            dma((2,)), dma((21,)),
            dma((4,)), dma((4, 20)),
        ],
        compiler_params=pltpu.CompilerParams(
            collective_id=0, has_side_effects=True, vmem_limit_bytes=60 * 1024 * 1024
        ),
    )(*small, *large)


def solution(mesh):
    sizes = mesh.shape
    fused = sizes["rep"] == 2 and sizes["fs"] == 4 and sizes["tp"] == 4
    return jax.shard_map(
        fused_body if fused else body,
        mesh=mesh,
        in_specs=(
            P(("rep", "fs", "tp"), None),
            P(),
            P("fs", "tp"),
            P("tp"),
            P("fs", "tp"),
            P("tp"),
            P("tp"),
            P("tp"),
            P("tp", None, None),
            P("tp", None),
            P("tp", "fs"),
            P("fs"),
            P(),
            P("fs", "tp"),
            P("tp"),
            P("tp", "fs"),
            P("fs"),
        ),
        out_specs=P(("rep", "fs", "tp"), None),
        check_vma=False,
    )
```
